32 devices in a mesh: sp: 4 (over y, x), tp: 8 (over z, core).
Axes of the slice: x: 2, y: 2, z: 4, core: 2. Of those that a mesh axis runs over, the one named last changes fastest.
Arguments:
- tokens: bfloat16 [3, 2048, 4096], P(None, 'sp', 'tp'), may hold values from -6 to 6
- new_token: bfloat16 [3, 1, 4096], P(None, None, 'tp'), may hold values from -6 to 6
- query_weight: bfloat16 [4096, 4096], P(None, 'tp'), may hold values from -0.09375 to 0.09375
- key_weight: bfloat16 [4096, 4096], P(None, 'tp'), may hold values from -0.09375 to 0.09375
- value_weight: bfloat16 [4096, 4096], P(None, 'tp'), may hold values from -0.09375 to 0.09375
- log_decay: float32 [64], P('tp'), may hold values from -0.034 to 0
Outputs:
- state: bfloat16 [3, 64, 64, 64], P(None, 'tp', 'sp')
- read: bfloat16 [3, 4096], P(None, 'tp')
The draws below stay inside these ranges and needn't reach their ends.
All inputs are finite; a program needn't handle non-finite values.
Results may differ from the reference program's by a relative error of at most 0.012.
Values may be sent and summed in bfloat16 or wider, within the bound.
A program may use at most 64 MiB of HBM per device.

```python
import jax
import jax.numpy as jnp
from jax import lax

D = 4096
HEADS = 64
HD = 64
SEQS = 3
SPAN = 512
LEN = 2048
N_SP = 4


def draw_log_decay(key, part):
    choose_key = jax.random.fold_in(key, 11)
    fast_key = jax.random.fold_in(key, 12)
    slow_key = jax.random.fold_in(key, 13)
    chain_len = max(LEN, 64)
    fast_heads = jax.random.randint(choose_key, (HEADS,), 0, 2) == 1
    slow_rates = -jax.random.uniform(slow_key, (HEADS,), jnp.float32, 0.1, 2.0) / chain_len
    fast_rates = -1.0 / jax.random.uniform(fast_key, (HEADS,), jnp.float32, 30.0, 100.0)
    return jnp.where(fast_heads, fast_rates, slow_rates).astype(jnp.float32)


def shard_levels(own_key, dims, shards, low, top_value):
    def one(axis_at, parts):
        heights = jax.random.uniform(jax.random.fold_in(jax.random.fold_in(own_key, 6), axis_at), (parts,), jnp.float32, low / len(shards), top_value / len(shards))
        return jnp.repeat(jnp.exp(heights), dims[axis_at] // parts).reshape((-1,) + (1,) * (len(dims) - axis_at - 1))

    loudness = one(*shards[0])
    for cut in shards[1:]:
        loudness = loudness * one(*cut)
    return loudness


def bell_draw(rng, shape, spread, bound, pieces=(), kind=jnp.bfloat16):
    drawn = jax.random.normal(rng, shape, jnp.float32) * spread
    if len(pieces) > 0:
        drawn = shard_levels(rng, shape, pieces, -0.22, 0.18) * drawn
    return jnp.clip(drawn, min=-bound, max=bound).astype(kind)


def setup_inputs(seed: int = 0) -> dict:
    streams_of = jax.random.split(jax.random.key(seed), 7)
    return {
        "tokens": bell_draw(streams_of[0], (SEQS, LEN, D), 1.0, 6.0, ((1, 4), (2, 8))),
        "new_token": bell_draw(streams_of[1], (SEQS, 1, D), 1.0, 6.0, ((2, 8),)),
        "query_weight": bell_draw(streams_of[2], (D, HEADS * HD), D ** -0.5, 0.09375, ((1, 8),)),
        "key_weight": bell_draw(streams_of[3], (D, HEADS * HD), D ** -0.5, 0.09375, ((1, 8),)),
        "value_weight": bell_draw(streams_of[4], (D, HEADS * HD), D ** -0.5, 0.09375, ((1, 8),)),
        "log_decay": draw_log_decay(jax.random.fold_in(streams_of[6], 71), 0),
    }


def rotate(values, positions):
    half_dim = values.shape[-1] // 2
    inverse = 10000.0 ** (-jnp.arange(half_dim, dtype=jnp.float32) / half_dim)
    angles = positions.astype(jnp.float32)[:, None, None] * inverse[None, None, :]
    cosine = jnp.cos(angles)
    sine_part = jnp.sin(angles)
    first = values[..., :half_dim]
    second = values[..., half_dim:]
    return jnp.concatenate([first * cosine - second * sine_part, first * sine_part + second * cosine], axis=-1)

def group_norm(output):
    centered = output - lax.optimization_barrier(jnp.mean(output, axis=-1, keepdims=True))
    return centered * lax.rsqrt(lax.optimization_barrier(jnp.mean(centered * centered, axis=-1, keepdims=True)) + 1e-05)

def reference(tokens, new_token, query_weight, key_weight, value_weight, log_decay):
    key_scale = HD ** (-0.5)
    positions = jnp.arange(LEN, dtype=jnp.int32)
    to_end = (SPAN - 1 - positions % SPAN).astype(jnp.float32)
    block_ids = jnp.arange(N_SP, dtype=jnp.float32)
    new_position = jnp.full((1,), LEN, jnp.int32)
    query_heads = query_weight.reshape(D, HEADS, HD).transpose(1, 0, 2)
    key_heads = key_weight.reshape(D, HEADS, HD).transpose(1, 0, 2)
    value_heads = value_weight.reshape(D, HEADS, HD).transpose(1, 0, 2)

    def single_head(inputs):
        w_query, w_key, w_value, logarithm_rate = inputs
        projected = jnp.dot(tokens, w_key, preferred_element_type=jnp.float32)[:, :, None, :]
        key_rows = (rotate(projected, positions) * key_scale).astype(jnp.bfloat16)[:, :, 0, :]
        value_rows = jnp.dot(tokens, w_value, preferred_element_type=jnp.float32).astype(jnp.bfloat16)
        weighted = (key_rows.astype(jnp.float32) * jnp.exp(logarithm_rate * to_end)[None, :, None]).astype(jnp.bfloat16)
        weighted = weighted.astype(jnp.float32).reshape(SEQS, N_SP, SPAN, HD)
        value_blocks = value_rows.astype(jnp.float32).reshape(SEQS, N_SP, SPAN, HD)
        segment_states = jnp.einsum('sbtk,sbtv->sbkv', weighted, value_blocks, precision=lax.Precision.HIGHEST)
        carried_state = jnp.exp(logarithm_rate * SPAN * (N_SP - 1 - block_ids))
        closing_state = jnp.einsum('eyzt,y->ezt', segment_states, carried_state, precision=lax.Precision.HIGHEST)
        new_query = rotate(jnp.dot(new_token, w_query, preferred_element_type=jnp.float32)[:, :, None, :], new_position)
        new_query = new_query.astype(jnp.bfloat16)[:, 0, 0, :]
        fresh_key = rotate(jnp.dot(new_token, w_key, preferred_element_type=jnp.float32)[:, :, None, :], new_position)
        fresh_key = (fresh_key * key_scale).astype(jnp.bfloat16)[:, 0, 0, :]
        new_value = jnp.dot(new_token, w_value, preferred_element_type=jnp.float32).astype(jnp.bfloat16)[:, 0, :]
        query_entries = new_query.astype(jnp.float32)
        unscaled_read = jnp.exp(logarithm_rate) * jnp.einsum('bol,bo->bl', closing_state, query_entries, precision=lax.Precision.HIGHEST)
        unscaled_read = unscaled_read + lax.optimization_barrier(jnp.sum(query_entries * fresh_key.astype(jnp.float32), axis=-1, keepdims=True)) * new_value.astype(jnp.float32)
        return (closing_state.astype(jnp.bfloat16), group_norm(unscaled_read).astype(jnp.bfloat16))
    states, reads = lax.map(single_head, (query_heads, key_heads, value_heads, log_decay))
    return (states.transpose(1, 0, 2, 3), reads.transpose(1, 0, 2).reshape(SEQS, HEADS * HD))
```

```python
import functools

import jax
import jax.numpy as jnp
import numpy as np
from jax import lax
from jax.experimental import pallas as pl
from jax.experimental.pallas import tpu as pltpu
from jax.sharding import PartitionSpec as P

HD = 64
LANES = 128
NEW_ROWS = 8
F32 = jnp.float32
BF16 = jnp.bfloat16


def lane_iota(shape):
    return lax.broadcasted_iota(jnp.int32, shape, len(shape) - 1)


def rotated(block, cosine, sine):
    half = HD // 2
    low = lane_iota(block.shape) % HD < half
    swapped = jnp.where(
        low, pltpu.roll(block, LANES - half, 1), pltpu.roll(block, half, 1)
    )
    return block * cosine + swapped * sine


def kernel(
    n_sp, n_tp, parts,
    tokens, fresh, wq_hbm, wk_hbm, wv_hbm, inverse_ref, decay_ref,
    state_out, read_out,
    x, nx, wq, wk, wv, acc_k, acc_v, cos_ref, sin_ref, fade_ref, rows_ref,
    q_spread, own_term, sums, stage, landed, totals,
    load_sem, weight_sem, rx, rn, fwd, share, nfwd, nshare, rs_tx, rs_rx,
):
    seqs, span, feat = tokens.shape
    inner = wk.shape[1]
    heads = inner // HD
    chips = n_tp // 2
    pieces = seqs * parts
    size = span // parts
    keep = HD // n_sp
    sp = lax.axis_index("sp")
    tp = lax.axis_index("tp")
    z, k = tp // 2, tp % 2
    MESH = pl.DeviceIdType.MESH

    def to_tp(index):
        return {"tp": index}

    partner = z * 2 + 1 - k
    own_loads = [
        pltpu.make_async_copy(
            tokens.at[s // parts, pl.ds(s % parts * size, size)], x.at[tp, s], load_sem.at[s]
        )
        for s in range(pieces)
    ]
    new_load = pltpu.make_async_copy(fresh, nx.at[tp], load_sem.at[pieces])
    new_load.start()
    for copy in own_loads:
        copy.start()
    weight_loads = [
        pltpu.make_async_copy(a, b, weight_sem.at[i])
        for i, (a, b) in enumerate(((wk_hbm, wk), (wv_hbm, wv), (wq_hbm, wq)))
    ]

    barrier = pltpu.get_barrier_semaphore()

    @pl.when(z > 0)
    def _():
        pl.semaphore_signal(barrier, inc=1, device_id=to_tp(tp - 2), device_id_type=MESH)

    @pl.when(z < chips - 1)
    def _():
        pl.semaphore_signal(barrier, inc=1, device_id=to_tp(tp + 2), device_id_type=MESH)

    pl.semaphore_signal(barrier, inc=1, device_id=to_tp(partner), device_id_type=MESH)
    for o in range(1, n_sp):
        pl.semaphore_signal(
            barrier, inc=1, device_id={"sp": lax.rem(sp + o, n_sp)}, device_id_type=MESH
        )
    pl.semaphore_wait(
        barrier, n_sp + (z > 0).astype(jnp.int32) + (z < chips - 1).astype(jnp.int32)
    )

    def x_copy(c, s, sem, target):
        p = 2 * c + k
        return pltpu.make_async_remote_copy(
            x.at[p, s], x.at[p, s], sem, rx.at[p, s], device_id=to_tp(target), device_id_type=MESH
        )

    def n_copy(c, sem, target):
        p = 2 * c + k
        return pltpu.make_async_remote_copy(
            nx.at[p], nx.at[p], sem, rn.at[p], device_id=to_tp(target), device_id_type=MESH
        )

    def x_arrived(p, s):
        pltpu.make_async_remote_copy(
            x.at[p, s], x.at[p, s], share.at[0, 0], rx.at[p, s],
            device_id=to_tp(partner), device_id_type=MESH,
        ).wait_recv()

    def n_arrived(p):
        pltpu.make_async_remote_copy(
            nx.at[p], nx.at[p], nshare.at[0], rn.at[p],
            device_id=to_tp(partner), device_id_type=MESH,
        ).wait_recv()

    new_load.wait()
    n_up = n_copy(z, nfwd.at[0, z], tp + 2)
    n_down = n_copy(z, nfwd.at[1, z], tp - 2)
    n_side = n_copy(z, nshare.at[z], partner)

    @pl.when(z < chips - 1)
    def _():
        n_up.start()

    @pl.when(z > 0)
    def _():
        n_down.start()

    n_side.start()
    for s in range(pieces):
        own_loads[s].wait()

        @pl.when(z < chips - 1)
        def _(s=s):
            x_copy(z, s, fwd.at[0, z, s], tp + 2).start()

        @pl.when(z > 0)
        def _(s=s):
            x_copy(z, s, fwd.at[1, z, s], tp - 2).start()

        x_copy(z, s, share.at[z, s], partner).start()

    for copy in weight_loads:
        copy.start()

    row = lax.broadcasted_iota(jnp.int32, (span, LANES), 0)
    within = lane_iota((1, LANES)) % HD
    first_half = jnp.where(within < HD // 2, -1.0, 1.0).astype(F32)
    inverse = inverse_ref[...]
    angles = (sp * span + row).astype(F32) * inverse
    cos_ref[...] = jnp.cos(angles)
    sin_ref[...] = jnp.sin(angles) * first_half
    new_angles = jnp.full((NEW_ROWS, LANES), n_sp * span, F32) * inverse
    new_cos = jnp.cos(new_angles)
    new_sin = jnp.sin(new_angles) * first_half
    head_of = lane_iota((1, inner)) // HD
    rate = jnp.zeros((1, inner), F32)
    for h in range(heads):
        rate = jnp.where(head_of == h, decay_ref[h], rate)
    to_end = (span - 1 - lax.broadcasted_iota(jnp.int32, (span, 1), 0)).astype(F32)
    fade_ref[...] = jnp.exp(to_end * rate)
    rows_ref[0:1] = jnp.exp(rate * (span * (n_sp - 1 - sp)).astype(F32))
    rows_ref[1:2] = jnp.exp(rate)

    for copy in weight_loads:
        copy.wait()

    def add(p, s, fresh_total):
        block = x[p, s]
        where = pl.ds(pl.multiple_of(p * feat, feat), feat)
        part_k = jnp.dot(block, wk[where, :], preferred_element_type=F32)
        part_v = jnp.dot(block, wv[where, :], preferred_element_type=F32)
        if fresh_total:
            acc_k[s] = part_k
            acc_v[s] = part_v
        else:
            acc_k[s] += part_k
            acc_v[s] += part_v

    @pl.loop(0, pieces)
    def _(s):
        add(tp, s, True)
        x_arrived(partner, s)
        add(partner, s, False)

    n_arrived(partner)

    def project_new():
        def piece(p, totals):
            where = pl.ds(pl.multiple_of(p * feat, feat), feat)
            block = jnp.concatenate(
                [nx[p].astype(F32), jnp.zeros((NEW_ROWS - seqs, feat), F32)], axis=0
            ).astype(BF16)
            return tuple(
                t + jnp.dot(block, w[where, :], preferred_element_type=F32)
                for t, w in zip(totals, (wk, wv, wq))
            )

        zero = jnp.zeros((NEW_ROWS, inner), F32)
        new_k, new_v, new_q = lax.fori_loop(0, n_tp, piece, (zero, zero, zero))
        keys, queries = [], []
        for j in range(inner // LANES):
            at = slice(j * LANES, (j + 1) * LANES)
            keys.append((rotated(new_k[:, at], new_cos, new_sin) * HD**-0.5).astype(BF16))
            queries.append(rotated(new_q[:, at], new_cos, new_sin).astype(BF16))
        key = jnp.concatenate(keys, axis=1).astype(F32)
        query = jnp.concatenate(queries, axis=1).astype(F32)
        value = new_v.astype(BF16).astype(F32)
        same = (
            lax.broadcasted_iota(jnp.int32, (inner, inner), 0) // HD
            == lax.broadcasted_iota(jnp.int32, (inner, inner), 1) // HD
        )
        product = query * key
        for h in range(heads):
            at = slice(h * HD, (h + 1) * HD)
            own_term[:, at] = jnp.sum(product[:, at], axis=-1, keepdims=True) * value[:, at]
        pick = lax.broadcasted_iota(jnp.int32, (HD, inner), 0) == lane_iota((HD, inner)) % HD
        for s in range(seqs):
            spread = jnp.where(pick, query[s : s + 1], 0.0).astype(BF16)
            q_spread[s] = jnp.dot(
                spread, jnp.where(same, 1.0, 0.0).astype(BF16), preferred_element_type=F32
            )

    def rs_copy(s, o):
        peer = lax.rem(sp + o, n_sp)
        return pltpu.make_async_remote_copy(
            stage.at[s, peer], landed.at[s, sp], rs_tx.at[s, peer], rs_rx.at[s, sp],
            device_id={"sp": peer}, device_id_type=MESH,
        )

    def finish(i):
        s, part = i // parts, i % parts
        where = pl.ds(pl.multiple_of(part * size, size), size)
        cosine, sine = cos_ref[where, :], sin_ref[where, :]
        lane = lane_iota((HD, LANES))
        for j in range(inner // LANES):
            at = slice(j * LANES, (j + 1) * LANES)
            key = (rotated(acc_k[i, :, at], cosine, sine) * HD**-0.5).astype(BF16)
            weighted = (key.astype(F32) * fade_ref[where, at]).astype(BF16)
            value = acc_v[i, :, at].astype(BF16)
            both = lax.dot_general(
                weighted, value, (((0,), (0,)), ((), ())), preferred_element_type=F32
            )
            state = jnp.where(lane < HD, both[:HD], both[HD:])
            sums[:, at] = jnp.where(part == 0, state, sums[:, at] + state)

        @pl.when(part == parts - 1)
        def _():
            scaled = sums[...] * rows_ref[0:1]
            read = jnp.sum(scaled * q_spread[s], axis=0, keepdims=True)
            for o in range(n_sp):
                stage[s, o, 0:keep] = scaled[o * keep : (o + 1) * keep]
                stage[s, o, keep : keep + 1] = read
            for o in range(1, n_sp):
                rs_copy(s, o).start()
            totals[s] = stage[s, sp]

    far = jnp.maximum(z, chips - 1 - z)

    def decode(i):
        d = i // (2 * pieces) + 1
        s = (i // 2) % pieces
        step = 2 * (i % 2) - 1
        c = z + step * d
        return d, s, step, c, (c >= 0) & (c < chips)

    def onward(step):
        nxt = z - step
        return nxt, (nxt >= 0) & (nxt < chips), (step + 1) // 2

    @pl.loop(0, 2 * pieces * (chips - 1))
    def _(i):
        d, s, step, c, valid = decode(i)
        nxt, pass_on, way = onward(step)

        @pl.when(valid)
        def _():
            @pl.when(s == 0)
            def _():
                n_arrived(2 * c + k)

                @pl.when(pass_on)
                def _():
                    n_copy(c, nfwd.at[way, c], 2 * nxt + k).start()

                n_copy(c, nshare.at[c], partner).start()

            x_arrived(2 * c + k, s)

            @pl.when(pass_on)
            def _():
                x_copy(c, s, fwd.at[way, c, s], 2 * nxt + k).start()

            x_copy(c, s, share.at[c, s], partner).start()
            add(2 * c + k, s, False)

            @pl.when(s == 0)
            def _():
                n_arrived(2 * c + 1 - k)

            x_arrived(2 * c + 1 - k, s)
            add(2 * c + 1 - k, s, False)

        last = (d == far) & (step == 1)

        @pl.when(last & (s == 0))
        def _():
            project_new()

        @pl.when(last)
        def _():
            finish(s)

    raws = []
    for s in range(seqs):
        for o in range(1, n_sp):
            src = lax.rem(sp + o, n_sp)
            pltpu.make_async_remote_copy(
                stage.at[s, src], landed.at[s, src], rs_tx.at[s, src], rs_rx.at[s, src],
                device_id={"sp": src}, device_id_type=MESH,
            ).wait_recv()
        total = None
        for j in range(n_sp):
            term = jnp.where(sp == j, totals[s], landed[s, j])
            total = term if total is None else total + term
        kept = total[0:keep].astype(BF16)
        for h in range(heads):
            state_out[s, h] = kept[:, h * HD : (h + 1) * HD]
        raws.append(total[keep : keep + 1] * rows_ref[1:2] + own_term[s : s + 1])
    raw = jnp.concatenate(raws, axis=0)
    for h in range(heads):
        at = slice(h * HD, (h + 1) * HD)
        head = raw[:, at]
        centered = head - jnp.mean(head, axis=-1, keepdims=True)
        spread = jnp.mean(centered * centered, axis=-1, keepdims=True)
        read_out[:, at] = (centered * lax.rsqrt(spread + 1e-05)).astype(BF16)

    @pl.when(z < chips - 1)
    def _():
        n_up.wait_send()

    @pl.when(z > 0)
    def _():
        n_down.wait_send()

    n_side.wait_send()
    for s in range(seqs):
        for o in range(1, n_sp):
            rs_copy(s, o).wait_send()
    for s in range(pieces):
        @pl.when(z < chips - 1)
        def _(s=s):
            x_copy(z, s, fwd.at[0, z, s], tp + 2).wait_send()

        @pl.when(z > 0)
        def _(s=s):
            x_copy(z, s, fwd.at[1, z, s], tp - 2).wait_send()

        x_copy(z, s, share.at[z, s], partner).wait_send()

    @pl.loop(0, 2 * pieces * (chips - 1))
    def _(i):
        d, s, step, c, valid = decode(i)
        nxt, pass_on, way = onward(step)

        @pl.when(valid)
        def _():
            @pl.when(s == 0)
            def _():
                @pl.when(pass_on)
                def _():
                    n_copy(c, nfwd.at[way, c], 2 * nxt + k).wait_send()

                n_copy(c, nshare.at[c], partner).wait_send()

            @pl.when(pass_on)
            def _():
                x_copy(c, s, fwd.at[way, c, s], 2 * nxt + k).wait_send()

            x_copy(c, s, share.at[c, s], partner).wait_send()


def one_of(n, values):
    total = 0
    for k, value in enumerate(values):
        if value:
            total = total + (n == k).astype(jnp.int32) * value
    return total


def middle_order(main, moved):
    near = [(0, i) for i in main]
    far = [(2, i) for i in moved + main]
    order = [(kind, i) for i in moved for kind in (0, 1)]
    order += [(1, i) for i in main]
    for at in range(max(len(near), len(far))):
        order += near[at : at + 1] + far[at : at + 1]
    return order


def moved_kernel(
    n_sp, n_tp, parts,
    tokens, fresh, wq_hbm, wk_hbm, wv_hbm, inverse_ref, decay_ref,
    state_out, read_out,
    x, xc, nx, wq, wk, wv, we, acc_k, acc_v, acc_c, cos_ref, sin_ref, fade_ref, rows_ref,
    q_spread, own_term, sums, stage, landed, totals, hint, hint_in, stage_c, landed_c,
    load_sem, weight_sem, rx, rn, ry, rw, fwd, share, nsend, ysend, yshare, wsend, wxsend,
    hint_sem, rs_tx, rs_rx, c_tx, c_rx,
):
    seqs, span, feat = tokens.shape
    inner = wk.shape[1]
    heads = inner // HD
    half = inner // 2
    chunks = half // LANES
    chips = n_tp // 2
    pieces = seqs * parts
    size = span // parts
    keep = HD // n_sp
    groups = n_tp // 2
    moved_seq = seqs - 1
    main = list(range(moved_seq * parts))
    moved = list(range(moved_seq * parts, pieces))
    sp = lax.axis_index("sp")
    tp = lax.axis_index("tp")
    z, k = tp // 2, tp % 2
    row_y, row_x = sp // 2, sp % 2
    x_peer = sp + 1 - 2 * row_x
    y_peer = sp + 2 - 4 * row_y
    MESH = pl.DeviceIdType.MESH
    end_int = (z == 0).astype(jnp.int32) + (z == chips - 1).astype(jnp.int32)
    end = end_int > 0
    mid = end_int == 0
    partner = z * 2 + 1 - k
    mate = z + 1 - 2 * (z % 2)
    mate_tp = 2 * mate + k
    other = chips - 1 - z
    other_tp = 2 * other + k
    second = end_int * (chips - 1 - mate) + (1 - end_int) * (chips - 1 - z)
    third = end_int * (chips - 1 - z) + (1 - end_int) * (chips - 1 - mate)

    own_loads = {
        s: pltpu.make_async_copy(
            tokens.at[s // parts, pl.ds(s % parts * size, size)], x.at[tp, s], load_sem.at[s]
        )
        for s in range(pieces)
    }
    new_load = pltpu.make_async_copy(fresh, nx.at[tp], load_sem.at[pieces])
    new_load.start()
    for s in moved + main:
        own_loads[s].start()
    weight_loads = [
        pltpu.make_async_copy(a, b, weight_sem.at[i])
        for i, (a, b) in enumerate(((wk_hbm, wk), (wv_hbm, wv), (wq_hbm, wq)))
    ]

    barrier = pltpu.get_barrier_semaphore()
    for o in range(1, n_tp):
        pl.semaphore_signal(
            barrier, inc=1, device_id={"tp": lax.rem(tp + o, n_tp)}, device_id_type=MESH
        )
    for o in range(1, n_sp):
        pl.semaphore_signal(
            barrier, inc=1, device_id={"sp": lax.rem(sp + o, n_sp)}, device_id_type=MESH
        )
        pl.semaphore_signal(
            barrier, inc=1, device_id={"sp": lax.rem(sp + o, n_sp), "tp": mate_tp},
            device_id_type=MESH,
        )
    pl.semaphore_wait(barrier, n_tp - 1 + 2 * (n_sp - 1))

    def x_copy(c, s, sem, target):
        p = 2 * c + k
        return pltpu.make_async_remote_copy(
            x.at[p, s], x.at[p, s], sem, rx.at[p, s],
            device_id={"tp": target}, device_id_type=MESH,
        )

    def to_mate(c, s):
        return x_copy(c, s, fwd.at[0, c, s], mate_tp)

    def to_other(c, s):
        return x_copy(c, s, fwd.at[1, c, s], other_tp)

    def to_partner(c, s):
        return x_copy(c, s, share.at[c, s], partner)

    def x_arrived(p, s):
        pltpu.make_async_remote_copy(
            x.at[p, s], x.at[p, s], share.at[0, 0], rx.at[p, s],
            device_id={"tp": partner}, device_id_type=MESH,
        ).wait_recv()

    def y_send(c, j):
        p = 2 * c + k
        return pltpu.make_async_remote_copy(
            x.at[p, moved[0] + j], xc.at[p, j], ysend.at[c, j], ry.at[p, j],
            device_id={"sp": y_peer}, device_id_type=MESH,
        )

    def y_share(c, j):
        p = 2 * c + k
        return pltpu.make_async_remote_copy(
            xc.at[p, j], xc.at[p, j], yshare.at[c, j], ry.at[p, j],
            device_id={"tp": partner}, device_id_type=MESH,
        )

    def y_arrived(p, j):
        pltpu.make_async_remote_copy(
            xc.at[p, j], xc.at[p, j], yshare.at[0, 0], ry.at[p, j],
            device_id={"tp": partner}, device_id_type=MESH,
        ).wait_recv()

    def w_rows(p):
        return pl.ds(pl.multiple_of(p * feat, feat), feat)

    def w_cols(cc):
        return pl.ds(pl.multiple_of(row_y * half + cc * LANES, LANES), LANES)

    def w_send(cc, g, kv):
        p = row_x * groups + g
        return pltpu.make_async_remote_copy(
            (wk, wv)[kv].at[w_rows(p), w_cols(cc)],
            we.at[cc, w_rows(p), pl.ds(kv * LANES, LANES)],
            wsend.at[cc, g, kv], rw.at[cc, p, kv],
            device_id={"tp": mate_tp}, device_id_type=MESH,
        )

    def w_pass(cc, g, kv):
        p = row_x * groups + g
        where = we.at[cc, w_rows(p), pl.ds(kv * LANES, LANES)]
        return pltpu.make_async_remote_copy(
            where, where, wxsend.at[cc, g, kv], rw.at[cc, p, kv],
            device_id={"sp": x_peer}, device_id_type=MESH,
        )

    def w_arrived(cc, p, kv):
        where = we.at[cc, w_rows(p), pl.ds(kv * LANES, LANES)]
        pltpu.make_async_remote_copy(
            where, where, wxsend.at[cc, 0, kv], rw.at[cc, p, kv],
            device_id={"sp": x_peer}, device_id_type=MESH,
        ).wait_recv()

    def n_copy(o):
        return pltpu.make_async_remote_copy(
            nx.at[tp], nx.at[tp], nsend.at[o], rn.at[tp],
            device_id={"tp": lax.rem(tp + o, n_tp)}, device_id_type=MESH,
        )

    def n_arrived(o):
        p = lax.rem(tp + o, n_tp)
        pltpu.make_async_remote_copy(
            nx.at[p], nx.at[p], nsend.at[0], rn.at[p],
            device_id={"tp": p}, device_id_type=MESH,
        ).wait_recv()

    hint_copy = pltpu.make_async_remote_copy(
        hint, hint_in, hint_sem.at[0], hint_sem.at[1],
        device_id={"tp": mate_tp}, device_id_type=MESH,
    )

    new_load.wait()
    for o in range(1, n_tp):
        n_copy(o).start()
    for j, s in enumerate(moved):
        own_loads[s].wait()

        @pl.when(mid)
        def _(j=j, s=s):
            to_other(z, s).start()
            y_send(z, j).start()
            to_partner(z, s).start()

        @pl.when(end)
        def _(s=s):
            to_mate(z, s).start()

    for s in main:
        own_loads[s].wait()
        to_partner(z, s).start()

        @pl.when(mid)
        def _(s=s):
            to_mate(z, s).start()
            to_other(z, s).start()

    for copy in weight_loads:
        copy.start()

    row = lax.broadcasted_iota(jnp.int32, (span, LANES), 0)
    within = lane_iota((1, LANES)) % HD
    first_half = jnp.where(within < HD // 2, -1.0, 1.0).astype(F32)
    inverse = inverse_ref[...]

    def tables(slot, column):
        angles = (column * span + row).astype(F32) * inverse
        cos_ref[slot] = jnp.cos(angles)
        sin_ref[slot] = jnp.sin(angles) * first_half

    for copy in weight_loads[:2]:
        copy.wait()

    @pl.when(end)
    def _():
        for g in range(groups):
            for kv in range(2):
                w_send(0, g, kv).start()
        for s in main:
            to_mate(z, s).start()
        for cc in range(1, chunks):
            for g in range(groups):
                for kv in range(2):
                    w_send(cc, g, kv).start()

    tables(0, sp)

    @pl.when(mid)
    def _():
        tables(1, y_peer)

    new_angles = jnp.full((NEW_ROWS, LANES), n_sp * span, F32) * inverse
    new_cos = jnp.cos(new_angles)
    new_sin = jnp.sin(new_angles) * first_half
    head_of = lane_iota((1, inner)) // HD
    rate = jnp.zeros((1, inner), F32)
    for h in range(heads):
        rate = jnp.where(head_of == h, decay_ref[h], rate)
    to_end = (span - 1 - lax.broadcasted_iota(jnp.int32, (span, 1), 0)).astype(F32)
    fade_ref[...] = jnp.exp(to_end * rate)
    rows_ref[0:1] = jnp.exp(rate * (span * (n_sp - 1 - sp)).astype(F32))
    rows_ref[1:2] = jnp.exp(rate)
    hint[...] = jnp.zeros(hint.shape, F32)
    hint[1:2] = rate
    weight_loads[2].wait()

    def add(p, s, fresh_total):
        block = x[p, s]
        where = w_rows(p)
        part_k = jnp.dot(block, wk[where, :], preferred_element_type=F32)
        part_v = jnp.dot(block, wv[where, :], preferred_element_type=F32)
        if fresh_total:
            acc_k[s] = part_k
            acc_v[s] = part_v
        else:
            acc_k[s] += part_k
            acc_v[s] += part_v

    own_pieces = end_int * len(main) + (1 - end_int) * pieces

    @pl.loop(0, pieces)
    def _(i):
        s = lax.rem(i + (1 - end_int) * len(main), pieces)

        @pl.when(i < own_pieces)
        def _():
            add(tp, s, True)

        @pl.when(i < own_pieces)
        def _():
            x_arrived(partner, s)
            add(partner, s, False)

    for o in range(1, n_tp):
        n_arrived(o)

    same = (
        lax.broadcasted_iota(jnp.int32, (inner, inner), 0) // HD
        == lax.broadcasted_iota(jnp.int32, (inner, inner), 1) // HD
    )
    pick = lax.broadcasted_iota(jnp.int32, (HD, inner), 0) == lane_iota((HD, inner)) % HD

    def project_new():
        def piece(p, totals):
            where = w_rows(p)
            block = jnp.concatenate(
                [nx[p].astype(F32), jnp.zeros((NEW_ROWS - seqs, feat), F32)], axis=0
            ).astype(BF16)
            return tuple(
                t + jnp.dot(block, w[where, :], preferred_element_type=F32)
                for t, w in zip(totals, (wk, wv, wq))
            )

        zero = jnp.zeros((NEW_ROWS, inner), F32)
        new_k, new_v, new_q = lax.fori_loop(0, n_tp, piece, (zero, zero, zero))
        keys, queries = [], []
        for j in range(inner // LANES):
            at = slice(j * LANES, (j + 1) * LANES)
            keys.append((rotated(new_k[:, at], new_cos, new_sin) * HD**-0.5).astype(BF16))
            queries.append(rotated(new_q[:, at], new_cos, new_sin).astype(BF16))
        key = jnp.concatenate(keys, axis=1).astype(F32)
        query = jnp.concatenate(queries, axis=1).astype(F32)
        value = new_v.astype(BF16).astype(F32)
        product = query * key
        for h in range(heads):
            at = slice(h * HD, (h + 1) * HD)
            own_term[:, at] = jnp.sum(product[:, at], axis=-1, keepdims=True) * value[:, at]
        hint[0:1] = query[moved_seq : moved_seq + 1]
        for s in range(seqs):
            spread = jnp.where(pick, query[s : s + 1], 0.0).astype(BF16)
            q_spread[s] = jnp.dot(
                spread, jnp.where(same, 1.0, 0.0).astype(BF16), preferred_element_type=F32
            )

    project_new()

    @pl.when(end)
    def _():
        hint_copy.start()

    def rs_copy(s, o):
        peer = lax.rem(sp + o, n_sp)
        return pltpu.make_async_remote_copy(
            stage.at[s, peer], landed.at[s, sp], rs_tx.at[s, peer], rs_rx.at[s, sp],
            device_id={"sp": peer}, device_id_type=MESH,
        )

    def outer(weighted, value):
        both = lax.dot_general(
            weighted, value, (((0,), (0,)), ((), ())), preferred_element_type=F32
        )
        return jnp.where(lane_iota((HD, LANES)) < HD, both[:HD], both[HD:])

    def finish(i):
        s, part = i // parts, i % parts
        where = pl.ds(pl.multiple_of(part * size, size), size)
        cosine, sine = cos_ref[0, where, :], sin_ref[0, where, :]
        for j in range(inner // LANES):
            at = slice(j * LANES, (j + 1) * LANES)
            key = (rotated(acc_k[i, :, at], cosine, sine) * HD**-0.5).astype(BF16)
            weighted = (key.astype(F32) * fade_ref[where, at]).astype(BF16)
            value = acc_v[i, :, at].astype(BF16)
            state = outer(weighted, value)
            sums[:, at] = jnp.where(part == 0, state, sums[:, at] + state)

        @pl.when(part == parts - 1)
        def _():
            scaled = sums[...] * rows_ref[0:1]
            read = jnp.sum(scaled * q_spread[s], axis=0, keepdims=True)
            for o in range(n_sp):
                stage[s, o, 0:keep] = scaled[o * keep : (o + 1) * keep]
                stage[s, o, keep : keep + 1] = read
            for o in range(1, n_sp):
                rs_copy(s, o).start()
            totals[s] = stage[s, sp]

    def c_add(cc, p, fresh_total):
        where = w_rows(p)
        for t in range(parts):
            for side, block in ((0, x[p, moved[0] + t]), (1, xc[p, t])):
                both = jnp.dot(block, we[cc, where, :], preferred_element_type=F32)
                if fresh_total:
                    acc_c[side, t] = both
                else:
                    acc_c[side, t] += both

    def c_copy(cc, o):
        return pltpu.make_async_remote_copy(
            stage_c.at[cc, o], landed_c.at[cc, sp], c_tx.at[cc, o], c_rx.at[cc, sp],
            device_id={"sp": o, "tp": mate_tp}, device_id_type=MESH,
        )

    def c_finish(cc):
        pair_rate = hint_in[1:2, w_cols(cc)]
        query = hint_in[0:1, w_cols(cc)]
        total = jnp.zeros((HD, LANES), F32)
        for side, column in ((0, sp), (1, y_peer)):
            state = jnp.zeros((HD, LANES), F32)
            for t in range(parts):
                at = slice(t * size, (t + 1) * size)
                key = (
                    rotated(acc_c[side, t, :, :LANES], cos_ref[side, at], sin_ref[side, at])
                    * HD**-0.5
                ).astype(BF16)
                fade = jnp.exp(to_end[at] * pair_rate)
                weighted = (key.astype(F32) * fade).astype(BF16)
                state = state + outer(weighted, acc_c[side, t, :, LANES:].astype(BF16))
            total = total + state * jnp.exp(
                pair_rate * (span * (n_sp - 1 - column)).astype(F32)
            )
        spread = jnp.where(pick[:, :LANES], query, 0.0).astype(BF16)
        spread = jnp.dot(
            spread, jnp.where(same[:LANES, :LANES], 1.0, 0.0).astype(BF16),
            preferred_element_type=F32,
        )
        read = jnp.sum(total * spread, axis=0, keepdims=True)
        for o in range(n_sp):
            stage_c[cc, o, 0:keep] = total[o * keep : (o + 1) * keep]
            stage_c[cc, o, keep : keep + 1] = read
        for o in range(n_sp):
            c_copy(cc, o).start()

    order = middle_order(main, moved)
    steps = end_int * (len(main) * (chips - 1)) + (1 - end_int) * len(order)

    def decode(n):
        kind = end_int * (n // len(main)) + (1 - end_int) * one_of(n, [o[0] for o in order])
        s = end_int * (n % len(main)) + (1 - end_int) * one_of(n, [o[1] for o in order])
        c = (
            (kind == 0).astype(jnp.int32) * mate
            + (kind == 1).astype(jnp.int32) * second
            + (kind == 2).astype(jnp.int32) * third
        )
        return kind, c, s

    first_w = 2 * len(moved) + 1
    c_at = len(order) - 2

    def y_pass(c, j):
        y_arrived(2 * c + k, j)
        y_share(c, j).start()

    @pl.loop(0, len(order) + 1)
    def _(n):
        kind, c, s = decode(n)
        is_moved = s >= moved[0]

        @pl.when(n < steps)
        def _():
            x_arrived(2 * c + k, s)

            @pl.when(mid & (kind == 0))
            def _():
                to_other(c, s).start()

            @pl.when(mid & (kind > 0) & (s < moved[0]))
            def _():
                to_mate(c, s).start()

            @pl.when(mid & is_moved)
            def _():
                y_send(c, s - moved[0]).start()

            to_partner(c, s).start()

        @pl.when(mid & (n >= first_w) & (n < first_w + groups))
        def _():
            for kv in range(2):
                w_arrived(0, row_x * groups + n - first_w, kv)
                w_pass(0, n - first_w, kv).start()

        @pl.when(mid & (n >= 3) & (n < 3 + parts))
        def _():
            y_pass(z, n - 3)

        @pl.when(mid & (n >= 6) & (n < 6 + 2 * parts))
        def _():
            m = n - 6
            y_pass((m % 2) * second + (1 - m % 2) * mate, m // 2)

        @pl.when(mid & (n >= c_at - parts) & (n < c_at))
        def _():
            y_pass(third, n - (c_at - parts))

        @pl.when(n < steps)
        def _():
            add(2 * c + k, s, False)

        kind_b, c_b, s_b = decode(n - 1)

        @pl.when((n >= 1) & (n <= steps))
        def _():
            x_arrived(2 * c_b + 1 - k, s_b)
            add(2 * c_b + 1 - k, s_b, False)

            @pl.when(kind_b == 2)
            def _():
                finish(s_b)

        @pl.when(mid & (n == c_at))
        def _():
            for cx in range(chips):
                for j in range(parts):
                    y_arrived(2 * cx + 1 - k, j)
            for g in range(groups):
                for kv in range(2):
                    w_arrived(0, (1 - row_x) * groups + g, kv)
            c_add(0, 0, True)

            @pl.loop(1, n_tp)
            def _(p):
                c_add(0, p, False)

            hint_copy.wait_recv()
            c_finish(0)

    @pl.when(mid)
    def _():
        for cc in range(1, chunks):
            for g in range(groups + 1):
                if g < groups:
                    for kv in range(2):
                        w_arrived(cc, row_x * groups + g, kv)
                        w_pass(cc, g, kv).start()
                    c_add(cc, row_x * groups + g, g == 0)
                if g > 0:
                    for kv in range(2):
                        w_arrived(cc, (1 - row_x) * groups + g - 1, kv)
                    c_add(cc, (1 - row_x) * groups + g - 1, False)
            c_finish(cc)

    def gather(s):
        for o in range(1, n_sp):
            src = lax.rem(sp + o, n_sp)
            pltpu.make_async_remote_copy(
                stage.at[s, src], landed.at[s, src], rs_tx.at[s, src], rs_rx.at[s, src],
                device_id={"sp": src}, device_id_type=MESH,
            ).wait_recv()
        total = None
        for j in range(n_sp):
            term = jnp.where(sp == j, totals[s], landed[s, j])
            total = term if total is None else total + term
        totals[s] = total

    for s in range(moved_seq):
        gather(s)

    @pl.when(mid)
    def _():
        gather(moved_seq)

    @pl.when(end)
    def _():
        for cc in range(chunks):
            for o in range(n_sp):
                pltpu.make_async_remote_copy(
                    stage_c.at[cc, o], landed_c.at[cc, o], c_tx.at[cc, o], c_rx.at[cc, o],
                    device_id={"sp": o, "tp": mate_tp}, device_id_type=MESH,
                ).wait_recv()
            for side in range(2):
                at = slice(side * half + cc * LANES, side * half + (cc + 1) * LANES)
                totals[moved_seq, :, at] = landed_c[cc, 2 * side] + landed_c[cc, 2 * side + 1]

    raws = []
    for s in range(seqs):
        total = totals[s]
        kept = total[0:keep].astype(BF16)
        for h in range(heads):
            state_out[s, h] = kept[:, h * HD : (h + 1) * HD]
        raws.append(total[keep : keep + 1] * rows_ref[1:2] + own_term[s : s + 1])
    raw = jnp.concatenate(raws, axis=0)
    for h in range(heads):
        at = slice(h * HD, (h + 1) * HD)
        head = raw[:, at]
        centered = head - jnp.mean(head, axis=-1, keepdims=True)
        spread = jnp.mean(centered * centered, axis=-1, keepdims=True)
        read_out[:, at] = (centered * lax.rsqrt(spread + 1e-05)).astype(BF16)

    for o in range(1, n_tp):
        n_copy(o).wait_send()
    for s in main:
        to_partner(z, s).wait_send()
        to_mate(z, s).wait_send()
        for o in range(1, n_sp):
            if s % parts == 0:
                rs_copy(s // parts, o).wait_send()

    @pl.when(end)
    def _():
        hint_copy.wait_send()
        for s in moved:
            to_mate(z, s).wait_send()
        for cc in range(chunks):
            for g in range(groups):
                for kv in range(2):
                    w_send(cc, g, kv).wait_send()

    @pl.when(mid)
    def _():
        for j, s in enumerate(moved):
            to_other(z, s).wait_send()
            to_partner(z, s).wait_send()
        for s in main:
            to_other(z, s).wait_send()
        for cx in range(chips):
            for j in range(parts):
                y_send(cx, j).wait_send()
                y_share(cx, j).wait_send()
        for o in range(1, n_sp):
            rs_copy(moved_seq, o).wait_send()
        for cc in range(chunks):
            for g in range(groups):
                for kv in range(2):
                    w_pass(cc, g, kv).wait_send()
            for o in range(n_sp):
                c_copy(cc, o).wait_send()

    @pl.loop(0, len(order))
    def _(n):
        kind, c, s = decode(n)

        @pl.when(n < steps)
        def _():
            @pl.when(mid & (kind == 0))
            def _():
                to_other(c, s).wait_send()

            @pl.when(mid & (kind > 0) & (s < moved[0]))
            def _():
                to_mate(c, s).wait_send()

            to_partner(c, s).wait_send()


def solution(mesh):
    n_sp, n_tp = mesh.shape["sp"], mesh.shape["tp"]

    def body(tokens, new_token, query_weight, key_weight, value_weight, log_decay):
        seqs, span, feat = tokens.shape
        width, inner = key_weight.shape
        heads = inner // HD
        keep = HD // n_sp
        rows = -(-(keep + 1) // 8) * 8
        chips = n_tp // 2
        half = HD // 2
        parts = max(1, 8 // chips)
        pieces = seqs * parts
        size = span // parts
        inverse = np.float32(10000.0) ** (-np.arange(half, dtype=np.float32) / half)
        inverse = jnp.asarray(np.tile(inverse.astype(np.float32), LANES // half)[None])
        anywhere = pl.BlockSpec(memory_space=pl.ANY)
        vmem = pl.BlockSpec(memory_space=pltpu.VMEM)
        dma = pltpu.SemaphoreType.DMA
        moves = chips == 4 and n_sp == 4 and seqs > 1 and inner % (2 * LANES) == 0
        tokens_in = [
            pltpu.VMEM((n_tp, pieces, size, feat), BF16),
            pltpu.VMEM((n_tp, seqs, feat), BF16),
        ]
        weights_in = [pltpu.VMEM((width, inner), BF16)] * 3
        totals = [pltpu.VMEM((pieces, size, inner), F32)] * 2
        ends = [
            pltpu.VMEM((8, inner), F32),
            pltpu.VMEM((seqs, HD, inner), F32),
            pltpu.VMEM((NEW_ROWS, inner), F32),
            pltpu.VMEM((HD, inner), F32),
            pltpu.VMEM((seqs, n_sp, rows, inner), F32),
            pltpu.VMEM((seqs, n_sp, rows, inner), F32),
            pltpu.VMEM((seqs, rows, inner), F32),
        ]
        if moves:
            chunks = inner // 2 // LANES
            groups = n_tp // 2
            call = moved_kernel
            scratch = (
                tokens_in[:1]
                + [pltpu.VMEM((n_tp, parts, size, feat), BF16)]
                + tokens_in[1:]
                + weights_in
                + [pltpu.VMEM((chunks, width, 2 * LANES), BF16)]
                + totals
                + [
                    pltpu.VMEM((2, parts, size, 2 * LANES), F32),
                    pltpu.VMEM((2, span, LANES), F32),
                    pltpu.VMEM((2, span, LANES), F32),
                    pltpu.VMEM((span, inner), F32),
                ]
                + ends
                + [
                    pltpu.VMEM((8, inner), F32),
                    pltpu.VMEM((8, inner), F32),
                    pltpu.VMEM((chunks, n_sp, rows, LANES), F32),
                    pltpu.VMEM((chunks, n_sp, rows, LANES), F32),
                    dma((pieces + 1,)),
                    dma((3,)),
                    dma((n_tp, pieces)),
                    dma((n_tp,)),
                    dma((n_tp, parts)),
                    dma((chunks, n_tp, 2)),
                    dma((2, chips, pieces)),
                    dma((chips, pieces)),
                    dma((n_tp,)),
                    dma((chips, parts)),
                    dma((chips, parts)),
                    dma((chunks, groups, 2)),
                    dma((chunks, groups, 2)),
                    dma((2,)),
                    dma((seqs, n_sp)),
                    dma((seqs, n_sp)),
                    dma((chunks, n_sp)),
                    dma((chunks, n_sp)),
                ]
            )
        else:
            call = kernel
            scratch = (
                tokens_in
                + weights_in
                + totals
                + [
                    pltpu.VMEM((span, LANES), F32),
                    pltpu.VMEM((span, LANES), F32),
                    pltpu.VMEM((span, inner), F32),
                ]
                + ends
                + [
                    dma((pieces + 1,)),
                    dma((3,)),
                    dma((n_tp, pieces)),
                    dma((n_tp,)),
                    dma((2, chips, pieces)),
                    dma((chips, pieces)),
                    dma((2, chips)),
                    dma((chips,)),
                    dma((seqs, n_sp)),
                    dma((seqs, n_sp)),
                ]
            )
        return pl.pallas_call(
            functools.partial(call, n_sp, n_tp, parts),
            out_shape=(
                jax.ShapeDtypeStruct((seqs, heads, keep, HD), BF16),
                jax.ShapeDtypeStruct((seqs, inner), BF16),
            ),
            in_specs=[anywhere] * 5 + [vmem, pl.BlockSpec(memory_space=pltpu.SMEM)],
            out_specs=(vmem, vmem),
            scratch_shapes=scratch,
            compiler_params=pltpu.CompilerParams(
                collective_id=0, has_side_effects=True, vmem_limit_bytes=60 * 1024 * 1024
            ),
            name="retention",
        )(tokens, new_token.reshape(seqs, feat), query_weight, key_weight, value_weight, inverse, log_decay)

    return jax.shard_map(
        body,
        mesh=mesh,
        in_specs=(
            P(None, "sp", "tp"),
            P(None, None, "tp"),
            P(None, "tp"),
            P(None, "tp"),
            P(None, "tp"),
            P("tp"),
        ),
        out_specs=(P(None, "tp", "sp", None), P(None, "tp")),
        check_vma=False,
    )
```

```python
import functools

import jax
import jax.numpy as jnp
import numpy as np
from jax import lax
from jax.experimental import pallas as pl
from jax.experimental.pallas import tpu as pltpu
from jax.sharding import PartitionSpec as P

HD = 64
LANES = 128
NEW_ROWS = 8
F32 = jnp.float32
BF16 = jnp.bfloat16


def lane_iota(shape):
    return lax.broadcasted_iota(jnp.int32, shape, len(shape) - 1)


def rotated(block, cosine, sine):
    half = HD // 2
    low = lane_iota(block.shape) % HD < half
    swapped = jnp.where(
        low, pltpu.roll(block, LANES - half, 1), pltpu.roll(block, half, 1)
    )
    return block * cosine + swapped * sine


def kernel(
    n_sp, n_tp, parts,
    tokens, fresh, wq_hbm, wk_hbm, wv_hbm, inverse_ref, decay_ref,
    state_out, read_out,
    x, nx, wq, wk, wv, acc_k, acc_v, cos_ref, sin_ref, fade_ref, rows_ref,
    q_spread, own_term, sums, stage, landed, totals,
    load_sem, weight_sem, rx, rn, fwd, share, nfwd, nshare, rs_tx, rs_rx,
):
    seqs, span, feat = tokens.shape
    inner = wk.shape[1]
    heads = inner // HD
    chips = n_tp // 2
    pieces = seqs * parts
    size = span // parts
    keep = HD // n_sp
    sp = lax.axis_index("sp")
    tp = lax.axis_index("tp")
    z, k = tp // 2, tp % 2
    MESH = pl.DeviceIdType.MESH

    def to_tp(index):
        return {"tp": index}

    partner = z * 2 + 1 - k
    own_loads = [
        pltpu.make_async_copy(
            tokens.at[s // parts, pl.ds(s % parts * size, size)], x.at[tp, s], load_sem.at[s]
        )
        for s in range(pieces)
    ]
    new_load = pltpu.make_async_copy(fresh, nx.at[tp], load_sem.at[pieces])
    new_load.start()
    for copy in own_loads:
        copy.start()
    weight_loads = [
        pltpu.make_async_copy(a, b, weight_sem.at[i])
        for i, (a, b) in enumerate(((wk_hbm, wk), (wv_hbm, wv), (wq_hbm, wq)))
    ]

    barrier = pltpu.get_barrier_semaphore()

    @pl.when(z > 0)
    def _():
        pl.semaphore_signal(barrier, inc=1, device_id=to_tp(tp - 2), device_id_type=MESH)

    @pl.when(z < chips - 1)
    def _():
        pl.semaphore_signal(barrier, inc=1, device_id=to_tp(tp + 2), device_id_type=MESH)

    pl.semaphore_signal(barrier, inc=1, device_id=to_tp(partner), device_id_type=MESH)
    for o in range(1, n_sp):
        pl.semaphore_signal(
            barrier, inc=1, device_id={"sp": lax.rem(sp + o, n_sp)}, device_id_type=MESH
        )
    pl.semaphore_wait(
        barrier, n_sp + (z > 0).astype(jnp.int32) + (z < chips - 1).astype(jnp.int32)
    )

    def x_copy(c, s, sem, target):
        p = 2 * c + k
        return pltpu.make_async_remote_copy(
            x.at[p, s], x.at[p, s], sem, rx.at[p, s], device_id=to_tp(target), device_id_type=MESH
        )

    def n_copy(c, sem, target):
        p = 2 * c + k
        return pltpu.make_async_remote_copy(
            nx.at[p], nx.at[p], sem, rn.at[p], device_id=to_tp(target), device_id_type=MESH
        )

    def x_arrived(p, s):
        pltpu.make_async_remote_copy(
            x.at[p, s], x.at[p, s], share.at[0, 0], rx.at[p, s],
            device_id=to_tp(partner), device_id_type=MESH,
        ).wait_recv()

    def n_arrived(p):
        pltpu.make_async_remote_copy(
            nx.at[p], nx.at[p], nshare.at[0], rn.at[p],
            device_id=to_tp(partner), device_id_type=MESH,
        ).wait_recv()

    new_load.wait()
    n_up = n_copy(z, nfwd.at[0, z], tp + 2)
    n_down = n_copy(z, nfwd.at[1, z], tp - 2)
    n_side = n_copy(z, nshare.at[z], partner)

    @pl.when(z < chips - 1)
    def _():
        n_up.start()

    @pl.when(z > 0)
    def _():
        n_down.start()

    n_side.start()
    for s in range(pieces):
        own_loads[s].wait()

        @pl.when(z < chips - 1)
        def _(s=s):
            x_copy(z, s, fwd.at[0, z, s], tp + 2).start()

        @pl.when(z > 0)
        def _(s=s):
            x_copy(z, s, fwd.at[1, z, s], tp - 2).start()

        x_copy(z, s, share.at[z, s], partner).start()

    for copy in weight_loads:
        copy.start()

    row = lax.broadcasted_iota(jnp.int32, (span, LANES), 0)
    within = lane_iota((1, LANES)) % HD
    first_half = jnp.where(within < HD // 2, -1.0, 1.0).astype(F32)
    inverse = inverse_ref[...]
    angles = (sp * span + row).astype(F32) * inverse
    cos_ref[...] = jnp.cos(angles)
    sin_ref[...] = jnp.sin(angles) * first_half
    new_angles = jnp.full((NEW_ROWS, LANES), n_sp * span, F32) * inverse
    new_cos = jnp.cos(new_angles)
    new_sin = jnp.sin(new_angles) * first_half
    head_of = lane_iota((1, inner)) // HD
    rate = jnp.zeros((1, inner), F32)
    for h in range(heads):
        rate = jnp.where(head_of == h, decay_ref[h], rate)
    to_end = (span - 1 - lax.broadcasted_iota(jnp.int32, (span, 1), 0)).astype(F32)
    fade_ref[...] = jnp.exp(to_end * rate)
    rows_ref[0:1] = jnp.exp(rate * (span * (n_sp - 1 - sp)).astype(F32))
    rows_ref[1:2] = jnp.exp(rate)

    for copy in weight_loads:
        copy.wait()

    def add(p, s, fresh_total):
        block = x[p, s]
        where = pl.ds(pl.multiple_of(p * feat, feat), feat)
        part_k = jnp.dot(block, wk[where, :], preferred_element_type=F32)
        part_v = jnp.dot(block, wv[where, :], preferred_element_type=F32)
        if fresh_total:
            acc_k[s] = part_k
            acc_v[s] = part_v
        else:
            acc_k[s] += part_k
            acc_v[s] += part_v

    @pl.loop(0, pieces)
    def _(s):
        add(tp, s, True)
        x_arrived(partner, s)
        add(partner, s, False)

    n_arrived(partner)

    def project_new():
        def piece(p, totals):
            where = pl.ds(pl.multiple_of(p * feat, feat), feat)
            block = jnp.concatenate(
                [nx[p].astype(F32), jnp.zeros((NEW_ROWS - seqs, feat), F32)], axis=0
            ).astype(BF16)
            return tuple(
                t + jnp.dot(block, w[where, :], preferred_element_type=F32)
                for t, w in zip(totals, (wk, wv, wq))
            )

        zero = jnp.zeros((NEW_ROWS, inner), F32)
        new_k, new_v, new_q = lax.fori_loop(0, n_tp, piece, (zero, zero, zero))
        keys, queries = [], []
        for j in range(inner // LANES):
            at = slice(j * LANES, (j + 1) * LANES)
            keys.append((rotated(new_k[:, at], new_cos, new_sin) * HD**-0.5).astype(BF16))
            queries.append(rotated(new_q[:, at], new_cos, new_sin).astype(BF16))
        key = jnp.concatenate(keys, axis=1).astype(F32)
        query = jnp.concatenate(queries, axis=1).astype(F32)
        value = new_v.astype(BF16).astype(F32)
        same = (
            lax.broadcasted_iota(jnp.int32, (inner, inner), 0) // HD
            == lax.broadcasted_iota(jnp.int32, (inner, inner), 1) // HD
        )
        product = query * key
        for h in range(heads):
            at = slice(h * HD, (h + 1) * HD)
            own_term[:, at] = jnp.sum(product[:, at], axis=-1, keepdims=True) * value[:, at]
        pick = lax.broadcasted_iota(jnp.int32, (HD, inner), 0) == lane_iota((HD, inner)) % HD
        for s in range(seqs):
            spread = jnp.where(pick, query[s : s + 1], 0.0).astype(BF16)
            q_spread[s] = jnp.dot(
                spread, jnp.where(same, 1.0, 0.0).astype(BF16), preferred_element_type=F32
            )

    def rs_copy(s, o):
        peer = lax.rem(sp + o, n_sp)
        return pltpu.make_async_remote_copy(
            stage.at[s, peer], landed.at[s, sp], rs_tx.at[s, peer], rs_rx.at[s, sp],
            device_id={"sp": peer}, device_id_type=MESH,
        )

    def finish(i):
        s, part = i // parts, i % parts
        where = pl.ds(pl.multiple_of(part * size, size), size)
        cosine, sine = cos_ref[where, :], sin_ref[where, :]
        lane = lane_iota((HD, LANES))
        for j in range(inner // LANES):
            at = slice(j * LANES, (j + 1) * LANES)
            key = (rotated(acc_k[i, :, at], cosine, sine) * HD**-0.5).astype(BF16)
            weighted = (key.astype(F32) * fade_ref[where, at]).astype(BF16)
            value = acc_v[i, :, at].astype(BF16)
            both = lax.dot_general(
                weighted, value, (((0,), (0,)), ((), ())), preferred_element_type=F32
            )
            state = jnp.where(lane < HD, both[:HD], both[HD:])
            sums[:, at] = jnp.where(part == 0, state, sums[:, at] + state)

        @pl.when(part == parts - 1)
        def _():
            scaled = sums[...] * rows_ref[0:1]
            read = jnp.sum(scaled * q_spread[s], axis=0, keepdims=True)
            for o in range(n_sp):
                stage[s, o, 0:keep] = scaled[o * keep : (o + 1) * keep]
                stage[s, o, keep : keep + 1] = read
            for o in range(1, n_sp):
                rs_copy(s, o).start()
            totals[s] = stage[s, sp]

    far = jnp.maximum(z, chips - 1 - z)

    def decode(i):
        d = i // (2 * pieces) + 1
        s = (i // 2) % pieces
        step = 2 * (i % 2) - 1
        c = z + step * d
        return d, s, step, c, (c >= 0) & (c < chips)

    def onward(step):
        nxt = z - step
        return nxt, (nxt >= 0) & (nxt < chips), (step + 1) // 2

    @pl.loop(0, 2 * pieces * (chips - 1))
    def _(i):
        d, s, step, c, valid = decode(i)
        nxt, pass_on, way = onward(step)

        @pl.when(valid)
        def _():
            @pl.when(s == 0)
            def _():
                n_arrived(2 * c + k)

                @pl.when(pass_on)
                def _():
                    n_copy(c, nfwd.at[way, c], 2 * nxt + k).start()

                n_copy(c, nshare.at[c], partner).start()

            x_arrived(2 * c + k, s)

            @pl.when(pass_on)
            def _():
                x_copy(c, s, fwd.at[way, c, s], 2 * nxt + k).start()

            x_copy(c, s, share.at[c, s], partner).start()
            add(2 * c + k, s, False)

            @pl.when(s == 0)
            def _():
                n_arrived(2 * c + 1 - k)

            x_arrived(2 * c + 1 - k, s)
            add(2 * c + 1 - k, s, False)

        last = (d == far) & (step == 1)

        @pl.when(last & (s == 0))
        def _():
            project_new()

        @pl.when(last)
        def _():
            finish(s)

    raws = []
    for s in range(seqs):
        for o in range(1, n_sp):
            src = lax.rem(sp + o, n_sp)
            pltpu.make_async_remote_copy(
                stage.at[s, src], landed.at[s, src], rs_tx.at[s, src], rs_rx.at[s, src],
                device_id={"sp": src}, device_id_type=MESH,
            ).wait_recv()
        total = None
        for j in range(n_sp):
            term = jnp.where(sp == j, totals[s], landed[s, j])
            total = term if total is None else total + term
        kept = total[0:keep].astype(BF16)
        for h in range(heads):
            state_out[s, h] = kept[:, h * HD : (h + 1) * HD]
        raws.append(total[keep : keep + 1] * rows_ref[1:2] + own_term[s : s + 1])
    raw = jnp.concatenate(raws, axis=0)
    for h in range(heads):
        at = slice(h * HD, (h + 1) * HD)
        head = raw[:, at]
        centered = head - jnp.mean(head, axis=-1, keepdims=True)
        spread = jnp.mean(centered * centered, axis=-1, keepdims=True)
        read_out[:, at] = (centered * lax.rsqrt(spread + 1e-05)).astype(BF16)

    @pl.when(z < chips - 1)
    def _():
        n_up.wait_send()

    @pl.when(z > 0)
    def _():
        n_down.wait_send()

    n_side.wait_send()
    for s in range(seqs):
        for o in range(1, n_sp):
            rs_copy(s, o).wait_send()
    for s in range(pieces):
        @pl.when(z < chips - 1)
        def _(s=s):
            x_copy(z, s, fwd.at[0, z, s], tp + 2).wait_send()

        @pl.when(z > 0)
        def _(s=s):
            x_copy(z, s, fwd.at[1, z, s], tp - 2).wait_send()

        x_copy(z, s, share.at[z, s], partner).wait_send()

    @pl.loop(0, 2 * pieces * (chips - 1))
    def _(i):
        d, s, step, c, valid = decode(i)
        nxt, pass_on, way = onward(step)

        @pl.when(valid)
        def _():
            @pl.when(s == 0)
            def _():
                @pl.when(pass_on)
                def _():
                    n_copy(c, nfwd.at[way, c], 2 * nxt + k).wait_send()

                n_copy(c, nshare.at[c], partner).wait_send()

            @pl.when(pass_on)
            def _():
                x_copy(c, s, fwd.at[way, c, s], 2 * nxt + k).wait_send()

            x_copy(c, s, share.at[c, s], partner).wait_send()


def one_of(n, values):
    total = 0
    for k, value in enumerate(values):
        if value:
            total = total + (n == k).astype(jnp.int32) * value
    return total


def middle_order(main, moved):
    near = [(0, i) for i in main]
    far = [(2, i) for i in moved + main]
    order = [(kind, i) for i in moved for kind in (0, 1)]
    order += [(1, i) for i in main]
    for at in range(max(len(near), len(far))):
        order += near[at : at + 1] + far[at : at + 1]
    return order


def moved_kernel(
    n_sp, n_tp, parts,
    tokens, fresh, wq_hbm, wk_hbm, wv_hbm, inverse_ref, decay_ref,
    state_out, read_out,
    x, xc, nx, wq, wk, wv, we, acc_k, acc_v, acc_c, cos_ref, sin_ref, fade_ref, rows_ref,
    q_spread, own_term, sums, stage, landed, totals, hint, hint_in, stage_c, landed_c,
    load_sem, weight_sem, rx, rn, ry, rw, fwd, share, nsend, ysend, yshare, wsend, wxsend,
    hint_sem, rs_tx, rs_rx, c_tx, c_rx,
):
    seqs, span, feat = tokens.shape
    inner = wk.shape[1]
    heads = inner // HD
    half = inner // 2
    chunks = half // LANES
    chips = n_tp // 2
    pieces = seqs * parts
    size = span // parts
    keep = HD // n_sp
    groups = n_tp // 2
    moved_seq = seqs - 1
    main = list(range(moved_seq * parts))
    moved = list(range(moved_seq * parts, pieces))
    sp = lax.axis_index("sp")
    tp = lax.axis_index("tp")
    z, k = tp // 2, tp % 2
    row_y, row_x = sp // 2, sp % 2
    x_peer = sp + 1 - 2 * row_x
    y_peer = sp + 2 - 4 * row_y
    MESH = pl.DeviceIdType.MESH
    end_int = (z == 0).astype(jnp.int32) + (z == chips - 1).astype(jnp.int32)
    end = end_int > 0
    mid = end_int == 0
    partner = z * 2 + 1 - k
    mate = z + 1 - 2 * (z % 2)
    mate_tp = 2 * mate + k
    other = chips - 1 - z
    other_tp = 2 * other + k
    second = end_int * (chips - 1 - mate) + (1 - end_int) * (chips - 1 - z)
    third = end_int * (chips - 1 - z) + (1 - end_int) * (chips - 1 - mate)

    own_loads = {
        s: pltpu.make_async_copy(
            tokens.at[s // parts, pl.ds(s % parts * size, size)], x.at[tp, s], load_sem.at[s]
        )
        for s in range(pieces)
    }
    new_load = pltpu.make_async_copy(fresh, nx.at[tp], load_sem.at[pieces])
    new_load.start()
    for s in moved + main:
        own_loads[s].start()
    weight_loads = [
        pltpu.make_async_copy(a, b, weight_sem.at[i])
        for i, (a, b) in enumerate(((wk_hbm, wk), (wv_hbm, wv), (wq_hbm, wq)))
    ]

    barrier = pltpu.get_barrier_semaphore()
    for o in range(1, n_tp):
        pl.semaphore_signal(
            barrier, inc=1, device_id={"tp": lax.rem(tp + o, n_tp)}, device_id_type=MESH
        )
    for o in range(1, n_sp):
        pl.semaphore_signal(
            barrier, inc=1, device_id={"sp": lax.rem(sp + o, n_sp)}, device_id_type=MESH
        )
        pl.semaphore_signal(
            barrier, inc=1, device_id={"sp": lax.rem(sp + o, n_sp), "tp": mate_tp},
            device_id_type=MESH,
        )
    pl.semaphore_wait(barrier, n_tp - 1 + 2 * (n_sp - 1))

    def x_copy(c, s, sem, target):
        p = 2 * c + k
        return pltpu.make_async_remote_copy(
            x.at[p, s], x.at[p, s], sem, rx.at[p, s],
            device_id={"tp": target}, device_id_type=MESH,
        )

    def to_mate(c, s):
        return x_copy(c, s, fwd.at[0, c, s], mate_tp)

    def to_other(c, s):
        return x_copy(c, s, fwd.at[1, c, s], other_tp)

    def to_partner(c, s):
        return x_copy(c, s, share.at[c, s], partner)

    def x_arrived(p, s):
        pltpu.make_async_remote_copy(
            x.at[p, s], x.at[p, s], share.at[0, 0], rx.at[p, s],
            device_id={"tp": partner}, device_id_type=MESH,
        ).wait_recv()

    def y_send(c, j):
        p = 2 * c + k
        return pltpu.make_async_remote_copy(
            x.at[p, moved[0] + j], xc.at[p, j], ysend.at[c, j], ry.at[p, j],
            device_id={"sp": y_peer}, device_id_type=MESH,
        )

    def y_share(c, j):
        p = 2 * c + k
        return pltpu.make_async_remote_copy(
            xc.at[p, j], xc.at[p, j], yshare.at[c, j], ry.at[p, j],
            device_id={"tp": partner}, device_id_type=MESH,
        )

    def y_arrived(p, j):
        pltpu.make_async_remote_copy(
            xc.at[p, j], xc.at[p, j], yshare.at[0, 0], ry.at[p, j],
            device_id={"tp": partner}, device_id_type=MESH,
        ).wait_recv()

    def w_rows(p):
        return pl.ds(pl.multiple_of(p * feat, feat), feat)

    def w_cols(cc):
        return pl.ds(pl.multiple_of(row_y * half + cc * LANES, LANES), LANES)

    def w_send(cc, g, kv):
        p = row_x * groups + g
        return pltpu.make_async_remote_copy(
            (wk, wv)[kv].at[w_rows(p), w_cols(cc)],
            we.at[cc, w_rows(p), pl.ds(kv * LANES, LANES)],
            wsend.at[cc, g, kv], rw.at[cc, p, kv],
            device_id={"tp": mate_tp}, device_id_type=MESH,
        )

    def w_pass(cc, g, kv):
        p = row_x * groups + g
        where = we.at[cc, w_rows(p), pl.ds(kv * LANES, LANES)]
        return pltpu.make_async_remote_copy(
            where, where, wxsend.at[cc, g, kv], rw.at[cc, p, kv],
            device_id={"sp": x_peer}, device_id_type=MESH,
        )

    def w_arrived(cc, p, kv):
        where = we.at[cc, w_rows(p), pl.ds(kv * LANES, LANES)]
        pltpu.make_async_remote_copy(
            where, where, wxsend.at[cc, 0, kv], rw.at[cc, p, kv],
            device_id={"sp": x_peer}, device_id_type=MESH,
        ).wait_recv()

    def n_copy(o):
        return pltpu.make_async_remote_copy(
            nx.at[tp], nx.at[tp], nsend.at[o], rn.at[tp],
            device_id={"tp": lax.rem(tp + o, n_tp)}, device_id_type=MESH,
        )

    def n_arrived(o):
        p = lax.rem(tp + o, n_tp)
        pltpu.make_async_remote_copy(
            nx.at[p], nx.at[p], nsend.at[0], rn.at[p],
            device_id={"tp": p}, device_id_type=MESH,
        ).wait_recv()

    hint_copy = pltpu.make_async_remote_copy(
        hint, hint_in, hint_sem.at[0], hint_sem.at[1],
        device_id={"tp": mate_tp}, device_id_type=MESH,
    )

    new_load.wait()
    for o in range(1, n_tp):
        n_copy(o).start()
    for j, s in enumerate(moved):
        own_loads[s].wait()

        @pl.when(mid)
        def _(j=j, s=s):
            to_other(z, s).start()
            y_send(z, j).start()
            to_partner(z, s).start()

        @pl.when(end)
        def _(s=s):
            to_mate(z, s).start()

    for s in main:
        own_loads[s].wait()
        to_partner(z, s).start()

        @pl.when(mid)
        def _(s=s):
            to_mate(z, s).start()
            to_other(z, s).start()

    for copy in weight_loads:
        copy.start()

    row = lax.broadcasted_iota(jnp.int32, (span, LANES), 0)
    within = lane_iota((1, LANES)) % HD
    first_half = jnp.where(within < HD // 2, -1.0, 1.0).astype(F32)
    inverse = inverse_ref[...]

    def tables(slot, column):
        angles = (column * span + row).astype(F32) * inverse
        cos_ref[slot] = jnp.cos(angles)
        sin_ref[slot] = jnp.sin(angles) * first_half

    for copy in weight_loads[:2]:
        copy.wait()

    @pl.when(end)
    def _():
        for g in range(groups):
            for kv in range(2):
                w_send(0, g, kv).start()

    tables(0, sp)

    @pl.when(mid)
    def _():
        tables(1, y_peer)

    new_angles = jnp.full((NEW_ROWS, LANES), n_sp * span, F32) * inverse
    new_cos = jnp.cos(new_angles)
    new_sin = jnp.sin(new_angles) * first_half
    head_of = lane_iota((1, inner)) // HD
    rate = jnp.zeros((1, inner), F32)
    for h in range(heads):
        rate = jnp.where(head_of == h, decay_ref[h], rate)
    to_end = (span - 1 - lax.broadcasted_iota(jnp.int32, (span, 1), 0)).astype(F32)
    fade_ref[...] = jnp.exp(to_end * rate)
    rows_ref[0:1] = jnp.exp(rate * (span * (n_sp - 1 - sp)).astype(F32))
    rows_ref[1:2] = jnp.exp(rate)
    hint[...] = jnp.zeros(hint.shape, F32)
    hint[1:2] = rate
    weight_loads[2].wait()

    def add(p, s, fresh_total):
        block = x[p, s]
        where = w_rows(p)
        part_k = jnp.dot(block, wk[where, :], preferred_element_type=F32)
        part_v = jnp.dot(block, wv[where, :], preferred_element_type=F32)
        if fresh_total:
            acc_k[s] = part_k
            acc_v[s] = part_v
        else:
            acc_k[s] += part_k
            acc_v[s] += part_v

    same = (
        lax.broadcasted_iota(jnp.int32, (inner, inner), 0) // HD
        == lax.broadcasted_iota(jnp.int32, (inner, inner), 1) // HD
    )
    pick = lax.broadcasted_iota(jnp.int32, (HD, inner), 0) == lane_iota((HD, inner)) % HD
    own_pieces = end_int * len(main) + (1 - end_int) * pieces

    @pl.loop(0, pieces)
    def _(i):
        s = lax.rem(i + (1 - end_int) * len(main), pieces)

        @pl.when(i < own_pieces)
        def _():
            add(tp, s, True)

        @pl.when(i < own_pieces)
        def _():
            x_arrived(partner, s)
            add(partner, s, False)

    for o in range(1, n_tp):
        n_arrived(o)

    def project_new():
        def piece(p, totals):
            where = w_rows(p)
            block = jnp.concatenate(
                [nx[p].astype(F32), jnp.zeros((NEW_ROWS - seqs, feat), F32)], axis=0
            ).astype(BF16)
            return tuple(
                t + jnp.dot(block, w[where, :], preferred_element_type=F32)
                for t, w in zip(totals, (wk, wv, wq))
            )

        zero = jnp.zeros((NEW_ROWS, inner), F32)
        new_k, new_v, new_q = lax.fori_loop(0, n_tp, piece, (zero, zero, zero))
        keys, queries = [], []
        for j in range(inner // LANES):
            at = slice(j * LANES, (j + 1) * LANES)
            keys.append((rotated(new_k[:, at], new_cos, new_sin) * HD**-0.5).astype(BF16))
            queries.append(rotated(new_q[:, at], new_cos, new_sin).astype(BF16))
        key = jnp.concatenate(keys, axis=1).astype(F32)
        query = jnp.concatenate(queries, axis=1).astype(F32)
        value = new_v.astype(BF16).astype(F32)
        product = query * key
        for h in range(heads):
            at = slice(h * HD, (h + 1) * HD)
            own_term[:, at] = jnp.sum(product[:, at], axis=-1, keepdims=True) * value[:, at]
        hint[0:1] = query[moved_seq : moved_seq + 1]
        for s in range(seqs):
            spread = jnp.where(pick, query[s : s + 1], 0.0).astype(BF16)
            q_spread[s] = jnp.dot(
                spread, jnp.where(same, 1.0, 0.0).astype(BF16), preferred_element_type=F32
            )

    project_new()

    @pl.when(end)
    def _():
        hint_copy.start()
        for s in main:
            to_mate(z, s).start()
        for cc in range(1, chunks):
            for g in range(groups):
                for kv in range(2):
                    w_send(cc, g, kv).start()

    def rs_copy(s, o):
        peer = lax.rem(sp + o, n_sp)
        return pltpu.make_async_remote_copy(
            stage.at[s, peer], landed.at[s, sp], rs_tx.at[s, peer], rs_rx.at[s, sp],
            device_id={"sp": peer}, device_id_type=MESH,
        )

    def outer(weighted, value):
        both = lax.dot_general(
            weighted, value, (((0,), (0,)), ((), ())), preferred_element_type=F32
        )
        return jnp.where(lane_iota((HD, LANES)) < HD, both[:HD], both[HD:])

    def finish(i):
        s, part = i // parts, i % parts
        where = pl.ds(pl.multiple_of(part * size, size), size)
        cosine, sine = cos_ref[0, where, :], sin_ref[0, where, :]
        for j in range(inner // LANES):
            at = slice(j * LANES, (j + 1) * LANES)
            key = (rotated(acc_k[i, :, at], cosine, sine) * HD**-0.5).astype(BF16)
            weighted = (key.astype(F32) * fade_ref[where, at]).astype(BF16)
            value = acc_v[i, :, at].astype(BF16)
            state = outer(weighted, value)
            sums[:, at] = jnp.where(part == 0, state, sums[:, at] + state)

        @pl.when(part == parts - 1)
        def _():
            scaled = sums[...] * rows_ref[0:1]
            read = jnp.sum(scaled * q_spread[s], axis=0, keepdims=True)
            for o in range(n_sp):
                stage[s, o, 0:keep] = scaled[o * keep : (o + 1) * keep]
                stage[s, o, keep : keep + 1] = read
            totals[s] = stage[s, sp]

            @pl.when(end | (s == moved_seq))
            def _():
                for o in range(1, n_sp):
                    rs_copy(s, o).start()

    def c_add(cc, p, fresh_total):
        where = w_rows(p)
        for t in range(parts):
            for side, block in ((0, x[p, moved[0] + t]), (1, xc[p, t])):
                both = jnp.dot(block, we[cc, where, :], preferred_element_type=F32)
                if fresh_total:
                    acc_c[side, t] = both
                else:
                    acc_c[side, t] += both

    def c_copy(cc, o):
        return pltpu.make_async_remote_copy(
            stage_c.at[cc, o], landed_c.at[cc, sp], c_tx.at[cc, o], c_rx.at[cc, sp],
            device_id={"sp": o, "tp": mate_tp}, device_id_type=MESH,
        )

    def c_finish(cc):
        pair_rate = hint_in[1:2, w_cols(cc)]
        query = hint_in[0:1, w_cols(cc)]
        total = jnp.zeros((HD, LANES), F32)
        for side, column in ((0, sp), (1, y_peer)):
            state = jnp.zeros((HD, LANES), F32)
            for t in range(parts):
                at = slice(t * size, (t + 1) * size)
                key = (
                    rotated(acc_c[side, t, :, :LANES], cos_ref[side, at], sin_ref[side, at])
                    * HD**-0.5
                ).astype(BF16)
                fade = jnp.exp(to_end[at] * pair_rate)
                weighted = (key.astype(F32) * fade).astype(BF16)
                state = state + outer(weighted, acc_c[side, t, :, LANES:].astype(BF16))
            total = total + state * jnp.exp(
                pair_rate * (span * (n_sp - 1 - column)).astype(F32)
            )
        spread = jnp.where(pick[:, :LANES], query, 0.0).astype(BF16)
        spread = jnp.dot(
            spread, jnp.where(same[:LANES, :LANES], 1.0, 0.0).astype(BF16),
            preferred_element_type=F32,
        )
        read = jnp.sum(total * spread, axis=0, keepdims=True)
        for o in range(n_sp):
            stage_c[cc, o, 0:keep] = total[o * keep : (o + 1) * keep]
            stage_c[cc, o, keep : keep + 1] = read
        for o in range(n_sp):
            c_copy(cc, o).start()

    order = middle_order(main, moved)
    steps = end_int * (len(main) * (chips - 1)) + (1 - end_int) * len(order)

    def decode(n):
        kind = end_int * (n // len(main)) + (1 - end_int) * one_of(n, [o[0] for o in order])
        s = end_int * (n % len(main)) + (1 - end_int) * one_of(n, [o[1] for o in order])
        c = (
            (kind == 0).astype(jnp.int32) * mate
            + (kind == 1).astype(jnp.int32) * second
            + (kind == 2).astype(jnp.int32) * third
        )
        return kind, c, s

    first_w = 2 * len(moved) + 1
    c_at = len(order) - 3

    def w_relay(cc, g, kv):
        w_arrived(cc, row_x * groups + g, kv)
        w_pass(cc, g, kv).start()

    def w_own(cc, g, fresh_total=False):
        c_add(cc, row_x * groups + g, fresh_total)

    def w_peer(cc, g):
        for kv in range(2):
            w_arrived(cc, (1 - row_x) * groups + g, kv)
        c_add(cc, (1 - row_x) * groups + g, False)

    def y_pass(c, j):
        y_arrived(2 * c + k, j)
        y_share(c, j).start()

    @pl.loop(0, len(order) + 1)
    def _(n):
        kind, c, s = decode(n)
        is_moved = s >= moved[0]

        @pl.when(mid & (n == len(order) - 2))
        def _():
            w_relay(1, 0, 1)

        @pl.when(mid & (n == len(order) - 1))
        def _():
            w_relay(1, 1, 0)

        @pl.when(n < steps)
        def _():
            x_arrived(2 * c + k, s)

            @pl.when(mid & (kind == 0))
            def _():
                to_other(c, s).start()

            @pl.when(mid & (kind > 0) & (s < moved[0]))
            def _():
                to_mate(c, s).start()

            @pl.when(mid & is_moved)
            def _():
                y_send(c, s - moved[0]).start()

            to_partner(c, s).start()

        @pl.when(mid & (n == len(order) - 1))
        def _():
            w_relay(1, 1, 1)

        @pl.when(mid & (n >= first_w) & (n < first_w + groups))
        def _():
            for kv in range(2):
                w_relay(0, n - first_w, kv)

        @pl.when(mid & (n >= 3) & (n < 3 + parts))
        def _():
            y_pass(z, n - 3)

        @pl.when(mid & (n >= 6) & (n < 6 + 2 * parts))
        def _():
            m = n - 6
            y_pass((m % 2) * second + (1 - m % 2) * mate, m // 2)

        @pl.when(mid & (n >= c_at - parts) & (n < c_at))
        def _():
            y_pass(third, n - (c_at - parts))

        @pl.when(n < steps)
        def _():
            add(2 * c + k, s, False)

        kind_b, c_b, s_b = decode(n - 1)

        @pl.when((n >= 1) & (n <= steps))
        def _():
            x_arrived(2 * c_b + 1 - k, s_b)
            add(2 * c_b + 1 - k, s_b, False)

            @pl.when(kind_b == 2)
            def _():
                finish(s_b)

        early = n - (c_at - 5)

        @pl.when(mid & (early == 0))
        def _():
            for cx in (z, mate, second):
                for j in range(parts):
                    y_arrived(2 * cx + 1 - k, j)
            for g in range(groups):
                for kv in range(2):
                    w_arrived(0, (1 - row_x) * groups + g, kv)
            acc_c[...] = jnp.zeros(acc_c.shape, F32)

        @pl.when(mid & (early >= 0) & (early < 6))
        def _():
            turn = early // 2
            cx = (
                (turn == 0).astype(jnp.int32) * z
                + (turn == 1).astype(jnp.int32) * mate
                + (turn == 2).astype(jnp.int32) * second
            )
            c_add(0, 2 * cx + early % 2, False)

        @pl.when(mid & (n == c_at))
        def _():
            for j in range(parts):
                y_arrived(2 * third + 1 - k, j)

            @pl.loop(0, 2)
            def _(m):
                c_add(0, 2 * third + m, False)

            w_relay(1, 0, 0)

            hint_copy.wait_recv()
            c_finish(0)

    @pl.when(mid)
    def _():
        w_relay(1, 2, 0)
        w_own(1, 0, True)
        w_peer(1, 0)
        w_own(1, 1)
        w_relay(1, 2, 1)
        w_peer(1, 1)
        w_own(1, 2)
        w_relay(1, 3, 0)
        w_relay(1, 3, 1)
        w_peer(1, 2)
        for s in range(moved_seq):
            for o in range(1, n_sp):
                rs_copy(s, o).start()
        w_own(1, 3)
        w_peer(1, 3)
        c_finish(1)

    def gather(s):
        for o in range(1, n_sp):
            src = lax.rem(sp + o, n_sp)
            pltpu.make_async_remote_copy(
                stage.at[s, src], landed.at[s, src], rs_tx.at[s, src], rs_rx.at[s, src],
                device_id={"sp": src}, device_id_type=MESH,
            ).wait_recv()
        total = None
        for j in range(n_sp):
            term = jnp.where(sp == j, totals[s], landed[s, j])
            total = term if total is None else total + term
        totals[s] = total

    for o in range(1, n_tp):
        n_copy(o).wait_send()
    for s in main:
        to_partner(z, s).wait_send()
        to_mate(z, s).wait_send()
        for o in range(1, n_sp):
            if s % parts == 0:
                rs_copy(s // parts, o).wait_send()

    @pl.when(end)
    def _():
        hint_copy.wait_send()
        for s in moved:
            to_mate(z, s).wait_send()
        for cc in range(chunks):
            for g in range(groups):
                for kv in range(2):
                    w_send(cc, g, kv).wait_send()

    @pl.when(mid)
    def _():
        for j, s in enumerate(moved):
            to_other(z, s).wait_send()
            to_partner(z, s).wait_send()
        for s in main:
            to_other(z, s).wait_send()
        for cx in range(chips):
            for j in range(parts):
                y_send(cx, j).wait_send()
                y_share(cx, j).wait_send()
        for o in range(1, n_sp):
            rs_copy(moved_seq, o).wait_send()
        for cc in range(chunks):
            for g in range(groups):
                for kv in range(2):
                    w_pass(cc, g, kv).wait_send()

    @pl.loop(0, len(order))
    def _(n):
        kind, c, s = decode(n)

        @pl.when(n < steps)
        def _():
            @pl.when(mid & (kind == 0))
            def _():
                to_other(c, s).wait_send()

            @pl.when(mid & (kind > 0) & (s < moved[0]))
            def _():
                to_mate(c, s).wait_send()

            to_partner(c, s).wait_send()

    for s in range(moved_seq):
        gather(s)

    @pl.when(mid)
    def _():
        gather(moved_seq)

    @pl.when(end)
    def _():
        for cc in range(chunks):
            for o in range(n_sp):
                pltpu.make_async_remote_copy(
                    stage_c.at[cc, o], landed_c.at[cc, o], c_tx.at[cc, o], c_rx.at[cc, o],
                    device_id={"sp": o, "tp": mate_tp}, device_id_type=MESH,
                ).wait_recv()
            for side in range(2):
                at = slice(side * half + cc * LANES, side * half + (cc + 1) * LANES)
                totals[moved_seq, :, at] = landed_c[cc, 2 * side] + landed_c[cc, 2 * side + 1]

    raws = []
    for s in range(seqs):
        total = totals[s]
        kept = total[0:keep].astype(BF16)
        for h in range(heads):
            state_out[s, h] = kept[:, h * HD : (h + 1) * HD]
        raws.append(total[keep : keep + 1] * rows_ref[1:2] + own_term[s : s + 1])
    raw = jnp.concatenate(raws, axis=0)
    for h in range(heads):
        at = slice(h * HD, (h + 1) * HD)
        head = raw[:, at]
        centered = head - jnp.mean(head, axis=-1, keepdims=True)
        spread = jnp.mean(centered * centered, axis=-1, keepdims=True)
        read_out[:, at] = (centered * lax.rsqrt(spread + 1e-05)).astype(BF16)

    @pl.when(mid)
    def _():
        for cc in range(chunks):
            for o in range(n_sp):
                c_copy(cc, o).wait_send()


def solution(mesh):
    n_sp, n_tp = mesh.shape["sp"], mesh.shape["tp"]

    def body(tokens, new_token, query_weight, key_weight, value_weight, log_decay):
        seqs, span, feat = tokens.shape
        width, inner = key_weight.shape
        heads = inner // HD
        keep = HD // n_sp
        rows = -(-(keep + 1) // 8) * 8
        chips = n_tp // 2
        half = HD // 2
        parts = max(1, 8 // chips)
        pieces = seqs * parts
        size = span // parts
        inverse = np.float32(10000.0) ** (-np.arange(half, dtype=np.float32) / half)
        inverse = jnp.asarray(np.tile(inverse.astype(np.float32), LANES // half)[None])
        anywhere = pl.BlockSpec(memory_space=pl.ANY)
        vmem = pl.BlockSpec(memory_space=pltpu.VMEM)
        dma = pltpu.SemaphoreType.DMA
        moves = chips == 4 and n_sp == 4 and seqs > 1 and inner == 4 * LANES
        tokens_in = [
            pltpu.VMEM((n_tp, pieces, size, feat), BF16),
            pltpu.VMEM((n_tp, seqs, feat), BF16),
        ]
        weights_in = [pltpu.VMEM((width, inner), BF16)] * 3
        totals = [pltpu.VMEM((pieces, size, inner), F32)] * 2
        ends = [
            pltpu.VMEM((8, inner), F32),
            pltpu.VMEM((seqs, HD, inner), F32),
            pltpu.VMEM((NEW_ROWS, inner), F32),
            pltpu.VMEM((HD, inner), F32),
            pltpu.VMEM((seqs, n_sp, rows, inner), F32),
            pltpu.VMEM((seqs, n_sp, rows, inner), F32),
            pltpu.VMEM((seqs, rows, inner), F32),
        ]
        if moves:
            chunks = inner // 2 // LANES
            groups = n_tp // 2
            call = moved_kernel
            scratch = (
                tokens_in[:1]
                + [pltpu.VMEM((n_tp, parts, size, feat), BF16)]
                + tokens_in[1:]
                + weights_in
                + [pltpu.VMEM((chunks, width, 2 * LANES), BF16)]
                + totals
                + [
                    pltpu.VMEM((2, parts, size, 2 * LANES), F32),
                    pltpu.VMEM((2, span, LANES), F32),
                    pltpu.VMEM((2, span, LANES), F32),
                    pltpu.VMEM((span, inner), F32),
                ]
                + ends
                + [
                    pltpu.VMEM((8, inner), F32),
                    pltpu.VMEM((8, inner), F32),
                    pltpu.VMEM((chunks, n_sp, rows, LANES), F32),
                    pltpu.VMEM((chunks, n_sp, rows, LANES), F32),
                    dma((pieces + 1,)),
                    dma((3,)),
                    dma((n_tp, pieces)),
                    dma((n_tp,)),
                    dma((n_tp, parts)),
                    dma((chunks, n_tp, 2)),
                    dma((2, chips, pieces)),
                    dma((chips, pieces)),
                    dma((n_tp,)),
                    dma((chips, parts)),
                    dma((chips, parts)),
                    dma((chunks, groups, 2)),
                    dma((chunks, groups, 2)),
                    dma((2,)),
                    dma((seqs, n_sp)),
                    dma((seqs, n_sp)),
                    dma((chunks, n_sp)),
                    dma((chunks, n_sp)),
                ]
            )
        else:
            call = kernel
            scratch = (
                tokens_in
                + weights_in
                + totals
                + [
                    pltpu.VMEM((span, LANES), F32),
                    pltpu.VMEM((span, LANES), F32),
                    pltpu.VMEM((span, inner), F32),
                ]
                + ends
                + [
                    dma((pieces + 1,)),
                    dma((3,)),
                    dma((n_tp, pieces)),
                    dma((n_tp,)),
                    dma((2, chips, pieces)),
                    dma((chips, pieces)),
                    dma((2, chips)),
                    dma((chips,)),
                    dma((seqs, n_sp)),
                    dma((seqs, n_sp)),
                ]
            )
        return pl.pallas_call(
            functools.partial(call, n_sp, n_tp, parts),
            out_shape=(
                jax.ShapeDtypeStruct((seqs, heads, keep, HD), BF16),
                jax.ShapeDtypeStruct((seqs, inner), BF16),
            ),
            in_specs=[anywhere] * 5 + [vmem, pl.BlockSpec(memory_space=pltpu.SMEM)],
            out_specs=(vmem, vmem),
            scratch_shapes=scratch,
            compiler_params=pltpu.CompilerParams(
                collective_id=0, has_side_effects=True, vmem_limit_bytes=60 * 1024 * 1024
            ),
            name="retention",
        )(tokens, new_token.reshape(seqs, feat), query_weight, key_weight, value_weight, inverse, log_decay)

    return jax.shard_map(
        body,
        mesh=mesh,
        in_specs=(
            P(None, "sp", "tp"),
            P(None, None, "tp"),
            P(None, "tp"),
            P(None, "tp"),
            P(None, "tp"),
            P("tp"),
        ),
        out_specs=(P(None, "tp", "sp", None), P(None, "tp")),
        check_vma=False,
    )
```

```python
import functools

import jax
import jax.numpy as jnp
import numpy as np
from jax import lax
from jax.experimental import pallas as pl
from jax.experimental.pallas import tpu as pltpu
from jax.sharding import PartitionSpec as P

HD = 64
LANES = 128
NEW_ROWS = 8
F32 = jnp.float32
BF16 = jnp.bfloat16


def lane_iota(shape):
    return lax.broadcasted_iota(jnp.int32, shape, len(shape) - 1)


def rotated(block, cosine, sine):
    half = HD // 2
    low = lane_iota(block.shape) % HD < half
    swapped = jnp.where(
        low, pltpu.roll(block, LANES - half, 1), pltpu.roll(block, half, 1)
    )
    return block * cosine + swapped * sine


def kernel(
    n_sp, n_tp, parts,
    tokens, fresh, wq_hbm, wk_hbm, wv_hbm, inverse_ref, decay_ref,
    state_out, read_out,
    x, nx, wq, wk, wv, acc_k, acc_v, cos_ref, sin_ref, fade_ref, rows_ref,
    q_spread, own_term, sums, stage, landed, totals,
    load_sem, weight_sem, rx, rn, fwd, share, nfwd, nshare, rs_tx, rs_rx,
):
    seqs, span, feat = tokens.shape
    inner = wk.shape[1]
    heads = inner // HD
    chips = n_tp // 2
    pieces = seqs * parts
    size = span // parts
    keep = HD // n_sp
    sp = lax.axis_index("sp")
    tp = lax.axis_index("tp")
    z, k = tp // 2, tp % 2
    MESH = pl.DeviceIdType.MESH

    def to_tp(index):
        return {"tp": index}

    partner = z * 2 + 1 - k
    own_loads = [
        pltpu.make_async_copy(
            tokens.at[s // parts, pl.ds(s % parts * size, size)], x.at[tp, s], load_sem.at[s]
        )
        for s in range(pieces)
    ]
    new_load = pltpu.make_async_copy(fresh, nx.at[tp], load_sem.at[pieces])
    new_load.start()
    for copy in own_loads:
        copy.start()
    weight_loads = [
        pltpu.make_async_copy(a, b, weight_sem.at[i])
        for i, (a, b) in enumerate(((wk_hbm, wk), (wv_hbm, wv), (wq_hbm, wq)))
    ]

    barrier = pltpu.get_barrier_semaphore()

    @pl.when(z > 0)
    def _():
        pl.semaphore_signal(barrier, inc=1, device_id=to_tp(tp - 2), device_id_type=MESH)

    @pl.when(z < chips - 1)
    def _():
        pl.semaphore_signal(barrier, inc=1, device_id=to_tp(tp + 2), device_id_type=MESH)

    pl.semaphore_signal(barrier, inc=1, device_id=to_tp(partner), device_id_type=MESH)
    for o in range(1, n_sp):
        pl.semaphore_signal(
            barrier, inc=1, device_id={"sp": lax.rem(sp + o, n_sp)}, device_id_type=MESH
        )
    pl.semaphore_wait(
        barrier, n_sp + (z > 0).astype(jnp.int32) + (z < chips - 1).astype(jnp.int32)
    )

    def x_copy(c, s, sem, target):
        p = 2 * c + k
        return pltpu.make_async_remote_copy(
            x.at[p, s], x.at[p, s], sem, rx.at[p, s], device_id=to_tp(target), device_id_type=MESH
        )

    def n_copy(c, sem, target):
        p = 2 * c + k
        return pltpu.make_async_remote_copy(
            nx.at[p], nx.at[p], sem, rn.at[p], device_id=to_tp(target), device_id_type=MESH
        )

    def x_arrived(p, s):
        pltpu.make_async_remote_copy(
            x.at[p, s], x.at[p, s], share.at[0, 0], rx.at[p, s],
            device_id=to_tp(partner), device_id_type=MESH,
        ).wait_recv()

    def n_arrived(p):
        pltpu.make_async_remote_copy(
            nx.at[p], nx.at[p], nshare.at[0], rn.at[p],
            device_id=to_tp(partner), device_id_type=MESH,
        ).wait_recv()

    new_load.wait()
    n_up = n_copy(z, nfwd.at[0, z], tp + 2)
    n_down = n_copy(z, nfwd.at[1, z], tp - 2)
    n_side = n_copy(z, nshare.at[z], partner)

    @pl.when(z < chips - 1)
    def _():
        n_up.start()

    @pl.when(z > 0)
    def _():
        n_down.start()

    n_side.start()
    for s in range(pieces):
        own_loads[s].wait()

        @pl.when(z < chips - 1)
        def _(s=s):
            x_copy(z, s, fwd.at[0, z, s], tp + 2).start()

        @pl.when(z > 0)
        def _(s=s):
            x_copy(z, s, fwd.at[1, z, s], tp - 2).start()

        x_copy(z, s, share.at[z, s], partner).start()

    for copy in weight_loads:
        copy.start()

    row = lax.broadcasted_iota(jnp.int32, (span, LANES), 0)
    within = lane_iota((1, LANES)) % HD
    first_half = jnp.where(within < HD // 2, -1.0, 1.0).astype(F32)
    inverse = inverse_ref[...]
    angles = (sp * span + row).astype(F32) * inverse
    cos_ref[...] = jnp.cos(angles)
    sin_ref[...] = jnp.sin(angles) * first_half
    new_angles = jnp.full((NEW_ROWS, LANES), n_sp * span, F32) * inverse
    new_cos = jnp.cos(new_angles)
    new_sin = jnp.sin(new_angles) * first_half
    head_of = lane_iota((1, inner)) // HD
    rate = jnp.zeros((1, inner), F32)
    for h in range(heads):
        rate = jnp.where(head_of == h, decay_ref[h], rate)
    to_end = (span - 1 - lax.broadcasted_iota(jnp.int32, (span, 1), 0)).astype(F32)
    fade_ref[...] = jnp.exp(to_end * rate)
    rows_ref[0:1] = jnp.exp(rate * (span * (n_sp - 1 - sp)).astype(F32))
    rows_ref[1:2] = jnp.exp(rate)

    for copy in weight_loads:
        copy.wait()

    def add(p, s, fresh_total):
        block = x[p, s]
        where = pl.ds(pl.multiple_of(p * feat, feat), feat)
        part_k = jnp.dot(block, wk[where, :], preferred_element_type=F32)
        part_v = jnp.dot(block, wv[where, :], preferred_element_type=F32)
        if fresh_total:
            acc_k[s] = part_k
            acc_v[s] = part_v
        else:
            acc_k[s] += part_k
            acc_v[s] += part_v

    @pl.loop(0, pieces)
    def _(s):
        add(tp, s, True)
        x_arrived(partner, s)
        add(partner, s, False)

    n_arrived(partner)

    def project_new():
        def piece(p, totals):
            where = pl.ds(pl.multiple_of(p * feat, feat), feat)
            block = jnp.concatenate(
                [nx[p].astype(F32), jnp.zeros((NEW_ROWS - seqs, feat), F32)], axis=0
            ).astype(BF16)
            return tuple(
                t + jnp.dot(block, w[where, :], preferred_element_type=F32)
                for t, w in zip(totals, (wk, wv, wq))
            )

        zero = jnp.zeros((NEW_ROWS, inner), F32)
        new_k, new_v, new_q = lax.fori_loop(0, n_tp, piece, (zero, zero, zero))
        keys, queries = [], []
        for j in range(inner // LANES):
            at = slice(j * LANES, (j + 1) * LANES)
            keys.append((rotated(new_k[:, at], new_cos, new_sin) * HD**-0.5).astype(BF16))
            queries.append(rotated(new_q[:, at], new_cos, new_sin).astype(BF16))
        key = jnp.concatenate(keys, axis=1).astype(F32)
        query = jnp.concatenate(queries, axis=1).astype(F32)
        value = new_v.astype(BF16).astype(F32)
        same = (
            lax.broadcasted_iota(jnp.int32, (inner, inner), 0) // HD
            == lax.broadcasted_iota(jnp.int32, (inner, inner), 1) // HD
        )
        product = query * key
        for h in range(heads):
            at = slice(h * HD, (h + 1) * HD)
            own_term[:, at] = jnp.sum(product[:, at], axis=-1, keepdims=True) * value[:, at]
        pick = lax.broadcasted_iota(jnp.int32, (HD, inner), 0) == lane_iota((HD, inner)) % HD
        for s in range(seqs):
            spread = jnp.where(pick, query[s : s + 1], 0.0).astype(BF16)
            q_spread[s] = jnp.dot(
                spread, jnp.where(same, 1.0, 0.0).astype(BF16), preferred_element_type=F32
            )

    def rs_copy(s, o):
        peer = lax.rem(sp + o, n_sp)
        return pltpu.make_async_remote_copy(
            stage.at[s, peer], landed.at[s, sp], rs_tx.at[s, peer], rs_rx.at[s, sp],
            device_id={"sp": peer}, device_id_type=MESH,
        )

    def finish(i):
        s, part = i // parts, i % parts
        where = pl.ds(pl.multiple_of(part * size, size), size)
        cosine, sine = cos_ref[where, :], sin_ref[where, :]
        lane = lane_iota((HD, LANES))
        for j in range(inner // LANES):
            at = slice(j * LANES, (j + 1) * LANES)
            key = (rotated(acc_k[i, :, at], cosine, sine) * HD**-0.5).astype(BF16)
            weighted = (key.astype(F32) * fade_ref[where, at]).astype(BF16)
            value = acc_v[i, :, at].astype(BF16)
            both = lax.dot_general(
                weighted, value, (((0,), (0,)), ((), ())), preferred_element_type=F32
            )
            state = jnp.where(lane < HD, both[:HD], both[HD:])
            sums[:, at] = jnp.where(part == 0, state, sums[:, at] + state)

        @pl.when(part == parts - 1)
        def _():
            scaled = sums[...] * rows_ref[0:1]
            read = jnp.sum(scaled * q_spread[s], axis=0, keepdims=True)
            for o in range(n_sp):
                stage[s, o, 0:keep] = scaled[o * keep : (o + 1) * keep]
                stage[s, o, keep : keep + 1] = read
            for o in range(1, n_sp):
                rs_copy(s, o).start()
            totals[s] = stage[s, sp]

    far = jnp.maximum(z, chips - 1 - z)

    def decode(i):
        d = i // (2 * pieces) + 1
        s = (i // 2) % pieces
        step = 2 * (i % 2) - 1
        c = z + step * d
        return d, s, step, c, (c >= 0) & (c < chips)

    def onward(step):
        nxt = z - step
        return nxt, (nxt >= 0) & (nxt < chips), (step + 1) // 2

    @pl.loop(0, 2 * pieces * (chips - 1))
    def _(i):
        d, s, step, c, valid = decode(i)
        nxt, pass_on, way = onward(step)

        @pl.when(valid)
        def _():
            @pl.when(s == 0)
            def _():
                n_arrived(2 * c + k)

                @pl.when(pass_on)
                def _():
                    n_copy(c, nfwd.at[way, c], 2 * nxt + k).start()

                n_copy(c, nshare.at[c], partner).start()

            x_arrived(2 * c + k, s)

            @pl.when(pass_on)
            def _():
                x_copy(c, s, fwd.at[way, c, s], 2 * nxt + k).start()

            x_copy(c, s, share.at[c, s], partner).start()
            add(2 * c + k, s, False)

            @pl.when(s == 0)
            def _():
                n_arrived(2 * c + 1 - k)

            x_arrived(2 * c + 1 - k, s)
            add(2 * c + 1 - k, s, False)

        last = (d == far) & (step == 1)

        @pl.when(last & (s == 0))
        def _():
            project_new()

        @pl.when(last)
        def _():
            finish(s)

    raws = []
    for s in range(seqs):
        for o in range(1, n_sp):
            src = lax.rem(sp + o, n_sp)
            pltpu.make_async_remote_copy(
                stage.at[s, src], landed.at[s, src], rs_tx.at[s, src], rs_rx.at[s, src],
                device_id={"sp": src}, device_id_type=MESH,
            ).wait_recv()
        total = None
        for j in range(n_sp):
            term = jnp.where(sp == j, totals[s], landed[s, j])
            total = term if total is None else total + term
        kept = total[0:keep].astype(BF16)
        for h in range(heads):
            state_out[s, h] = kept[:, h * HD : (h + 1) * HD]
        raws.append(total[keep : keep + 1] * rows_ref[1:2] + own_term[s : s + 1])
    raw = jnp.concatenate(raws, axis=0)
    for h in range(heads):
        at = slice(h * HD, (h + 1) * HD)
        head = raw[:, at]
        centered = head - jnp.mean(head, axis=-1, keepdims=True)
        spread = jnp.mean(centered * centered, axis=-1, keepdims=True)
        read_out[:, at] = (centered * lax.rsqrt(spread + 1e-05)).astype(BF16)

    @pl.when(z < chips - 1)
    def _():
        n_up.wait_send()

    @pl.when(z > 0)
    def _():
        n_down.wait_send()

    n_side.wait_send()
    for s in range(seqs):
        for o in range(1, n_sp):
            rs_copy(s, o).wait_send()
    for s in range(pieces):
        @pl.when(z < chips - 1)
        def _(s=s):
            x_copy(z, s, fwd.at[0, z, s], tp + 2).wait_send()

        @pl.when(z > 0)
        def _(s=s):
            x_copy(z, s, fwd.at[1, z, s], tp - 2).wait_send()

        x_copy(z, s, share.at[z, s], partner).wait_send()

    @pl.loop(0, 2 * pieces * (chips - 1))
    def _(i):
        d, s, step, c, valid = decode(i)
        nxt, pass_on, way = onward(step)

        @pl.when(valid)
        def _():
            @pl.when(s == 0)
            def _():
                @pl.when(pass_on)
                def _():
                    n_copy(c, nfwd.at[way, c], 2 * nxt + k).wait_send()

                n_copy(c, nshare.at[c], partner).wait_send()

            @pl.when(pass_on)
            def _():
                x_copy(c, s, fwd.at[way, c, s], 2 * nxt + k).wait_send()

            x_copy(c, s, share.at[c, s], partner).wait_send()


def one_of(n, values):
    total = 0
    for k, value in enumerate(values):
        if value:
            total = total + (n == k).astype(jnp.int32) * value
    return total


def middle_order(main, moved):
    near = [(0, i) for i in main]
    far = [(2, i) for i in moved + main]
    order = [(kind, i) for i in moved for kind in (0, 1)]
    order += [(1, i) for i in main]
    for at in range(max(len(near), len(far))):
        order += near[at : at + 1] + far[at : at + 1]
    return order


def moved_kernel(
    n_sp, n_tp, parts,
    tokens, fresh, wq_hbm, wk_hbm, wv_hbm, inverse_ref, decay_ref,
    state_out, read_out,
    x, xc, nx, wq, wk, wv, we, acc_k, acc_v, acc_c, cos_ref, sin_ref, fade_ref, rows_ref,
    q_spread, own_term, sums, stage, landed, totals, hint, hint_in, stage_c, landed_c,
    load_sem, weight_sem, rx, rn, ry, rw, tx, hint_rx, rs_rx, c_rx, ready,
):
    seqs, span, feat = tokens.shape
    inner = wk.shape[1]
    heads = inner // HD
    half = inner // 2
    chunks = half // LANES
    chips = n_tp // 2
    pieces = seqs * parts
    size = span // parts
    keep = HD // n_sp
    groups = n_tp // 2
    moved_seq = seqs - 1
    to_mate_tx, to_other_tx, share_tx, n_tx, n_share_tx, y_tx, y_share_tx, w_tx, w_pass_tx = range(9)
    hint_tx, rs_tx, c_tx = range(9, 12)
    main = list(range(moved_seq * parts))
    moved = list(range(moved_seq * parts, pieces))
    sp = lax.axis_index("sp")
    tp = lax.axis_index("tp")
    z, k = tp // 2, tp % 2
    row_y, row_x = sp // 2, sp % 2
    x_peer = sp + 1 - 2 * row_x
    y_peer = sp + 2 - 4 * row_y
    MESH = pl.DeviceIdType.MESH
    end_int = (z == 0).astype(jnp.int32) + (z == chips - 1).astype(jnp.int32)
    end = end_int > 0
    mid = end_int == 0
    partner = z * 2 + 1 - k
    mate = z + 1 - 2 * (z % 2)
    mate_tp = 2 * mate + k
    other = chips - 1 - z
    other_tp = 2 * other + k
    second = end_int * (chips - 1 - mate) + (1 - end_int) * (chips - 1 - z)
    third = end_int * (chips - 1 - z) + (1 - end_int) * (chips - 1 - mate)

    own_loads = {
        s: pltpu.make_async_copy(
            tokens.at[s // parts, pl.ds(s % parts * size, size)], x.at[tp, s], load_sem.at[s]
        )
        for s in range(pieces)
    }
    new_load = pltpu.make_async_copy(fresh, nx.at[tp], load_sem.at[pieces])
    new_load.start()
    for s in moved + main:
        own_loads[s].start()
    weight_loads = [
        pltpu.make_async_copy(a, b, weight_sem.at[i])
        for i, (a, b) in enumerate(((wk_hbm, wk), (wv_hbm, wv), (wq_hbm, wq)))
    ]

    barrier = pltpu.get_barrier_semaphore()
    for target in ({"tp": partner}, {"tp": mate_tp}, {"sp": x_peer}, {"sp": y_peer}):
        pl.semaphore_signal(barrier, inc=1, device_id=target, device_id_type=MESH)

    @pl.when(mid)
    def _():
        pl.semaphore_signal(barrier, inc=1, device_id={"tp": other_tp}, device_id_type=MESH)

    pl.semaphore_wait(barrier, 5 - end_int)
    for target in ({"sp": x_peer}, {"sp": y_peer}):
        pl.semaphore_signal(ready.at[0], inc=1, device_id=target, device_id_type=MESH)

    def remote(source, dest, send, recv, target):
        return pltpu.make_async_remote_copy(
            source, dest, send, recv, device_id=target, device_id_type=MESH
        )

    def sent(ref, kind):
        remote(ref, ref, tx.at[kind], hint_rx.at[0], {"tp": partner}).wait_send()

    def arrived(ref, sem):
        remote(ref, ref, tx.at[0], sem, {"tp": partner}).wait_recv()

    def x_copy(c, s, kind, target):
        here = x.at[2 * c + k, s]
        return remote(here, here, tx.at[kind], rx.at[2 * c + k, s], {"tp": target})

    def to_mate(c, s):
        return x_copy(c, s, to_mate_tx, mate_tp)

    def to_other(c, s):
        return x_copy(c, s, to_other_tx, other_tp)

    def to_partner(c, s):
        return x_copy(c, s, share_tx, partner)

    def x_arrived(p, s):
        arrived(x.at[p, s], rx.at[p, s])

    def y_send(c, j):
        p = 2 * c + k
        return remote(
            x.at[p, moved[0] + j], xc.at[p, j], tx.at[y_tx], ry.at[c * parts + j], {"sp": y_peer}
        )

    def y_share(c, j):
        here = xc.at[2 * c + k, j]
        late = (c == third).astype(jnp.int32)
        return remote(
            here, here, tx.at[y_share_tx], ry.at[chips * parts + late], {"tp": partner}
        )

    def w_rows(p):
        return pl.ds(pl.multiple_of(p * feat, feat), feat)

    def w_cols(cc):
        return pl.ds(pl.multiple_of(row_y * half + cc * LANES, LANES), LANES)

    def w_place(cc, g, kv):
        return we.at[cc, w_rows(row_x * groups + g), pl.ds(kv * LANES, LANES)]

    def w_sem(cc, g, kv):
        return rw.at[g if cc == 0 else groups + 2 * g + kv]

    def w_peer_sem(cc, g):
        return rw.at[3 * groups + cc * (1 + g)]

    def w_send(cc, g, kv):
        mine = (wk, wv)[kv].at[w_rows(row_x * groups + g), w_cols(cc)]
        return remote(mine, w_place(cc, g, kv), tx.at[w_tx], w_sem(cc, g, kv), {"tp": mate_tp})

    def w_pass(cc, g, kv):
        here = w_place(cc, g, kv)
        return remote(here, here, tx.at[w_pass_tx], w_peer_sem(cc, g), {"sp": x_peer})

    def n_copy(c, kind, sem, target):
        here = nx.at[2 * c + k]
        return remote(here, here, tx.at[kind], sem, {"tp": target})

    def n_to(c, target):
        n_copy(c, n_tx, rn.at[c], target).start()

    def n_share(c):
        n_copy(c, n_share_tx, rn.at[chips], partner).start()

    def n_arrived(c):
        arrived(nx.at[2 * c + k], rn.at[c])

    hint_copy = remote(hint, hint_in, tx.at[hint_tx], hint_rx.at[0], {"tp": mate_tp})

    new_load.wait()
    n_to(z, mate_tp)
    n_share(z)

    @pl.when(mid)
    def _():
        n_to(z, other_tp)

    for s in moved + main:
        own_loads[s].wait()

    def send_moved(j):
        s = moved[j]

        @pl.when(mid)
        def _():
            to_other(z, s).start()
            y_send(z, j).start()
            to_partner(z, s).start()

        @pl.when(end)
        def _():
            to_mate(z, s).start()

    send_moved(0)
    to_partner(z, main[0]).start()

    @pl.when(mid)
    def _():
        to_mate(z, main[0]).start()

    for copy in weight_loads:
        copy.start()

    @pl.when(mid)
    def _():
        n_arrived(mate)
        n_to(mate, other_tp)
        n_share(mate)
        n_arrived(other)
        n_to(other, mate_tp)
        n_share(other)

    for j in range(1, parts):
        send_moved(j)
    for s in main[1:]:
        to_partner(z, s).start()

    @pl.when(mid)
    def _():
        for s in main[1:2]:
            to_mate(z, s).start()
        for s in main:
            to_other(z, s).start()

    row = lax.broadcasted_iota(jnp.int32, (span, LANES), 0)
    within = lane_iota((1, LANES)) % HD
    first_half = jnp.where(within < HD // 2, -1.0, 1.0).astype(F32)
    inverse = inverse_ref[...]

    def tables(slot, column):
        angles = (column * span + row).astype(F32) * inverse
        cos_ref[slot] = jnp.cos(angles)
        sin_ref[slot] = jnp.sin(angles) * first_half

    for copy in weight_loads[:2]:
        copy.wait()

    @pl.when(end)
    def _():
        for g in range(groups):
            for kv in range(2):
                w_send(0, g, kv).start()

    tables(0, sp)

    @pl.when(mid)
    def _():
        tables(1, y_peer)

    new_angles = jnp.full((NEW_ROWS, LANES), n_sp * span, F32) * inverse
    new_cos = jnp.cos(new_angles)
    new_sin = jnp.sin(new_angles) * first_half
    head_of = lane_iota((1, inner)) // HD
    rate = jnp.zeros((1, inner), F32)
    for h in range(heads):
        rate = jnp.where(head_of == h, decay_ref[h], rate)
    to_end = (span - 1 - lax.broadcasted_iota(jnp.int32, (span, 1), 0)).astype(F32)
    fade_ref[...] = jnp.exp(to_end * rate)
    rows_ref[0:1] = jnp.exp(rate * (span * (n_sp - 1 - sp)).astype(F32))
    rows_ref[1:2] = jnp.exp(rate)
    hint[...] = jnp.zeros(hint.shape, F32)
    hint[1:2] = rate
    weight_loads[2].wait()

    def add(p, s, fresh_total):
        block = x[p, s]
        where = w_rows(p)
        part_k = jnp.dot(block, wk[where, :], preferred_element_type=F32)
        part_v = jnp.dot(block, wv[where, :], preferred_element_type=F32)
        if fresh_total:
            acc_k[s] = part_k
            acc_v[s] = part_v
        else:
            acc_k[s] += part_k
            acc_v[s] += part_v

    same = (
        lax.broadcasted_iota(jnp.int32, (inner, inner), 0) // HD
        == lax.broadcasted_iota(jnp.int32, (inner, inner), 1) // HD
    )
    pick = lax.broadcasted_iota(jnp.int32, (HD, inner), 0) == lane_iota((HD, inner)) % HD

    @pl.when(mid)
    def _():
        n_arrived(third)
        n_to(third, mate_tp)
        n_share(third)
        for s in main[2:]:
            to_mate(z, s).start()

    own_pieces = end_int * len(main) + (1 - end_int) * pieces

    @pl.loop(0, pieces)
    def _(i):
        s = lax.rem(i + (1 - end_int) * len(main), pieces)

        @pl.when(i < own_pieces)
        def _():
            add(tp, s, True)

        @pl.when(i < own_pieces)
        def _():
            x_arrived(partner, s)
            add(partner, s, False)

    @pl.when(end)
    def _():
        for c in (mate, second, third):
            n_arrived(c)
            n_share(c)

    arrived(nx.at[pl.ds(0, chips)], rn.at[chips])

    def project_new():
        def piece(p, totals):
            where = w_rows(p)
            block = jnp.concatenate(
                [nx[p].astype(F32), jnp.zeros((NEW_ROWS - seqs, feat), F32)], axis=0
            ).astype(BF16)
            return tuple(
                t + jnp.dot(block, w[where, :], preferred_element_type=F32)
                for t, w in zip(totals, (wk, wv, wq))
            )

        zero = jnp.zeros((NEW_ROWS, inner), F32)
        new_k, new_v, new_q = lax.fori_loop(0, n_tp, piece, (zero, zero, zero))
        keys, queries = [], []
        for j in range(inner // LANES):
            at = slice(j * LANES, (j + 1) * LANES)
            keys.append((rotated(new_k[:, at], new_cos, new_sin) * HD**-0.5).astype(BF16))
            queries.append(rotated(new_q[:, at], new_cos, new_sin).astype(BF16))
        key = jnp.concatenate(keys, axis=1).astype(F32)
        query = jnp.concatenate(queries, axis=1).astype(F32)
        value = new_v.astype(BF16).astype(F32)
        product = query * key
        for h in range(heads):
            at = slice(h * HD, (h + 1) * HD)
            own_term[:, at] = jnp.sum(product[:, at], axis=-1, keepdims=True) * value[:, at]
        hint[0:1] = query[moved_seq : moved_seq + 1]
        for s in range(seqs):
            spread = jnp.where(pick, query[s : s + 1], 0.0).astype(BF16)
            q_spread[s] = jnp.dot(
                spread, jnp.where(same, 1.0, 0.0).astype(BF16), preferred_element_type=F32
            )

    project_new()

    @pl.when(end)
    def _():
        hint_copy.start()
        for s in main:
            to_mate(z, s).start()
        for cc in range(1, chunks):
            for g in range(groups):
                for kv in range(2):
                    w_send(cc, g, kv).start()

    def rs_copy(s, o):
        peer = lax.rem(sp + o, n_sp)
        return remote(
            stage.at[s, peer], landed.at[s, sp], tx.at[rs_tx], rs_rx.at[s], {"sp": peer}
        )

    pl.semaphore_wait(ready.at[0], 2)
    pl.semaphore_signal(ready.at[1], inc=1, device_id={"sp": x_peer}, device_id_type=MESH)

    def outer(weighted, value):
        both = lax.dot_general(
            weighted, value, (((0,), (0,)), ((), ())), preferred_element_type=F32
        )
        return jnp.where(lane_iota((HD, LANES)) < HD, both[:HD], both[HD:])

    def finish(i):
        s, part = i // parts, i % parts
        where = pl.ds(pl.multiple_of(part * size, size), size)
        cosine, sine = cos_ref[0, where, :], sin_ref[0, where, :]
        for j in range(inner // LANES):
            at = slice(j * LANES, (j + 1) * LANES)
            key = (rotated(acc_k[i, :, at], cosine, sine) * HD**-0.5).astype(BF16)
            weighted = (key.astype(F32) * fade_ref[where, at]).astype(BF16)
            value = acc_v[i, :, at].astype(BF16)
            state = outer(weighted, value)
            sums[:, at] = jnp.where(part == 0, state, sums[:, at] + state)

        @pl.when(part == parts - 1)
        def _():
            scaled = sums[...] * rows_ref[0:1]
            read = jnp.sum(scaled * q_spread[s], axis=0, keepdims=True)
            for o in range(n_sp):
                stage[s, o, 0:keep] = scaled[o * keep : (o + 1) * keep]
                stage[s, o, keep : keep + 1] = read
            totals[s] = stage[s, sp]

            @pl.when(end | (s == moved_seq))
            def _():
                for o in range(1, n_sp):
                    rs_copy(s, o).start()

    def c_add(cc, p, fresh_total):
        where = w_rows(p)
        for t in range(parts):
            for side, block in ((0, x[p, moved[0] + t]), (1, xc[p, t])):
                both = jnp.dot(block, we[cc, where, :], preferred_element_type=F32)
                if fresh_total:
                    acc_c[side, t] = both
                else:
                    acc_c[side, t] += both

    def c_copy(cc, o):
        return remote(
            stage_c.at[cc, o], landed_c.at[cc, sp], tx.at[c_tx], c_rx.at[cc],
            {"sp": o, "tp": mate_tp},
        )

    def c_finish(cc):
        pair_rate = hint_in[1:2, w_cols(cc)]
        query = hint_in[0:1, w_cols(cc)]
        total = jnp.zeros((HD, LANES), F32)
        for side, column in ((0, sp), (1, y_peer)):
            state = jnp.zeros((HD, LANES), F32)
            for t in range(parts):
                at = slice(t * size, (t + 1) * size)
                key = (
                    rotated(acc_c[side, t, :, :LANES], cos_ref[side, at], sin_ref[side, at])
                    * HD**-0.5
                ).astype(BF16)
                fade = jnp.exp(to_end[at] * pair_rate)
                weighted = (key.astype(F32) * fade).astype(BF16)
                state = state + outer(weighted, acc_c[side, t, :, LANES:].astype(BF16))
            total = total + state * jnp.exp(
                pair_rate * (span * (n_sp - 1 - column)).astype(F32)
            )
        spread = jnp.where(pick[:, :LANES], query, 0.0).astype(BF16)
        spread = jnp.dot(
            spread, jnp.where(same[:LANES, :LANES], 1.0, 0.0).astype(BF16),
            preferred_element_type=F32,
        )
        read = jnp.sum(total * spread, axis=0, keepdims=True)
        for o in range(n_sp):
            stage_c[cc, o, 0:keep] = total[o * keep : (o + 1) * keep]
            stage_c[cc, o, keep : keep + 1] = read
        for o in range(n_sp):
            c_copy(cc, o).start()

    order = middle_order(main, moved)
    steps = end_int * (len(main) * (chips - 1)) + (1 - end_int) * len(order)

    def decode(n):
        kind = end_int * (n // len(main)) + (1 - end_int) * one_of(n, [o[0] for o in order])
        s = end_int * (n % len(main)) + (1 - end_int) * one_of(n, [o[1] for o in order])
        c = (
            (kind == 0).astype(jnp.int32) * mate
            + (kind == 1).astype(jnp.int32) * second
            + (kind == 2).astype(jnp.int32) * third
        )
        return kind, c, s

    first_w = 2 * len(moved) + 1
    c_at = len(order) - 3

    def w_relay(cc, g, kv):
        arrived(w_place(cc, g, kv), w_sem(cc, g, kv))
        w_pass(cc, g, kv).start()

    def w_own(cc, g, fresh_total=False):
        c_add(cc, row_x * groups + g, fresh_total)

    def w_peer(cc, g):
        p = (1 - row_x) * groups + g
        arrived(we.at[cc, w_rows(p)], w_peer_sem(cc, g))
        c_add(cc, p, False)

    def y_pass(c, j):
        arrived(xc.at[2 * c + k, j], ry.at[c * parts + j])
        y_share(c, j).start()

    @pl.loop(0, len(order) + 1)
    def _(n):
        kind, c, s = decode(n)
        is_moved = s >= moved[0]

        @pl.when(mid & (n == len(order) - 2))
        def _():
            w_relay(1, 0, 1)

        @pl.when(mid & (n == len(order) - 1))
        def _():
            w_relay(1, 1, 0)

        @pl.when(n < steps)
        def _():
            x_arrived(2 * c + k, s)

            @pl.when(mid & (kind == 0))
            def _():
                to_other(c, s).start()

            @pl.when(mid & (kind > 0) & (s < moved[0]))
            def _():
                to_mate(c, s).start()

            @pl.when(mid & is_moved)
            def _():
                y_send(c, s - moved[0]).start()

            to_partner(c, s).start()

        @pl.when(mid & (n == len(order) - 1))
        def _():
            w_relay(1, 1, 1)

        @pl.when(mid & (n >= first_w) & (n < first_w + groups))
        def _():
            g = n - first_w
            arrived(we.at[0, w_rows(row_x * groups + g)], w_sem(0, g, 0))
            for kv in range(2):
                w_pass(0, g, kv).start()

        @pl.when(mid & (n >= 3) & (n < 3 + parts))
        def _():
            y_pass(z, n - 3)

        @pl.when(mid & (n >= 6) & (n < 6 + 2 * parts))
        def _():
            m = n - 6
            y_pass((m % 2) * second + (1 - m % 2) * mate, m // 2)

        @pl.when(mid & (n >= c_at - parts) & (n < c_at))
        def _():
            y_pass(third, n - (c_at - parts))

        @pl.when(n < steps)
        def _():
            add(2 * c + k, s, False)

        kind_b, c_b, s_b = decode(n - 1)

        @pl.when((n >= 1) & (n <= steps))
        def _():
            x_arrived(2 * c_b + 1 - k, s_b)
            add(2 * c_b + 1 - k, s_b, False)

            @pl.when(kind_b == 2)
            def _():
                finish(s_b)

        early = n - (c_at - 5)

        @pl.when(mid & (early == 0))
        def _():
            arrived(xc.at[pl.ds(0, chips - 1)], ry.at[chips * parts])
            arrived(we.at[0, pl.ds(0, groups * feat)], w_peer_sem(0, 0))
            acc_c[...] = jnp.zeros(acc_c.shape, F32)

        @pl.when(mid & (early >= 0) & (early < 6))
        def _():
            turn = early // 2
            cx = (
                (turn == 0).astype(jnp.int32) * z
                + (turn == 1).astype(jnp.int32) * mate
                + (turn == 2).astype(jnp.int32) * second
            )
            c_add(0, 2 * cx + early % 2, False)

        @pl.when(mid & (n == c_at))
        def _():
            arrived(xc.at[0], ry.at[chips * parts + 1])

            @pl.loop(0, 2)
            def _(m):
                c_add(0, 2 * third + m, False)

            w_relay(1, 0, 0)

            hint_copy.wait_recv()
            pl.semaphore_wait(ready.at[1], 1)
            c_finish(0)

    @pl.when(mid)
    def _():
        w_relay(1, 2, 0)
        w_own(1, 0, True)
        w_peer(1, 0)
        w_own(1, 1)
        w_relay(1, 2, 1)
        w_peer(1, 1)
        w_own(1, 2)
        w_relay(1, 3, 0)
        w_relay(1, 3, 1)
        w_peer(1, 2)
        for s in range(moved_seq):
            for o in range(1, n_sp):
                rs_copy(s, o).start()
        w_own(1, 3)
        w_peer(1, 3)
        c_finish(1)

    def gather(s):
        arrived(landed.at[s, pl.ds(0, n_sp - 1)], rs_rx.at[s])
        total = None
        for j in range(n_sp):
            term = jnp.where(sp == j, totals[s], landed[s, j])
            total = term if total is None else total + term
        totals[s] = total

    sent(nx.at[pl.ds(0, chips)], n_share_tx)

    @pl.when(end)
    def _():
        pl.semaphore_wait(ready.at[1], 1)
        sent(nx.at[0], n_tx)
        sent(hint, hint_tx)
        sent(x.at[0], to_mate_tx)
        sent(x.at[pl.ds(0, chips), pl.ds(0, len(main))], share_tx)
        sent(we.at[pl.ds(0, chunks), pl.ds(0, groups * feat)], w_tx)
        sent(stage.at[pl.ds(0, moved_seq), pl.ds(0, n_sp - 1)], rs_tx)

    @pl.when(mid)
    def _():
        sent(nx.at[pl.ds(0, 5)], n_tx)
        sent(x.at[pl.ds(0, chips - 1), pl.ds(0, len(main))], to_mate_tx)
        sent(x.at[pl.ds(0, 2)], to_other_tx)
        sent(x.at[pl.ds(0, chips)], share_tx)
        sent(xc.at[pl.ds(0, chips)], y_tx)
        sent(xc.at[pl.ds(0, chips)], y_share_tx)
        sent(we.at[pl.ds(0, chunks), pl.ds(0, groups * feat)], w_pass_tx)
        sent(stage.at[:, pl.ds(0, n_sp - 1)], rs_tx)

    for s in range(moved_seq):
        gather(s)

    @pl.when(mid)
    def _():
        gather(moved_seq)

    @pl.when(end)
    def _():
        for cc in range(chunks):
            arrived(landed_c.at[cc], c_rx.at[cc])
            for side in range(2):
                at = slice(side * half + cc * LANES, side * half + (cc + 1) * LANES)
                totals[moved_seq, :, at] = landed_c[cc, 2 * side] + landed_c[cc, 2 * side + 1]

    raws = []
    for s in range(seqs):
        total = totals[s]
        kept = total[0:keep].astype(BF16)
        for h in range(heads):
            state_out[s, h] = kept[:, h * HD : (h + 1) * HD]
        raws.append(total[keep : keep + 1] * rows_ref[1:2] + own_term[s : s + 1])
    raw = jnp.concatenate(raws, axis=0)
    for h in range(heads):
        at = slice(h * HD, (h + 1) * HD)
        head = raw[:, at]
        centered = head - jnp.mean(head, axis=-1, keepdims=True)
        spread = jnp.mean(centered * centered, axis=-1, keepdims=True)
        read_out[:, at] = (centered * lax.rsqrt(spread + 1e-05)).astype(BF16)

    @pl.when(mid)
    def _():
        sent(stage_c, c_tx)


def solution(mesh):
    n_sp, n_tp = mesh.shape["sp"], mesh.shape["tp"]

    def body(tokens, new_token, query_weight, key_weight, value_weight, log_decay):
        seqs, span, feat = tokens.shape
        width, inner = key_weight.shape
        heads = inner // HD
        keep = HD // n_sp
        rows = -(-(keep + 1) // 8) * 8
        chips = n_tp // 2
        half = HD // 2
        parts = max(1, 8 // chips)
        pieces = seqs * parts
        size = span // parts
        inverse = np.float32(10000.0) ** (-np.arange(half, dtype=np.float32) / half)
        inverse = jnp.asarray(np.tile(inverse.astype(np.float32), LANES // half)[None])
        anywhere = pl.BlockSpec(memory_space=pl.ANY)
        vmem = pl.BlockSpec(memory_space=pltpu.VMEM)
        dma = pltpu.SemaphoreType.DMA
        moves = chips == 4 and n_sp == 4 and seqs > 1 and inner == 4 * LANES
        tokens_in = [
            pltpu.VMEM((n_tp, pieces, size, feat), BF16),
            pltpu.VMEM((n_tp, seqs, feat), BF16),
        ]
        weights_in = [pltpu.VMEM((width, inner), BF16)] * 3
        totals = [pltpu.VMEM((pieces, size, inner), F32)] * 2
        ends = [
            pltpu.VMEM((8, inner), F32),
            pltpu.VMEM((seqs, HD, inner), F32),
            pltpu.VMEM((NEW_ROWS, inner), F32),
            pltpu.VMEM((HD, inner), F32),
            pltpu.VMEM((seqs, n_sp, rows, inner), F32),
            pltpu.VMEM((seqs, n_sp, rows, inner), F32),
            pltpu.VMEM((seqs, rows, inner), F32),
        ]
        if moves:
            chunks = inner // 2 // LANES
            groups = n_tp // 2
            call = moved_kernel
            scratch = (
                tokens_in[:1]
                + [pltpu.VMEM((n_tp, parts, size, feat), BF16)]
                + tokens_in[1:]
                + weights_in
                + [pltpu.VMEM((chunks, width, 2 * LANES), BF16)]
                + totals
                + [
                    pltpu.VMEM((2, parts, size, 2 * LANES), F32),
                    pltpu.VMEM((2, span, LANES), F32),
                    pltpu.VMEM((2, span, LANES), F32),
                    pltpu.VMEM((span, inner), F32),
                ]
                + ends
                + [
                    pltpu.VMEM((8, inner), F32),
                    pltpu.VMEM((8, inner), F32),
                    pltpu.VMEM((chunks, n_sp, rows, LANES), F32),
                    pltpu.VMEM((chunks, n_sp, rows, LANES), F32),
                    dma((pieces + 1,)),
                    dma((3,)),
                    dma((n_tp, pieces)),
                    dma((chips + 1,)),
                    dma((chips * parts + 2,)),
                    dma((4 * groups + 1,)),
                    dma((12,)),
                    dma((1,)),
                    dma((seqs,)),
                    dma((chunks,)),
                    pltpu.SemaphoreType.REGULAR((2,)),
                ]
            )
        else:
            call = kernel
            scratch = (
                tokens_in
                + weights_in
                + totals
                + [
                    pltpu.VMEM((span, LANES), F32),
                    pltpu.VMEM((span, LANES), F32),
                    pltpu.VMEM((span, inner), F32),
                ]
                + ends
                + [
                    dma((pieces + 1,)),
                    dma((3,)),
                    dma((n_tp, pieces)),
                    dma((n_tp,)),
                    dma((2, chips, pieces)),
                    dma((chips, pieces)),
                    dma((2, chips)),
                    dma((chips,)),
                    dma((seqs, n_sp)),
                    dma((seqs, n_sp)),
                ]
            )
        return pl.pallas_call(
            functools.partial(call, n_sp, n_tp, parts),
            out_shape=(
                jax.ShapeDtypeStruct((seqs, heads, keep, HD), BF16),
                jax.ShapeDtypeStruct((seqs, inner), BF16),
            ),
            in_specs=[anywhere] * 5 + [vmem, pl.BlockSpec(memory_space=pltpu.SMEM)],
            out_specs=(vmem, vmem),
            scratch_shapes=scratch,
            compiler_params=pltpu.CompilerParams(
                collective_id=0, has_side_effects=True, vmem_limit_bytes=60 * 1024 * 1024
            ),
            name="retention",
        )(tokens, new_token.reshape(seqs, feat), query_weight, key_weight, value_weight, inverse, log_decay)

    return jax.shard_map(
        body,
        mesh=mesh,
        in_specs=(
            P(None, "sp", "tp"),
            P(None, None, "tp"),
            P(None, "tp"),
            P(None, "tp"),
            P(None, "tp"),
            P("tp"),
        ),
        out_specs=(P(None, "tp", "sp", None), P(None, "tp")),
        check_vma=False,
    )
```

```python
import functools

import jax
import jax.numpy as jnp
import numpy as np
from jax import lax
from jax.experimental import pallas as pl
from jax.experimental.pallas import tpu as pltpu
from jax.sharding import PartitionSpec as P

HD = 64
LANES = 128
NEW_ROWS = 8
F32 = jnp.float32
BF16 = jnp.bfloat16


def lane_iota(shape):
    return lax.broadcasted_iota(jnp.int32, shape, len(shape) - 1)


def rotated(block, cosine, sine):
    half = HD // 2
    low = lane_iota(block.shape) % HD < half
    swapped = jnp.where(
        low, pltpu.roll(block, LANES - half, 1), pltpu.roll(block, half, 1)
    )
    return block * cosine + swapped * sine


def kernel(
    n_sp, n_tp, parts,
    tokens, fresh, wq_hbm, wk_hbm, wv_hbm, inverse_ref, decay_ref,
    state_out, read_out,
    x, nx, wq, wk, wv, acc_k, acc_v, cos_ref, sin_ref, fade_ref, rows_ref,
    q_spread, own_term, sums, stage, landed, totals,
    load_sem, weight_sem, rx, rn, fwd, share, nfwd, nshare, rs_tx, rs_rx,
):
    seqs, span, feat = tokens.shape
    inner = wk.shape[1]
    heads = inner // HD
    chips = n_tp // 2
    pieces = seqs * parts
    size = span // parts
    keep = HD // n_sp
    sp = lax.axis_index("sp")
    tp = lax.axis_index("tp")
    z, k = tp // 2, tp % 2
    MESH = pl.DeviceIdType.MESH

    def to_tp(index):
        return {"tp": index}

    partner = z * 2 + 1 - k
    own_loads = [
        pltpu.make_async_copy(
            tokens.at[s // parts, pl.ds(s % parts * size, size)], x.at[tp, s], load_sem.at[s]
        )
        for s in range(pieces)
    ]
    new_load = pltpu.make_async_copy(fresh, nx.at[tp], load_sem.at[pieces])
    new_load.start()
    for copy in own_loads:
        copy.start()
    weight_loads = [
        pltpu.make_async_copy(a, b, weight_sem.at[i])
        for i, (a, b) in enumerate(((wk_hbm, wk), (wv_hbm, wv), (wq_hbm, wq)))
    ]

    barrier = pltpu.get_barrier_semaphore()

    @pl.when(z > 0)
    def _():
        pl.semaphore_signal(barrier, inc=1, device_id=to_tp(tp - 2), device_id_type=MESH)

    @pl.when(z < chips - 1)
    def _():
        pl.semaphore_signal(barrier, inc=1, device_id=to_tp(tp + 2), device_id_type=MESH)

    pl.semaphore_signal(barrier, inc=1, device_id=to_tp(partner), device_id_type=MESH)
    for o in range(1, n_sp):
        pl.semaphore_signal(
            barrier, inc=1, device_id={"sp": lax.rem(sp + o, n_sp)}, device_id_type=MESH
        )
    pl.semaphore_wait(
        barrier, n_sp + (z > 0).astype(jnp.int32) + (z < chips - 1).astype(jnp.int32)
    )

    def x_copy(c, s, sem, target):
        p = 2 * c + k
        return pltpu.make_async_remote_copy(
            x.at[p, s], x.at[p, s], sem, rx.at[p, s], device_id=to_tp(target), device_id_type=MESH
        )

    def n_copy(c, sem, target):
        p = 2 * c + k
        return pltpu.make_async_remote_copy(
            nx.at[p], nx.at[p], sem, rn.at[p], device_id=to_tp(target), device_id_type=MESH
        )

    def x_arrived(p, s):
        pltpu.make_async_remote_copy(
            x.at[p, s], x.at[p, s], share.at[0, 0], rx.at[p, s],
            device_id=to_tp(partner), device_id_type=MESH,
        ).wait_recv()

    def n_arrived(p):
        pltpu.make_async_remote_copy(
            nx.at[p], nx.at[p], nshare.at[0], rn.at[p],
            device_id=to_tp(partner), device_id_type=MESH,
        ).wait_recv()

    new_load.wait()
    n_up = n_copy(z, nfwd.at[0, z], tp + 2)
    n_down = n_copy(z, nfwd.at[1, z], tp - 2)
    n_side = n_copy(z, nshare.at[z], partner)

    @pl.when(z < chips - 1)
    def _():
        n_up.start()

    @pl.when(z > 0)
    def _():
        n_down.start()

    n_side.start()
    for s in range(pieces):
        own_loads[s].wait()

        @pl.when(z < chips - 1)
        def _(s=s):
            x_copy(z, s, fwd.at[0, z, s], tp + 2).start()

        @pl.when(z > 0)
        def _(s=s):
            x_copy(z, s, fwd.at[1, z, s], tp - 2).start()

        x_copy(z, s, share.at[z, s], partner).start()

    for copy in weight_loads:
        copy.start()

    row = lax.broadcasted_iota(jnp.int32, (span, LANES), 0)
    within = lane_iota((1, LANES)) % HD
    first_half = jnp.where(within < HD // 2, -1.0, 1.0).astype(F32)
    inverse = inverse_ref[...]
    angles = (sp * span + row).astype(F32) * inverse
    cos_ref[...] = jnp.cos(angles)
    sin_ref[...] = jnp.sin(angles) * first_half
    new_angles = jnp.full((NEW_ROWS, LANES), n_sp * span, F32) * inverse
    new_cos = jnp.cos(new_angles)
    new_sin = jnp.sin(new_angles) * first_half
    head_of = lane_iota((1, inner)) // HD
    rate = jnp.zeros((1, inner), F32)
    for h in range(heads):
        rate = jnp.where(head_of == h, decay_ref[h], rate)
    to_end = (span - 1 - lax.broadcasted_iota(jnp.int32, (span, 1), 0)).astype(F32)
    fade_ref[...] = jnp.exp(to_end * rate)
    rows_ref[0:1] = jnp.exp(rate * (span * (n_sp - 1 - sp)).astype(F32))
    rows_ref[1:2] = jnp.exp(rate)

    for copy in weight_loads:
        copy.wait()

    def add(p, s, fresh_total):
        block = x[p, s]
        where = pl.ds(pl.multiple_of(p * feat, feat), feat)
        part_k = jnp.dot(block, wk[where, :], preferred_element_type=F32)
        part_v = jnp.dot(block, wv[where, :], preferred_element_type=F32)
        if fresh_total:
            acc_k[s] = part_k
            acc_v[s] = part_v
        else:
            acc_k[s] += part_k
            acc_v[s] += part_v

    @pl.loop(0, pieces)
    def _(s):
        add(tp, s, True)
        x_arrived(partner, s)
        add(partner, s, False)

    n_arrived(partner)

    def project_new():
        def piece(p, totals):
            where = pl.ds(pl.multiple_of(p * feat, feat), feat)
            block = jnp.concatenate(
                [nx[p].astype(F32), jnp.zeros((NEW_ROWS - seqs, feat), F32)], axis=0
            ).astype(BF16)
            return tuple(
                t + jnp.dot(block, w[where, :], preferred_element_type=F32)
                for t, w in zip(totals, (wk, wv, wq))
            )

        zero = jnp.zeros((NEW_ROWS, inner), F32)
        new_k, new_v, new_q = lax.fori_loop(0, n_tp, piece, (zero, zero, zero))
        keys, queries = [], []
        for j in range(inner // LANES):
            at = slice(j * LANES, (j + 1) * LANES)
            keys.append((rotated(new_k[:, at], new_cos, new_sin) * HD**-0.5).astype(BF16))
            queries.append(rotated(new_q[:, at], new_cos, new_sin).astype(BF16))
        key = jnp.concatenate(keys, axis=1).astype(F32)
        query = jnp.concatenate(queries, axis=1).astype(F32)
        value = new_v.astype(BF16).astype(F32)
        same = (
            lax.broadcasted_iota(jnp.int32, (inner, inner), 0) // HD
            == lax.broadcasted_iota(jnp.int32, (inner, inner), 1) // HD
        )
        product = query * key
        for h in range(heads):
            at = slice(h * HD, (h + 1) * HD)
            own_term[:, at] = jnp.sum(product[:, at], axis=-1, keepdims=True) * value[:, at]
        pick = lax.broadcasted_iota(jnp.int32, (HD, inner), 0) == lane_iota((HD, inner)) % HD
        for s in range(seqs):
            spread = jnp.where(pick, query[s : s + 1], 0.0).astype(BF16)
            q_spread[s] = jnp.dot(
                spread, jnp.where(same, 1.0, 0.0).astype(BF16), preferred_element_type=F32
            )

    def rs_copy(s, o):
        peer = lax.rem(sp + o, n_sp)
        return pltpu.make_async_remote_copy(
            stage.at[s, peer], landed.at[s, sp], rs_tx.at[s, peer], rs_rx.at[s, sp],
            device_id={"sp": peer}, device_id_type=MESH,
        )

    def finish(i):
        s, part = i // parts, i % parts
        where = pl.ds(pl.multiple_of(part * size, size), size)
        cosine, sine = cos_ref[where, :], sin_ref[where, :]
        lane = lane_iota((HD, LANES))
        for j in range(inner // LANES):
            at = slice(j * LANES, (j + 1) * LANES)
            key = (rotated(acc_k[i, :, at], cosine, sine) * HD**-0.5).astype(BF16)
            weighted = (key.astype(F32) * fade_ref[where, at]).astype(BF16)
            value = acc_v[i, :, at].astype(BF16)
            both = lax.dot_general(
                weighted, value, (((0,), (0,)), ((), ())), preferred_element_type=F32
            )
            state = jnp.where(lane < HD, both[:HD], both[HD:])
            sums[:, at] = jnp.where(part == 0, state, sums[:, at] + state)

        @pl.when(part == parts - 1)
        def _():
            scaled = sums[...] * rows_ref[0:1]
            read = jnp.sum(scaled * q_spread[s], axis=0, keepdims=True)
            for o in range(n_sp):
                stage[s, o, 0:keep] = scaled[o * keep : (o + 1) * keep]
                stage[s, o, keep : keep + 1] = read
            for o in range(1, n_sp):
                rs_copy(s, o).start()
            totals[s] = stage[s, sp]

    far = jnp.maximum(z, chips - 1 - z)

    def decode(i):
        d = i // (2 * pieces) + 1
        s = (i // 2) % pieces
        step = 2 * (i % 2) - 1
        c = z + step * d
        return d, s, step, c, (c >= 0) & (c < chips)

    def onward(step):
        nxt = z - step
        return nxt, (nxt >= 0) & (nxt < chips), (step + 1) // 2

    @pl.loop(0, 2 * pieces * (chips - 1))
    def _(i):
        d, s, step, c, valid = decode(i)
        nxt, pass_on, way = onward(step)

        @pl.when(valid)
        def _():
            @pl.when(s == 0)
            def _():
                n_arrived(2 * c + k)

                @pl.when(pass_on)
                def _():
                    n_copy(c, nfwd.at[way, c], 2 * nxt + k).start()

                n_copy(c, nshare.at[c], partner).start()

            x_arrived(2 * c + k, s)

            @pl.when(pass_on)
            def _():
                x_copy(c, s, fwd.at[way, c, s], 2 * nxt + k).start()

            x_copy(c, s, share.at[c, s], partner).start()
            add(2 * c + k, s, False)

            @pl.when(s == 0)
            def _():
                n_arrived(2 * c + 1 - k)

            x_arrived(2 * c + 1 - k, s)
            add(2 * c + 1 - k, s, False)

        last = (d == far) & (step == 1)

        @pl.when(last & (s == 0))
        def _():
            project_new()

        @pl.when(last)
        def _():
            finish(s)

    raws = []
    for s in range(seqs):
        for o in range(1, n_sp):
            src = lax.rem(sp + o, n_sp)
            pltpu.make_async_remote_copy(
                stage.at[s, src], landed.at[s, src], rs_tx.at[s, src], rs_rx.at[s, src],
                device_id={"sp": src}, device_id_type=MESH,
            ).wait_recv()
        total = None
        for j in range(n_sp):
            term = jnp.where(sp == j, totals[s], landed[s, j])
            total = term if total is None else total + term
        kept = total[0:keep].astype(BF16)
        for h in range(heads):
            state_out[s, h] = kept[:, h * HD : (h + 1) * HD]
        raws.append(total[keep : keep + 1] * rows_ref[1:2] + own_term[s : s + 1])
    raw = jnp.concatenate(raws, axis=0)
    for h in range(heads):
        at = slice(h * HD, (h + 1) * HD)
        head = raw[:, at]
        centered = head - jnp.mean(head, axis=-1, keepdims=True)
        spread = jnp.mean(centered * centered, axis=-1, keepdims=True)
        read_out[:, at] = (centered * lax.rsqrt(spread + 1e-05)).astype(BF16)

    @pl.when(z < chips - 1)
    def _():
        n_up.wait_send()

    @pl.when(z > 0)
    def _():
        n_down.wait_send()

    n_side.wait_send()
    for s in range(seqs):
        for o in range(1, n_sp):
            rs_copy(s, o).wait_send()
    for s in range(pieces):
        @pl.when(z < chips - 1)
        def _(s=s):
            x_copy(z, s, fwd.at[0, z, s], tp + 2).wait_send()

        @pl.when(z > 0)
        def _(s=s):
            x_copy(z, s, fwd.at[1, z, s], tp - 2).wait_send()

        x_copy(z, s, share.at[z, s], partner).wait_send()

    @pl.loop(0, 2 * pieces * (chips - 1))
    def _(i):
        d, s, step, c, valid = decode(i)
        nxt, pass_on, way = onward(step)

        @pl.when(valid)
        def _():
            @pl.when(s == 0)
            def _():
                @pl.when(pass_on)
                def _():
                    n_copy(c, nfwd.at[way, c], 2 * nxt + k).wait_send()

                n_copy(c, nshare.at[c], partner).wait_send()

            @pl.when(pass_on)
            def _():
                x_copy(c, s, fwd.at[way, c, s], 2 * nxt + k).wait_send()

            x_copy(c, s, share.at[c, s], partner).wait_send()


def one_of(n, values):
    total = 0
    for k, value in enumerate(values):
        if value:
            total = total + (n == k).astype(jnp.int32) * value
    return total


def middle_order(main, moved):
    near = [(0, i) for i in main]
    far = [(2, i) for i in moved + main]
    order = [(kind, i) for i in moved for kind in (0, 1)]
    order += [(1, i) for i in main]
    for at in range(max(len(near), len(far))):
        order += far[at : at + 1] + near[at : at + 1]
    return order


def moved_kernel(
    n_sp, n_tp, parts,
    tokens, fresh, wq_hbm, wk_hbm, wv_hbm, inverse_ref, decay_ref,
    state_out, read_out,
    x, xc, nx, wq, wk, wv, we, acc_k, acc_v, acc_c, cos_ref, sin_ref, fade_ref, rows_ref,
    q_spread, own_term, sums, stage, landed, totals, hint, hint_in, stage_c, landed_c,
    load_sem, weight_sem, rx, rn, ry, rw, tx, hint_rx, rs_rx, c_rx, ready,
):
    seqs, span, feat = tokens.shape
    inner = wk.shape[1]
    heads = inner // HD
    half = inner // 2
    chunks = half // LANES
    chips = n_tp // 2
    pieces = seqs * parts
    size = span // parts
    keep = HD // n_sp
    groups = n_tp // 2
    moved_seq = seqs - 1
    to_mate_tx, to_other_tx, share_tx, n_tx, n_share_tx, y_tx, y_share_tx, w_tx, w_pass_tx = range(9)
    hint_tx, rs_tx, c_tx = range(9, 12)
    main = list(range(moved_seq * parts))
    moved = list(range(moved_seq * parts, pieces))
    sp = lax.axis_index("sp")
    tp = lax.axis_index("tp")
    z, k = tp // 2, tp % 2
    row_y, row_x = sp // 2, sp % 2
    x_peer = sp + 1 - 2 * row_x
    y_peer = sp + 2 - 4 * row_y
    MESH = pl.DeviceIdType.MESH
    end_int = (z == 0).astype(jnp.int32) + (z == chips - 1).astype(jnp.int32)
    end = end_int > 0
    mid = end_int == 0
    partner = z * 2 + 1 - k
    mate = z + 1 - 2 * (z % 2)
    mate_tp = 2 * mate + k
    other = chips - 1 - z
    other_tp = 2 * other + k
    second = end_int * (chips - 1 - mate) + (1 - end_int) * (chips - 1 - z)
    third = end_int * (chips - 1 - z) + (1 - end_int) * (chips - 1 - mate)

    own_loads = {
        s: pltpu.make_async_copy(
            tokens.at[s // parts, pl.ds(s % parts * size, size)], x.at[tp, s], load_sem.at[s]
        )
        for s in range(pieces)
    }
    new_load = pltpu.make_async_copy(fresh, nx.at[tp], load_sem.at[pieces])
    new_load.start()
    for s in moved + main:
        own_loads[s].start()
    weight_loads = [
        pltpu.make_async_copy(a, b, weight_sem.at[i])
        for i, (a, b) in enumerate(((wk_hbm, wk), (wv_hbm, wv), (wq_hbm, wq)))
    ]

    barrier = pltpu.get_barrier_semaphore()
    for target in ({"tp": partner}, {"tp": mate_tp}, {"sp": x_peer}, {"sp": y_peer}):
        pl.semaphore_signal(barrier, inc=1, device_id=target, device_id_type=MESH)

    @pl.when(mid)
    def _():
        pl.semaphore_signal(barrier, inc=1, device_id={"tp": other_tp}, device_id_type=MESH)

    pl.semaphore_wait(barrier, 5 - end_int)
    for target in ({"sp": x_peer}, {"sp": y_peer}):
        pl.semaphore_signal(ready.at[0], inc=1, device_id=target, device_id_type=MESH)

    def remote(source, dest, send, recv, target):
        return pltpu.make_async_remote_copy(
            source, dest, send, recv, device_id=target, device_id_type=MESH
        )

    def sent(ref, kind):
        remote(ref, ref, tx.at[kind], hint_rx.at[0], {"tp": partner}).wait_send()

    def arrived(ref, sem):
        remote(ref, ref, tx.at[0], sem, {"tp": partner}).wait_recv()

    def x_copy(c, s, kind, target):
        here = x.at[2 * c + k, s]
        return remote(here, here, tx.at[kind], rx.at[2 * c + k, s], {"tp": target})

    def to_mate(c, s):
        return x_copy(c, s, to_mate_tx, mate_tp)

    def to_other(c, s):
        return x_copy(c, s, to_other_tx, other_tp)

    def to_partner(c, s):
        return x_copy(c, s, share_tx, partner)

    def x_arrived(p, s):
        arrived(x.at[p, s], rx.at[p, s])

    def y_send(c, j):
        p = 2 * c + k
        return remote(
            x.at[p, moved[0] + j], xc.at[p, j], tx.at[y_tx], ry.at[c * parts + j], {"sp": y_peer}
        )

    def y_share(c, j):
        here = xc.at[2 * c + k, j]
        late = (c == third).astype(jnp.int32)
        return remote(
            here, here, tx.at[y_share_tx], ry.at[chips * parts + late], {"tp": partner}
        )

    def w_rows(p):
        return pl.ds(pl.multiple_of(p * feat, feat), feat)

    def w_cols(cc):
        return pl.ds(pl.multiple_of(row_y * half + cc * LANES, LANES), LANES)

    def w_part(g, r):
        if r is None:
            return w_rows(row_x * groups + g)
        start = (row_x * groups + g) * feat + r * (feat // 2)
        return pl.ds(pl.multiple_of(start, feat // 2), feat // 2)

    def w_place(cc, g, kv, r):
        return we.at[cc, w_part(g, r), pl.ds(kv * LANES, LANES)]

    def w_sem(cc, g, kv, r):
        if r is None:
            return rw.at[cc * groups + g]
        return rw.at[groups + 1 + 4 * (g - 1) + 2 * r + kv]

    def w_peer_sem(cc, g):
        return rw.at[5 * groups - 3 + cc * (1 + g)]

    def w_send(cc, g, kv, r=None):
        mine = (wk, wv)[kv].at[w_part(g, r), w_cols(cc)]
        return remote(
            mine, w_place(cc, g, kv, r), tx.at[w_tx], w_sem(cc, g, kv, r), {"tp": mate_tp}
        )

    def w_pass(cc, g, kv, r=None):
        here = w_place(cc, g, kv, r)
        return remote(here, here, tx.at[w_pass_tx], w_peer_sem(cc, g), {"sp": x_peer})

    def n_copy(c, kind, sem, target):
        here = nx.at[2 * c + k]
        return remote(here, here, tx.at[kind], sem, {"tp": target})

    def n_to(c, target):
        n_copy(c, n_tx, rn.at[c], target).start()

    def n_share(c):
        n_copy(c, n_share_tx, rn.at[chips], partner).start()

    def n_arrived(c):
        arrived(nx.at[2 * c + k], rn.at[c])

    hint_copy = remote(hint, hint_in, tx.at[hint_tx], hint_rx.at[0], {"tp": mate_tp})

    new_load.wait()
    n_to(z, mate_tp)
    n_share(z)

    @pl.when(mid)
    def _():
        n_to(z, other_tp)

    for s in moved + main:
        own_loads[s].wait()

    def send_moved(j):
        s = moved[j]

        @pl.when(mid)
        def _():
            to_other(z, s).start()
            y_send(z, j).start()
            to_partner(z, s).start()

        @pl.when(end)
        def _():
            to_mate(z, s).start()

    send_moved(0)
    to_partner(z, main[0]).start()

    @pl.when(mid)
    def _():
        to_mate(z, main[0]).start()

    for copy in weight_loads:
        copy.start()

    @pl.when(mid)
    def _():
        n_arrived(mate)
        n_to(mate, other_tp)
        n_share(mate)
        n_arrived(other)
        n_to(other, mate_tp)
        n_share(other)

    for j in range(1, parts):
        send_moved(j)
    for s in main[1:]:
        to_partner(z, s).start()

    @pl.when(mid)
    def _():
        for s in main[1:2]:
            to_mate(z, s).start()
        for s in main:
            to_other(z, s).start()

    row = lax.broadcasted_iota(jnp.int32, (span, LANES), 0)
    within = lane_iota((1, LANES)) % HD
    first_half = jnp.where(within < HD // 2, -1.0, 1.0).astype(F32)
    inverse = inverse_ref[...]

    def tables(slot, column):
        angles = (column * span + row).astype(F32) * inverse
        cos_ref[slot] = jnp.cos(angles)
        sin_ref[slot] = jnp.sin(angles) * first_half

    for copy in weight_loads[:2]:
        copy.wait()

    @pl.when(end)
    def _():
        for cc, g in [(0, g) for g in range(groups)] + [(1, 0)]:
            for kv in range(2):
                w_send(cc, g, kv).start()

    tables(0, sp)

    @pl.when(mid)
    def _():
        tables(1, y_peer)

    new_angles = jnp.full((NEW_ROWS, LANES), n_sp * span, F32) * inverse
    new_cos = jnp.cos(new_angles)
    new_sin = jnp.sin(new_angles) * first_half
    head_of = lane_iota((1, inner)) // HD
    rate = jnp.zeros((1, inner), F32)
    for h in range(heads):
        rate = jnp.where(head_of == h, decay_ref[h], rate)
    to_end = (span - 1 - lax.broadcasted_iota(jnp.int32, (span, 1), 0)).astype(F32)
    fade_ref[...] = jnp.exp(to_end * rate)
    rows_ref[0:1] = jnp.exp(rate * (span * (n_sp - 1 - sp)).astype(F32))
    rows_ref[1:2] = jnp.exp(rate)
    hint[...] = jnp.zeros(hint.shape, F32)
    hint[1:2] = rate
    weight_loads[2].wait()

    def add(p, s, fresh_total):
        block = x[p, s]
        where = w_rows(p)
        part_k = jnp.dot(block, wk[where, :], preferred_element_type=F32)
        part_v = jnp.dot(block, wv[where, :], preferred_element_type=F32)
        if fresh_total:
            acc_k[s] = part_k
            acc_v[s] = part_v
        else:
            acc_k[s] += part_k
            acc_v[s] += part_v

    same = (
        lax.broadcasted_iota(jnp.int32, (inner, inner), 0) // HD
        == lax.broadcasted_iota(jnp.int32, (inner, inner), 1) // HD
    )
    pick = lax.broadcasted_iota(jnp.int32, (HD, inner), 0) == lane_iota((HD, inner)) % HD

    @pl.when(mid)
    def _():
        n_arrived(third)
        n_to(third, mate_tp)
        n_share(third)
        for s in main[2:]:
            to_mate(z, s).start()

    own_pieces = end_int * len(main) + (1 - end_int) * pieces

    @pl.loop(0, pieces)
    def _(i):
        s = lax.rem(i + (1 - end_int) * len(main), pieces)

        @pl.when(i < own_pieces)
        def _():
            add(tp, s, True)

        @pl.when(i < own_pieces)
        def _():
            x_arrived(partner, s)
            add(partner, s, False)

    @pl.when(end)
    def _():
        for c in (mate, second, third):
            n_arrived(c)
            n_share(c)

    arrived(nx.at[pl.ds(0, chips)], rn.at[chips])

    def project_new():
        def piece(p, totals):
            where = w_rows(p)
            block = jnp.concatenate(
                [nx[p].astype(F32), jnp.zeros((NEW_ROWS - seqs, feat), F32)], axis=0
            ).astype(BF16)
            return tuple(
                t + jnp.dot(block, w[where, :], preferred_element_type=F32)
                for t, w in zip(totals, (wk, wv, wq))
            )

        zero = jnp.zeros((NEW_ROWS, inner), F32)
        new_k, new_v, new_q = lax.fori_loop(0, n_tp, piece, (zero, zero, zero))
        keys, queries = [], []
        for j in range(inner // LANES):
            at = slice(j * LANES, (j + 1) * LANES)
            keys.append((rotated(new_k[:, at], new_cos, new_sin) * HD**-0.5).astype(BF16))
            queries.append(rotated(new_q[:, at], new_cos, new_sin).astype(BF16))
        key = jnp.concatenate(keys, axis=1).astype(F32)
        query = jnp.concatenate(queries, axis=1).astype(F32)
        value = new_v.astype(BF16).astype(F32)
        product = query * key
        for h in range(heads):
            at = slice(h * HD, (h + 1) * HD)
            own_term[:, at] = jnp.sum(product[:, at], axis=-1, keepdims=True) * value[:, at]
        hint[0:1] = query[moved_seq : moved_seq + 1]
        for s in range(seqs):
            spread = jnp.where(pick, query[s : s + 1], 0.0).astype(BF16)
            q_spread[s] = jnp.dot(
                spread, jnp.where(same, 1.0, 0.0).astype(BF16), preferred_element_type=F32
            )

    project_new()

    @pl.when(end)
    def _():
        hint_copy.start()
        for s in main:
            to_mate(z, s).start()
        for g in range(1, groups):
            for r in range(2):
                for kv in range(2):
                    w_send(1, g, kv, r).start()

    def rs_copy(s, o):
        peer = lax.rem(sp + o, n_sp)
        return remote(
            stage.at[s, peer], landed.at[s, sp], tx.at[rs_tx], rs_rx.at[s], {"sp": peer}
        )

    pl.semaphore_wait(ready.at[0], 2)
    pl.semaphore_signal(ready.at[1], inc=1, device_id={"sp": x_peer}, device_id_type=MESH)

    def y_half(s):
        return remote(
            stage.at[s, pl.ds(2 - 2 * row_y, 2)], landed.at[s, pl.ds(0, 2)],
            tx.at[rs_tx], rs_rx.at[s], {"sp": y_peer},
        )

    def x_half(s):
        return remote(
            stage.at[s, x_peer], landed.at[s, 2], tx.at[rs_tx], rs_rx.at[seqs + s], {"sp": x_peer}
        )

    def outer(weighted, value):
        both = lax.dot_general(
            weighted, value, (((0,), (0,)), ((), ())), preferred_element_type=F32
        )
        return jnp.where(lane_iota((HD, LANES)) < HD, both[:HD], both[HD:])

    def finish(i):
        s, part = i // parts, i % parts
        where = pl.ds(pl.multiple_of(part * size, size), size)
        cosine, sine = cos_ref[0, where, :], sin_ref[0, where, :]
        for j in range(inner // LANES):
            at = slice(j * LANES, (j + 1) * LANES)
            key = (rotated(acc_k[i, :, at], cosine, sine) * HD**-0.5).astype(BF16)
            weighted = (key.astype(F32) * fade_ref[where, at]).astype(BF16)
            value = acc_v[i, :, at].astype(BF16)
            state = outer(weighted, value)
            sums[:, at] = jnp.where(part == 0, state, sums[:, at] + state)

        @pl.when(part == parts - 1)
        def _():
            scaled = sums[...] * rows_ref[0:1]
            read = jnp.sum(scaled * q_spread[s], axis=0, keepdims=True)
            for o in range(n_sp):
                stage[s, o, 0:keep] = scaled[o * keep : (o + 1) * keep]
                stage[s, o, keep : keep + 1] = read
            totals[s] = stage[s, sp]

            @pl.when(end | (s == moved_seq))
            def _():
                for o in range(1, n_sp):
                    rs_copy(s, o).start()

            @pl.when(mid & (s < moved_seq))
            def _():
                y_half(s).start()

    def c_add(cc, p, fresh_total):
        where = w_rows(p)
        for t in range(parts):
            for side, block in ((0, x[p, moved[0] + t]), (1, xc[p, t])):
                both = jnp.dot(block, we[cc, where, :], preferred_element_type=F32)
                if fresh_total:
                    acc_c[side, t] = both
                else:
                    acc_c[side, t] += both

    def c_copy(cc, o):
        return remote(
            stage_c.at[cc, o], landed_c.at[cc, sp], tx.at[c_tx], c_rx.at[cc],
            {"sp": o, "tp": mate_tp},
        )

    def c_finish(cc):
        pair_rate = hint_in[1:2, w_cols(cc)]
        query = hint_in[0:1, w_cols(cc)]
        total = jnp.zeros((HD, LANES), F32)
        for side, column in ((0, sp), (1, y_peer)):
            state = jnp.zeros((HD, LANES), F32)
            for t in range(parts):
                at = slice(t * size, (t + 1) * size)
                key = (
                    rotated(acc_c[side, t, :, :LANES], cos_ref[side, at], sin_ref[side, at])
                    * HD**-0.5
                ).astype(BF16)
                fade = jnp.exp(to_end[at] * pair_rate)
                weighted = (key.astype(F32) * fade).astype(BF16)
                state = state + outer(weighted, acc_c[side, t, :, LANES:].astype(BF16))
            total = total + state * jnp.exp(
                pair_rate * (span * (n_sp - 1 - column)).astype(F32)
            )
        spread = jnp.where(pick[:, :LANES], query, 0.0).astype(BF16)
        spread = jnp.dot(
            spread, jnp.where(same[:LANES, :LANES], 1.0, 0.0).astype(BF16),
            preferred_element_type=F32,
        )
        read = jnp.sum(total * spread, axis=0, keepdims=True)
        for o in range(n_sp):
            stage_c[cc, o, 0:keep] = total[o * keep : (o + 1) * keep]
            stage_c[cc, o, keep : keep + 1] = read
        for o in range(n_sp):
            c_copy(cc, o).start()

    order = middle_order(main, moved)
    steps = end_int * (len(main) * (chips - 1)) + (1 - end_int) * len(order)

    def decode(n):
        kind = end_int * (n // len(main)) + (1 - end_int) * one_of(n, [o[0] for o in order])
        s = end_int * (n % len(main)) + (1 - end_int) * one_of(n, [o[1] for o in order])
        c = (
            (kind == 0).astype(jnp.int32) * mate
            + (kind == 1).astype(jnp.int32) * second
            + (kind == 2).astype(jnp.int32) * third
        )
        return kind, c, s

    first_w = 2 * len(moved) + 1
    c_at = len(order) - 4
    last = len(order) - 1

    def w_pair(cc, g):
        arrived(we.at[cc, w_part(g, None)], w_sem(cc, g, 0, None))
        for kv in range(2):
            w_pass(cc, g, kv).start()

    def w_relay(g, r, kv):
        arrived(w_place(1, g, kv, r), w_sem(1, g, kv, r))
        w_pass(1, g, kv, r).start()

    def w_own(cc, g, fresh_total=False):
        c_add(cc, row_x * groups + g, fresh_total)

    def w_peer(cc, g):
        p = (1 - row_x) * groups + g
        arrived(we.at[cc, w_rows(p)], w_peer_sem(cc, g))
        c_add(cc, p, False)

    def y_pass(c, j):
        arrived(xc.at[2 * c + k, j], ry.at[c * parts + j])
        y_share(c, j).start()

    @pl.loop(0, len(order) + 1)
    def _(n):
        kind, c, s = decode(n)
        is_moved = s >= moved[0]

        @pl.when(mid & (n == last - 1))
        def _():
            w_relay(1, 0, 1)

        @pl.when(mid & (n == last))
        def _():
            w_relay(1, 1, 1)

        @pl.when(n < steps)
        def _():
            x_arrived(2 * c + k, s)

            @pl.when(mid & (kind == 0))
            def _():
                to_other(c, s).start()

            @pl.when(mid & (kind > 0) & (s < moved[0]))
            def _():
                to_mate(c, s).start()

            @pl.when(mid & is_moved)
            def _():
                y_send(c, s - moved[0]).start()

            to_partner(c, s).start()

        @pl.when(mid & (n == last - 2))
        def _():
            w_relay(1, 0, 0)

        @pl.when(mid & (n == last - 1))
        def _():
            w_relay(1, 1, 0)

        @pl.when(mid & (n == last))
        def _():
            w_relay(2, 0, 0)

        @pl.when(mid & (n >= first_w) & (n < first_w + groups))
        def _():
            w_pair(0, n - first_w)

        @pl.when(mid & (n == first_w + groups))
        def _():
            w_pair(1, 0)

        @pl.when(mid & (n >= 3) & (n < 3 + parts))
        def _():
            y_pass(z, n - 3)

        @pl.when(mid & (n >= 6) & (n < 6 + 2 * parts))
        def _():
            m = n - 6
            y_pass((m % 2) * second + (1 - m % 2) * mate, m // 2)

        @pl.when(mid & (n >= c_at - parts) & (n < c_at))
        def _():
            y_pass(third, n - (c_at - parts))

        @pl.when(n < steps)
        def _():
            add(2 * c + k, s, False)

        @pl.when(mid & (n == last))
        def _():
            w_relay(2, 0, 1)

        kind_b, c_b, s_b = decode(n - 1)

        @pl.when((n >= 1) & (n <= steps))
        def _():
            x_arrived(2 * c_b + 1 - k, s_b)
            add(2 * c_b + 1 - k, s_b, False)

            @pl.when(mid & (n == last + 1))
            def _():
                w_relay(2, 1, 1)

            @pl.when(kind_b == 2)
            def _():
                finish(s_b)

        @pl.when(mid & (n == last))
        def _():
            w_relay(2, 1, 0)

        early = n - (c_at - 5)

        @pl.when(mid & (early == 0))
        def _():
            arrived(xc.at[pl.ds(0, chips - 1)], ry.at[chips * parts])
            arrived(we.at[0, pl.ds(0, groups * feat)], w_peer_sem(0, 0))
            acc_c[...] = jnp.zeros(acc_c.shape, F32)

        @pl.when(mid & (early >= 0) & (early < 6))
        def _():
            turn = early // 2
            cx = (
                (turn == 0).astype(jnp.int32) * z
                + (turn == 1).astype(jnp.int32) * mate
                + (turn == 2).astype(jnp.int32) * second
            )
            c_add(0, 2 * cx + early % 2, False)

        @pl.when(mid & (n == c_at))
        def _():
            arrived(xc.at[0], ry.at[chips * parts + 1])

            @pl.loop(0, 2)
            def _(m):
                c_add(0, 2 * third + m, False)

            hint_copy.wait_recv()
            pl.semaphore_wait(ready.at[1], 1)
            c_finish(0)

    @pl.when(mid)
    def _():
        w_own(1, 0, True)
        w_peer(1, 0)
        w_relay(3, 0, 0)
        w_own(1, 1)
        w_peer(1, 1)
        w_relay(3, 0, 1)
        w_own(1, 2)
        w_relay(3, 1, 0)
        w_relay(3, 1, 1)
        w_peer(1, 2)
        w_own(1, 3)
        for s in range(moved_seq):
            arrived(landed.at[s, pl.ds(0, 2)], rs_rx.at[s])
            for side in range(2):
                stage[s, 2 * row_y + side] += landed[s, side]
            x_half(s).start()
        w_peer(1, 3)
        c_finish(1)

    def gather(s):
        arrived(landed.at[s, pl.ds(0, n_sp - 1)], rs_rx.at[s])
        total = None
        for j in range(n_sp):
            term = jnp.where(sp == j, totals[s], landed[s, j])
            total = term if total is None else total + term
        totals[s] = total

    sent(nx.at[pl.ds(0, chips)], n_share_tx)

    @pl.when(end)
    def _():
        pl.semaphore_wait(ready.at[1], 1)
        sent(nx.at[0], n_tx)
        sent(hint, hint_tx)
        sent(x.at[0], to_mate_tx)
        sent(x.at[pl.ds(0, chips), pl.ds(0, len(main))], share_tx)
        sent(we.at[pl.ds(0, chunks), pl.ds(0, groups * feat)], w_tx)
        sent(stage.at[pl.ds(0, moved_seq), pl.ds(0, n_sp - 1)], rs_tx)

    @pl.when(mid)
    def _():
        sent(nx.at[pl.ds(0, 5)], n_tx)
        sent(x.at[pl.ds(0, chips - 1), pl.ds(0, len(main))], to_mate_tx)
        sent(x.at[pl.ds(0, 2)], to_other_tx)
        sent(x.at[pl.ds(0, chips)], share_tx)
        sent(xc.at[pl.ds(0, chips)], y_tx)
        sent(xc.at[pl.ds(0, chips)], y_share_tx)
        sent(we.at[pl.ds(0, chunks), pl.ds(0, groups * feat)], w_pass_tx)
        sent(stage.at[:, pl.ds(0, n_sp - 1)], rs_tx)

    @pl.when(mid)
    def _():
        for s in range(moved_seq):
            arrived(landed.at[s, 2], rs_rx.at[seqs + s])
            totals[s] = stage[s, sp] + landed[s, 2]
        gather(moved_seq)

    @pl.when(end)
    def _():
        for s in range(moved_seq):
            gather(s)
        for cc in range(chunks):
            arrived(landed_c.at[cc], c_rx.at[cc])
            for side in range(2):
                at = slice(side * half + cc * LANES, side * half + (cc + 1) * LANES)
                totals[moved_seq, :, at] = landed_c[cc, 2 * side] + landed_c[cc, 2 * side + 1]

    raws = []
    for s in range(seqs):
        total = totals[s]
        kept = total[0:keep].astype(BF16)
        for h in range(heads):
            state_out[s, h] = kept[:, h * HD : (h + 1) * HD]
        raws.append(total[keep : keep + 1] * rows_ref[1:2] + own_term[s : s + 1])
    raw = jnp.concatenate(raws, axis=0)
    for h in range(heads):
        at = slice(h * HD, (h + 1) * HD)
        head = raw[:, at]
        centered = head - jnp.mean(head, axis=-1, keepdims=True)
        spread = jnp.mean(centered * centered, axis=-1, keepdims=True)
        read_out[:, at] = (centered * lax.rsqrt(spread + 1e-05)).astype(BF16)

    @pl.when(mid)
    def _():
        sent(stage_c, c_tx)


def solution(mesh):
    n_sp, n_tp = mesh.shape["sp"], mesh.shape["tp"]

    def body(tokens, new_token, query_weight, key_weight, value_weight, log_decay):
        seqs, span, feat = tokens.shape
        width, inner = key_weight.shape
        heads = inner // HD
        keep = HD // n_sp
        rows = -(-(keep + 1) // 8) * 8
        chips = n_tp // 2
        half = HD // 2
        parts = max(1, 8 // chips)
        pieces = seqs * parts
        size = span // parts
        inverse = np.float32(10000.0) ** (-np.arange(half, dtype=np.float32) / half)
        inverse = jnp.asarray(np.tile(inverse.astype(np.float32), LANES // half)[None])
        anywhere = pl.BlockSpec(memory_space=pl.ANY)
        vmem = pl.BlockSpec(memory_space=pltpu.VMEM)
        dma = pltpu.SemaphoreType.DMA
        moves = chips == 4 and n_sp == 4 and seqs > 1 and inner == 4 * LANES
        tokens_in = [
            pltpu.VMEM((n_tp, pieces, size, feat), BF16),
            pltpu.VMEM((n_tp, seqs, feat), BF16),
        ]
        weights_in = [pltpu.VMEM((width, inner), BF16)] * 3
        totals = [pltpu.VMEM((pieces, size, inner), F32)] * 2
        ends = [
            pltpu.VMEM((8, inner), F32),
            pltpu.VMEM((seqs, HD, inner), F32),
            pltpu.VMEM((NEW_ROWS, inner), F32),
            pltpu.VMEM((HD, inner), F32),
            pltpu.VMEM((seqs, n_sp, rows, inner), F32),
            pltpu.VMEM((seqs, n_sp, rows, inner), F32),
            pltpu.VMEM((seqs, rows, inner), F32),
        ]
        if moves:
            chunks = inner // 2 // LANES
            groups = n_tp // 2
            call = moved_kernel
            scratch = (
                tokens_in[:1]
                + [pltpu.VMEM((n_tp, parts, size, feat), BF16)]
                + tokens_in[1:]
                + weights_in
                + [pltpu.VMEM((chunks, width, 2 * LANES), BF16)]
                + totals
                + [
                    pltpu.VMEM((2, parts, size, 2 * LANES), F32),
                    pltpu.VMEM((2, span, LANES), F32),
                    pltpu.VMEM((2, span, LANES), F32),
                    pltpu.VMEM((span, inner), F32),
                ]
                + ends
                + [
                    pltpu.VMEM((8, inner), F32),
                    pltpu.VMEM((8, inner), F32),
                    pltpu.VMEM((chunks, n_sp, rows, LANES), F32),
                    pltpu.VMEM((chunks, n_sp, rows, LANES), F32),
                    dma((pieces + 1,)),
                    dma((3,)),
                    dma((n_tp, pieces)),
                    dma((chips + 1,)),
                    dma((chips * parts + 2,)),
                    dma((6 * groups - 2,)),
                    dma((12,)),
                    dma((1,)),
                    dma((2 * seqs,)),
                    dma((chunks,)),
                    pltpu.SemaphoreType.REGULAR((2,)),
                ]
            )
        else:
            call = kernel
            scratch = (
                tokens_in
                + weights_in
                + totals
                + [
                    pltpu.VMEM((span, LANES), F32),
                    pltpu.VMEM((span, LANES), F32),
                    pltpu.VMEM((span, inner), F32),
                ]
                + ends
                + [
                    dma((pieces + 1,)),
                    dma((3,)),
                    dma((n_tp, pieces)),
                    dma((n_tp,)),
                    dma((2, chips, pieces)),
                    dma((chips, pieces)),
                    dma((2, chips)),
                    dma((chips,)),
                    dma((seqs, n_sp)),
                    dma((seqs, n_sp)),
                ]
            )
        return pl.pallas_call(
            functools.partial(call, n_sp, n_tp, parts),
            out_shape=(
                jax.ShapeDtypeStruct((seqs, heads, keep, HD), BF16),
                jax.ShapeDtypeStruct((seqs, inner), BF16),
            ),
            in_specs=[anywhere] * 5 + [vmem, pl.BlockSpec(memory_space=pltpu.SMEM)],
            out_specs=(vmem, vmem),
            scratch_shapes=scratch,
            compiler_params=pltpu.CompilerParams(
                collective_id=0, has_side_effects=True, vmem_limit_bytes=60 * 1024 * 1024
            ),
            name="retention",
        )(tokens, new_token.reshape(seqs, feat), query_weight, key_weight, value_weight, inverse, log_decay)

    return jax.shard_map(
        body,
        mesh=mesh,
        in_specs=(
            P(None, "sp", "tp"),
            P(None, None, "tp"),
            P(None, "tp"),
            P(None, "tp"),
            P(None, "tp"),
            P("tp"),
        ),
        out_specs=(P(None, "tp", "sp", None), P(None, "tp")),
        check_vma=False,
    )
```

```python
import functools

import jax
import jax.numpy as jnp
import numpy as np
from jax import lax
from jax.experimental import pallas as pl
from jax.experimental.pallas import tpu as pltpu
from jax.sharding import PartitionSpec as P

HD = 64
LANES = 128
NEW_ROWS = 8
F32 = jnp.float32
BF16 = jnp.bfloat16


def inverse_angles():
    half = HD // 2
    return np.float32(10000.0) ** (-np.arange(half, dtype=np.float32) / half)


def lane_iota(shape):
    return lax.broadcasted_iota(jnp.int32, shape, len(shape) - 1)


def rotated(block, cosine, sine):
    half = HD // 2
    low = lane_iota(block.shape) % HD < half
    swapped = jnp.where(
        low, pltpu.roll(block, LANES - half, 1), pltpu.roll(block, half, 1)
    )
    return block * cosine + swapped * sine


def kernel(
    n_sp, n_tp, parts,
    tokens, fresh, wq_hbm, wk_hbm, wv_hbm, inverse_ref, decay_ref,
    state_out, read_out,
    x, nx, wq, wk, wv, acc_k, acc_v, cos_ref, sin_ref, fade_ref, rows_ref,
    q_spread, own_term, sums, stage, landed, totals,
    load_sem, weight_sem, rx, rn, fwd, share, nfwd, nshare, rs_tx, rs_rx,
):
    seqs, span, feat = tokens.shape
    inner = wk.shape[1]
    heads = inner // HD
    chips = n_tp // 2
    pieces = seqs * parts
    size = span // parts
    keep = HD // n_sp
    sp = lax.axis_index("sp")
    tp = lax.axis_index("tp")
    z, k = tp // 2, tp % 2
    MESH = pl.DeviceIdType.MESH

    def to_tp(index):
        return {"tp": index}

    partner = z * 2 + 1 - k
    own_loads = [
        pltpu.make_async_copy(
            tokens.at[s // parts, pl.ds(s % parts * size, size)], x.at[tp, s], load_sem.at[s]
        )
        for s in range(pieces)
    ]
    new_load = pltpu.make_async_copy(fresh, nx.at[tp], load_sem.at[pieces])
    new_load.start()
    for copy in own_loads:
        copy.start()
    weight_loads = [
        pltpu.make_async_copy(a, b, weight_sem.at[i])
        for i, (a, b) in enumerate(((wk_hbm, wk), (wv_hbm, wv), (wq_hbm, wq)))
    ]

    barrier = pltpu.get_barrier_semaphore()

    @pl.when(z > 0)
    def _():
        pl.semaphore_signal(barrier, inc=1, device_id=to_tp(tp - 2), device_id_type=MESH)

    @pl.when(z < chips - 1)
    def _():
        pl.semaphore_signal(barrier, inc=1, device_id=to_tp(tp + 2), device_id_type=MESH)

    pl.semaphore_signal(barrier, inc=1, device_id=to_tp(partner), device_id_type=MESH)
    for o in range(1, n_sp):
        pl.semaphore_signal(
            barrier, inc=1, device_id={"sp": lax.rem(sp + o, n_sp)}, device_id_type=MESH
        )
    pl.semaphore_wait(
        barrier, n_sp + (z > 0).astype(jnp.int32) + (z < chips - 1).astype(jnp.int32)
    )

    def x_copy(c, s, sem, target):
        p = 2 * c + k
        return pltpu.make_async_remote_copy(
            x.at[p, s], x.at[p, s], sem, rx.at[p, s], device_id=to_tp(target), device_id_type=MESH
        )

    def n_copy(c, sem, target):
        p = 2 * c + k
        return pltpu.make_async_remote_copy(
            nx.at[p], nx.at[p], sem, rn.at[p], device_id=to_tp(target), device_id_type=MESH
        )

    def x_arrived(p, s):
        pltpu.make_async_remote_copy(
            x.at[p, s], x.at[p, s], share.at[0, 0], rx.at[p, s],
            device_id=to_tp(partner), device_id_type=MESH,
        ).wait_recv()

    def n_arrived(p):
        pltpu.make_async_remote_copy(
            nx.at[p], nx.at[p], nshare.at[0], rn.at[p],
            device_id=to_tp(partner), device_id_type=MESH,
        ).wait_recv()

    new_load.wait()
    n_up = n_copy(z, nfwd.at[0, z], tp + 2)
    n_down = n_copy(z, nfwd.at[1, z], tp - 2)
    n_side = n_copy(z, nshare.at[z], partner)

    @pl.when(z < chips - 1)
    def _():
        n_up.start()

    @pl.when(z > 0)
    def _():
        n_down.start()

    n_side.start()
    for s in range(pieces):
        own_loads[s].wait()

        @pl.when(z < chips - 1)
        def _(s=s):
            x_copy(z, s, fwd.at[0, z, s], tp + 2).start()

        @pl.when(z > 0)
        def _(s=s):
            x_copy(z, s, fwd.at[1, z, s], tp - 2).start()

        x_copy(z, s, share.at[z, s], partner).start()

    for copy in weight_loads:
        copy.start()

    row = lax.broadcasted_iota(jnp.int32, (span, LANES), 0)
    within = lane_iota((1, LANES)) % HD
    first_half = jnp.where(within < HD // 2, -1.0, 1.0).astype(F32)
    inverse = inverse_ref[...]
    angles = (sp * span + row).astype(F32) * inverse
    cos_ref[...] = jnp.cos(angles)
    sin_ref[...] = jnp.sin(angles) * first_half
    new_angles = jnp.full((NEW_ROWS, LANES), n_sp * span, F32) * inverse
    new_cos = jnp.cos(new_angles)
    new_sin = jnp.sin(new_angles) * first_half
    head_of = lane_iota((1, inner)) // HD
    rate = jnp.zeros((1, inner), F32)
    for h in range(heads):
        rate = jnp.where(head_of == h, decay_ref[h], rate)
    to_end = (span - 1 - lax.broadcasted_iota(jnp.int32, (span, 1), 0)).astype(F32)
    fade_ref[...] = jnp.exp(to_end * rate)
    rows_ref[0:1] = jnp.exp(rate * (span * (n_sp - 1 - sp)).astype(F32))
    rows_ref[1:2] = jnp.exp(rate)

    for copy in weight_loads:
        copy.wait()

    def add(p, s, fresh_total):
        block = x[p, s]
        where = pl.ds(pl.multiple_of(p * feat, feat), feat)
        part_k = jnp.dot(block, wk[where, :], preferred_element_type=F32)
        part_v = jnp.dot(block, wv[where, :], preferred_element_type=F32)
        if fresh_total:
            acc_k[s] = part_k
            acc_v[s] = part_v
        else:
            acc_k[s] += part_k
            acc_v[s] += part_v

    @pl.loop(0, pieces)
    def _(s):
        add(tp, s, True)
        x_arrived(partner, s)
        add(partner, s, False)

    n_arrived(partner)

    def project_new():
        def piece(p, totals):
            where = pl.ds(pl.multiple_of(p * feat, feat), feat)
            block = jnp.concatenate(
                [nx[p].astype(F32), jnp.zeros((NEW_ROWS - seqs, feat), F32)], axis=0
            ).astype(BF16)
            return tuple(
                t + jnp.dot(block, w[where, :], preferred_element_type=F32)
                for t, w in zip(totals, (wk, wv, wq))
            )

        zero = jnp.zeros((NEW_ROWS, inner), F32)
        new_k, new_v, new_q = lax.fori_loop(0, n_tp, piece, (zero, zero, zero))
        keys, queries = [], []
        for j in range(inner // LANES):
            at = slice(j * LANES, (j + 1) * LANES)
            keys.append((rotated(new_k[:, at], new_cos, new_sin) * HD**-0.5).astype(BF16))
            queries.append(rotated(new_q[:, at], new_cos, new_sin).astype(BF16))
        key = jnp.concatenate(keys, axis=1).astype(F32)
        query = jnp.concatenate(queries, axis=1).astype(F32)
        value = new_v.astype(BF16).astype(F32)
        same = (
            lax.broadcasted_iota(jnp.int32, (inner, inner), 0) // HD
            == lax.broadcasted_iota(jnp.int32, (inner, inner), 1) // HD
        )
        product = query * key
        for h in range(heads):
            at = slice(h * HD, (h + 1) * HD)
            own_term[:, at] = jnp.sum(product[:, at], axis=-1, keepdims=True) * value[:, at]
        pick = lax.broadcasted_iota(jnp.int32, (HD, inner), 0) == lane_iota((HD, inner)) % HD
        for s in range(seqs):
            spread = jnp.where(pick, query[s : s + 1], 0.0).astype(BF16)
            q_spread[s] = jnp.dot(
                spread, jnp.where(same, 1.0, 0.0).astype(BF16), preferred_element_type=F32
            )

    def rs_copy(s, o):
        peer = lax.rem(sp + o, n_sp)
        return pltpu.make_async_remote_copy(
            stage.at[s, peer], landed.at[s, sp], rs_tx.at[s, peer], rs_rx.at[s, sp],
            device_id={"sp": peer}, device_id_type=MESH,
        )

    def finish(i):
        s, part = i // parts, i % parts
        where = pl.ds(pl.multiple_of(part * size, size), size)
        cosine, sine = cos_ref[where, :], sin_ref[where, :]
        lane = lane_iota((HD, LANES))
        for j in range(inner // LANES):
            at = slice(j * LANES, (j + 1) * LANES)
            key = (rotated(acc_k[i, :, at], cosine, sine) * HD**-0.5).astype(BF16)
            weighted = (key.astype(F32) * fade_ref[where, at]).astype(BF16)
            value = acc_v[i, :, at].astype(BF16)
            both = lax.dot_general(
                weighted, value, (((0,), (0,)), ((), ())), preferred_element_type=F32
            )
            state = jnp.where(lane < HD, both[:HD], both[HD:])
            sums[:, at] = jnp.where(part == 0, state, sums[:, at] + state)

        @pl.when(part == parts - 1)
        def _():
            scaled = sums[...] * rows_ref[0:1]
            read = jnp.sum(scaled * q_spread[s], axis=0, keepdims=True)
            for o in range(n_sp):
                stage[s, o, 0:keep] = scaled[o * keep : (o + 1) * keep]
                stage[s, o, keep : keep + 1] = read
            for o in range(1, n_sp):
                rs_copy(s, o).start()
            totals[s] = stage[s, sp]

    far = jnp.maximum(z, chips - 1 - z)

    def decode(i):
        d = i // (2 * pieces) + 1
        s = (i // 2) % pieces
        step = 2 * (i % 2) - 1
        c = z + step * d
        return d, s, step, c, (c >= 0) & (c < chips)

    def onward(step):
        nxt = z - step
        return nxt, (nxt >= 0) & (nxt < chips), (step + 1) // 2

    @pl.loop(0, 2 * pieces * (chips - 1))
    def _(i):
        d, s, step, c, valid = decode(i)
        nxt, pass_on, way = onward(step)

        @pl.when(valid)
        def _():
            @pl.when(s == 0)
            def _():
                n_arrived(2 * c + k)

                @pl.when(pass_on)
                def _():
                    n_copy(c, nfwd.at[way, c], 2 * nxt + k).start()

                n_copy(c, nshare.at[c], partner).start()

            x_arrived(2 * c + k, s)

            @pl.when(pass_on)
            def _():
                x_copy(c, s, fwd.at[way, c, s], 2 * nxt + k).start()

            x_copy(c, s, share.at[c, s], partner).start()
            add(2 * c + k, s, False)

            @pl.when(s == 0)
            def _():
                n_arrived(2 * c + 1 - k)

            x_arrived(2 * c + 1 - k, s)
            add(2 * c + 1 - k, s, False)

        last = (d == far) & (step == 1)

        @pl.when(last & (s == 0))
        def _():
            project_new()

        @pl.when(last)
        def _():
            finish(s)

    raws = []
    for s in range(seqs):
        for o in range(1, n_sp):
            src = lax.rem(sp + o, n_sp)
            pltpu.make_async_remote_copy(
                stage.at[s, src], landed.at[s, src], rs_tx.at[s, src], rs_rx.at[s, src],
                device_id={"sp": src}, device_id_type=MESH,
            ).wait_recv()
        total = None
        for j in range(n_sp):
            term = jnp.where(sp == j, totals[s], landed[s, j])
            total = term if total is None else total + term
        kept = total[0:keep].astype(BF16)
        for h in range(heads):
            state_out[s, h] = kept[:, h * HD : (h + 1) * HD]
        raws.append(total[keep : keep + 1] * rows_ref[1:2] + own_term[s : s + 1])
    raw = jnp.concatenate(raws, axis=0)
    for h in range(heads):
        at = slice(h * HD, (h + 1) * HD)
        head = raw[:, at]
        centered = head - jnp.mean(head, axis=-1, keepdims=True)
        spread = jnp.mean(centered * centered, axis=-1, keepdims=True)
        read_out[:, at] = (centered * lax.rsqrt(spread + 1e-05)).astype(BF16)

    @pl.when(z < chips - 1)
    def _():
        n_up.wait_send()

    @pl.when(z > 0)
    def _():
        n_down.wait_send()

    n_side.wait_send()
    for s in range(seqs):
        for o in range(1, n_sp):
            rs_copy(s, o).wait_send()
    for s in range(pieces):
        @pl.when(z < chips - 1)
        def _(s=s):
            x_copy(z, s, fwd.at[0, z, s], tp + 2).wait_send()

        @pl.when(z > 0)
        def _(s=s):
            x_copy(z, s, fwd.at[1, z, s], tp - 2).wait_send()

        x_copy(z, s, share.at[z, s], partner).wait_send()

    @pl.loop(0, 2 * pieces * (chips - 1))
    def _(i):
        d, s, step, c, valid = decode(i)
        nxt, pass_on, way = onward(step)

        @pl.when(valid)
        def _():
            @pl.when(s == 0)
            def _():
                @pl.when(pass_on)
                def _():
                    n_copy(c, nfwd.at[way, c], 2 * nxt + k).wait_send()

                n_copy(c, nshare.at[c], partner).wait_send()

            @pl.when(pass_on)
            def _():
                x_copy(c, s, fwd.at[way, c, s], 2 * nxt + k).wait_send()

            x_copy(c, s, share.at[c, s], partner).wait_send()


def one_of(n, values):
    total = 0
    for k, value in enumerate(values):
        if value:
            total = total + (n == k).astype(jnp.int32) * value
    return total


def middle_order(main, moved):
    near = [(0, i) for i in main]
    far = [(2, i) for i in moved + main]
    order = [(kind, i) for i in moved for kind in (0, 1)]
    order += [(1, i) for i in main]
    for at in range(max(len(near), len(far))):
        order += far[at : at + 1] + near[at : at + 1]
    return order


def outputs(totals, state_out, read_out):
    seqs, heads, keep, _ = state_out.shape
    raws = []
    for s in range(seqs):
        kept = totals[s, 0:keep].astype(BF16)
        for h in range(heads):
            state_out[s, h] = kept[:, h * HD : (h + 1) * HD]
        raws.append(totals[s, keep : keep + 1])
    raw = jnp.concatenate(raws, axis=0)
    for h in range(heads):
        at = slice(h * HD, (h + 1) * HD)
        head = raw[:, at]
        centered = head - jnp.mean(head, axis=-1, keepdims=True)
        spread = jnp.mean(centered * centered, axis=-1, keepdims=True)
        read_out[:, at] = (centered * lax.rsqrt(spread + 1e-05)).astype(BF16)


def moved_kernel(
    n_sp, n_tp, parts,
    tokens, fresh, wq_hbm, wk_hbm, wv_hbm, decay_ref,
    totals,
    x, xc, nx, wq, wk, wv, we, acc_k, acc_v, acc_c, cos_ref, sin_ref, fade_ref, rows_ref,
    q_spread, own_term, sums, stage, landed, hint, hint_in, stage_c, landed_c,
    load_sem, weight_sem, rx, rn, ry, rw, tx, hint_rx, rs_rx, c_rx, ready,
):
    seqs, span, feat = tokens.shape
    inner = wk.shape[1]
    heads = inner // HD
    half = inner // 2
    chunks = half // LANES
    chips = n_tp // 2
    pieces = seqs * parts
    size = span // parts
    keep = HD // n_sp
    groups = n_tp // 2
    moved_seq = seqs - 1
    to_mate_tx, to_other_tx, share_tx, n_tx, n_share_tx, y_tx, y_share_tx, w_tx, w_pass_tx = range(9)
    hint_tx, rs_tx, c_tx = range(9, 12)
    main = list(range(moved_seq * parts))
    moved = list(range(moved_seq * parts, pieces))
    sp = lax.axis_index("sp")
    tp = lax.axis_index("tp")
    z, k = tp // 2, tp % 2
    row_y, row_x = sp // 2, sp % 2
    x_peer = sp + 1 - 2 * row_x
    y_peer = sp + 2 - 4 * row_y
    MESH = pl.DeviceIdType.MESH
    end_int = (z == 0).astype(jnp.int32) + (z == chips - 1).astype(jnp.int32)
    end = end_int > 0
    mid = end_int == 0
    partner = z * 2 + 1 - k
    mate = z + 1 - 2 * (z % 2)
    mate_tp = 2 * mate + k
    other = chips - 1 - z
    other_tp = 2 * other + k
    second = end_int * (chips - 1 - mate) + (1 - end_int) * (chips - 1 - z)
    third = end_int * (chips - 1 - z) + (1 - end_int) * (chips - 1 - mate)

    own_loads = {
        s: pltpu.make_async_copy(
            tokens.at[s // parts, pl.ds(s % parts * size, size)], x.at[tp, s], load_sem.at[s]
        )
        for s in range(pieces)
    }
    new_load = pltpu.make_async_copy(fresh, nx.at[tp], load_sem.at[pieces])
    new_load.start()
    for s in moved + main:
        own_loads[s].start()
    weight_loads = [
        pltpu.make_async_copy(a, b, weight_sem.at[i])
        for i, (a, b) in enumerate(((wk_hbm, wk), (wv_hbm, wv), (wq_hbm, wq)))
    ]

    barrier = pltpu.get_barrier_semaphore()
    for target in ({"tp": partner}, {"tp": mate_tp}, {"sp": x_peer}, {"sp": y_peer}):
        pl.semaphore_signal(barrier, inc=1, device_id=target, device_id_type=MESH)

    @pl.when(mid)
    def _():
        pl.semaphore_signal(barrier, inc=1, device_id={"tp": other_tp}, device_id_type=MESH)

    pl.semaphore_wait(barrier, 5 - end_int)
    for target in ({"sp": x_peer}, {"sp": y_peer}):
        pl.semaphore_signal(ready.at[0], inc=1, device_id=target, device_id_type=MESH)

    def remote(source, dest, send, recv, target):
        return pltpu.make_async_remote_copy(
            source, dest, send, recv, device_id=target, device_id_type=MESH
        )

    def sent(ref, kind):
        remote(ref, ref, tx.at[kind], hint_rx.at[0], {"tp": partner}).wait_send()

    def arrived(ref, sem):
        remote(ref, ref, tx.at[0], sem, {"tp": partner}).wait_recv()

    def x_copy(c, s, kind, target):
        here = x.at[2 * c + k, s]
        return remote(here, here, tx.at[kind], rx.at[2 * c + k, s], {"tp": target})

    def to_mate(c, s):
        return x_copy(c, s, to_mate_tx, mate_tp)

    def to_other(c, s):
        return x_copy(c, s, to_other_tx, other_tp)

    def to_partner(c, s):
        return x_copy(c, s, share_tx, partner)

    def x_arrived(p, s):
        arrived(x.at[p, s], rx.at[p, s])

    def y_send(c, j):
        p = 2 * c + k
        return remote(
            x.at[p, moved[0] + j], xc.at[p, j], tx.at[y_tx], ry.at[c * parts + j], {"sp": y_peer}
        )

    def y_share(c, j):
        here = xc.at[2 * c + k, j]
        late = (c == third).astype(jnp.int32)
        return remote(
            here, here, tx.at[y_share_tx], ry.at[chips * parts + late], {"tp": partner}
        )

    def w_rows(p):
        return pl.ds(pl.multiple_of(p * feat, feat), feat)

    def w_cols(cc):
        return pl.ds(pl.multiple_of(row_y * half + cc * LANES, LANES), LANES)

    def w_part(g, r):
        if r is None:
            return w_rows(row_x * groups + g)
        start = (row_x * groups + g) * feat + r * (feat // 2)
        return pl.ds(pl.multiple_of(start, feat // 2), feat // 2)

    def w_place(cc, g, kv, r):
        return we.at[cc, w_part(g, r), pl.ds(kv * LANES, LANES)]

    def w_sem(cc, g, kv, r):
        if r is None:
            return rw.at[cc * groups + g]
        return rw.at[groups + 1 + 4 * (g - 1) + 2 * r + kv]

    def w_peer_sem(cc, g):
        return rw.at[5 * groups - 3 + cc * (1 + g)]

    def w_send(cc, g, kv, r=None):
        mine = (wk, wv)[kv].at[w_part(g, r), w_cols(cc)]
        return remote(
            mine, w_place(cc, g, kv, r), tx.at[w_tx], w_sem(cc, g, kv, r), {"tp": mate_tp}
        )

    def w_pass(cc, g, kv, r=None):
        here = w_place(cc, g, kv, r)
        return remote(here, here, tx.at[w_pass_tx], w_peer_sem(cc, g), {"sp": x_peer})

    def n_copy(c, kind, sem, target):
        here = nx.at[2 * c + k]
        return remote(here, here, tx.at[kind], sem, {"tp": target})

    def n_to(c, target):
        n_copy(c, n_tx, rn.at[c], target).start()

    def n_share(c):
        n_copy(c, n_share_tx, rn.at[chips], partner).start()

    def n_arrived(c):
        arrived(nx.at[2 * c + k], rn.at[c])

    hint_copy = remote(hint, hint_in, tx.at[hint_tx], hint_rx.at[0], {"tp": mate_tp})

    new_load.wait()
    n_to(z, mate_tp)
    n_share(z)

    @pl.when(mid)
    def _():
        n_to(z, other_tp)

    for s in moved + main:
        own_loads[s].wait()

    def send_moved(j):
        s = moved[j]

        @pl.when(mid)
        def _():
            to_other(z, s).start()
            y_send(z, j).start()
            to_partner(z, s).start()

        @pl.when(end)
        def _():
            to_mate(z, s).start()

    send_moved(0)
    to_partner(z, main[0]).start()

    @pl.when(mid)
    def _():
        to_mate(z, main[0]).start()

    for copy in weight_loads:
        copy.start()

    @pl.when(mid)
    def _():
        n_arrived(mate)
        n_to(mate, other_tp)
        n_share(mate)
        n_arrived(other)
        n_to(other, mate_tp)
        n_share(other)

    for j in range(1, parts):
        send_moved(j)
    for s in main[1:]:
        to_partner(z, s).start()

    @pl.when(mid)
    def _():
        for s in main[1:2]:
            to_mate(z, s).start()
        for s in main:
            to_other(z, s).start()

    row = lax.broadcasted_iota(jnp.int32, (span, LANES), 0)
    within = lane_iota((1, LANES)) % HD
    first_half = jnp.where(within < HD // 2, -1.0, 1.0).astype(F32)
    inverse = jnp.zeros((1, LANES), F32)
    for j, step in enumerate(inverse_angles()):
        inverse = jnp.where(within % (HD // 2) == j, float(step), inverse)

    def tables(slot, column):
        angles = (column * span + row).astype(F32) * inverse
        cos_ref[slot] = jnp.cos(angles)
        sin_ref[slot] = jnp.sin(angles) * first_half

    for copy in weight_loads[:2]:
        copy.wait()

    @pl.when(end)
    def _():
        for cc, g in [(0, g) for g in range(groups)] + [(1, 0)]:
            for kv in range(2):
                w_send(cc, g, kv).start()

    tables(0, sp)

    @pl.when(mid)
    def _():
        tables(1, y_peer)

    new_angles = jnp.full((NEW_ROWS, LANES), n_sp * span, F32) * inverse
    new_cos = jnp.cos(new_angles)
    new_sin = jnp.sin(new_angles) * first_half
    head_of = lane_iota((1, inner)) // HD
    rate = jnp.zeros((1, inner), F32)
    for h in range(heads):
        rate = jnp.where(head_of == h, decay_ref[h], rate)
    to_end = (span - 1 - lax.broadcasted_iota(jnp.int32, (span, 1), 0)).astype(F32)
    fade_ref[...] = jnp.exp(to_end * rate)
    rows_ref[0:1] = jnp.exp(rate * (span * (n_sp - 1 - sp)).astype(F32))
    rows_ref[1:2] = jnp.exp(rate)
    hint[...] = jnp.zeros(hint.shape, F32)
    hint[1:2] = rate
    weight_loads[2].wait()

    def add(p, s, fresh_total):
        block = x[p, s]
        where = w_rows(p)
        part_k = jnp.dot(block, wk[where, :], preferred_element_type=F32)
        part_v = jnp.dot(block, wv[where, :], preferred_element_type=F32)
        if fresh_total:
            acc_k[s] = part_k
            acc_v[s] = part_v
        else:
            acc_k[s] += part_k
            acc_v[s] += part_v

    same = (
        lax.broadcasted_iota(jnp.int32, (inner, inner), 0) // HD
        == lax.broadcasted_iota(jnp.int32, (inner, inner), 1) // HD
    )
    pick = lax.broadcasted_iota(jnp.int32, (HD, inner), 0) == lane_iota((HD, inner)) % HD

    @pl.when(mid)
    def _():
        n_arrived(third)
        n_to(third, mate_tp)
        n_share(third)
        for s in main[2:]:
            to_mate(z, s).start()

    own_pieces = end_int * len(main) + (1 - end_int) * pieces

    @pl.loop(0, pieces)
    def _(i):
        s = lax.rem(i + (1 - end_int) * len(main), pieces)

        @pl.when(i < own_pieces)
        def _():
            add(tp, s, True)

        @pl.when(i < own_pieces)
        def _():
            x_arrived(partner, s)
            add(partner, s, False)

    @pl.when(end)
    def _():
        for c in (mate, second, third):
            n_arrived(c)
            n_share(c)

    arrived(nx.at[pl.ds(0, chips)], rn.at[chips])

    def project_new():
        def piece(p, totals):
            where = w_rows(p)
            block = jnp.concatenate(
                [nx[p].astype(F32), jnp.zeros((NEW_ROWS - seqs, feat), F32)], axis=0
            ).astype(BF16)
            return tuple(
                t + jnp.dot(block, w[where, :], preferred_element_type=F32)
                for t, w in zip(totals, (wk, wv, wq))
            )

        zero = jnp.zeros((NEW_ROWS, inner), F32)
        new_k, new_v, new_q = lax.fori_loop(0, n_tp, piece, (zero, zero, zero))
        keys, queries = [], []
        for j in range(inner // LANES):
            at = slice(j * LANES, (j + 1) * LANES)
            keys.append((rotated(new_k[:, at], new_cos, new_sin) * HD**-0.5).astype(BF16))
            queries.append(rotated(new_q[:, at], new_cos, new_sin).astype(BF16))
        key = jnp.concatenate(keys, axis=1).astype(F32)
        query = jnp.concatenate(queries, axis=1).astype(F32)
        value = new_v.astype(BF16).astype(F32)
        product = query * key
        for h in range(heads):
            at = slice(h * HD, (h + 1) * HD)
            own_term[:, at] = jnp.sum(product[:, at], axis=-1, keepdims=True) * value[:, at]
        hint[0:1] = query[moved_seq : moved_seq + 1]
        for s in range(seqs):
            spread = jnp.where(pick, query[s : s + 1], 0.0).astype(BF16)
            q_spread[s] = jnp.dot(
                spread, jnp.where(same, 1.0, 0.0).astype(BF16), preferred_element_type=F32
            )

    project_new()

    @pl.when(end)
    def _():
        hint_copy.start()
        for s in main:
            to_mate(z, s).start()
        for g in range(1, groups):
            for r in range(2):
                for kv in range(2):
                    w_send(1, g, kv, r).start()

    def rs_copy(s, o):
        peer = lax.rem(sp + o, n_sp)
        return remote(
            stage.at[s, peer], landed.at[s, sp], tx.at[rs_tx], rs_rx.at[s], {"sp": peer}
        )

    pl.semaphore_wait(ready.at[0], 2)
    pl.semaphore_signal(ready.at[1], inc=1, device_id={"sp": x_peer}, device_id_type=MESH)

    def y_half(s):
        return remote(
            stage.at[s, pl.ds(2 - 2 * row_y, 2)], landed.at[s, pl.ds(0, 2)],
            tx.at[rs_tx], rs_rx.at[s], {"sp": y_peer},
        )

    def x_half(s):
        return remote(
            stage.at[s, x_peer], landed.at[s, 2], tx.at[rs_tx], rs_rx.at[seqs + s], {"sp": x_peer}
        )

    def outer(weighted, value):
        both = lax.dot_general(
            weighted, value, (((0,), (0,)), ((), ())), preferred_element_type=F32
        )
        return jnp.where(lane_iota((HD, LANES)) < HD, both[:HD], both[HD:])

    def finish(i):
        s, part = i // parts, i % parts
        where = pl.ds(pl.multiple_of(part * size, size), size)
        cosine, sine = cos_ref[0, where, :], sin_ref[0, where, :]
        for j in range(inner // LANES):
            at = slice(j * LANES, (j + 1) * LANES)
            key = (rotated(acc_k[i, :, at], cosine, sine) * HD**-0.5).astype(BF16)
            weighted = (key.astype(F32) * fade_ref[where, at]).astype(BF16)
            value = acc_v[i, :, at].astype(BF16)
            state = outer(weighted, value)
            sums[:, at] = jnp.where(part == 0, state, sums[:, at] + state)

        @pl.when(part == parts - 1)
        def _():
            scaled = sums[...] * rows_ref[0:1]
            read = jnp.sum(scaled * q_spread[s], axis=0, keepdims=True)
            for o in range(n_sp):
                stage[s, o, 0:keep] = scaled[o * keep : (o + 1) * keep]
                stage[s, o, keep : keep + 1] = read
            totals[s] = stage[s, sp]

            @pl.when(end | (s == moved_seq))
            def _():
                for o in range(1, n_sp):
                    rs_copy(s, o).start()

            @pl.when(mid & (s < moved_seq))
            def _():
                y_half(s).start()

    def c_add(cc, p, fresh_total):
        where = w_rows(p)
        for t in range(parts):
            for side, block in ((0, x[p, moved[0] + t]), (1, xc[p, t])):
                both = jnp.dot(block, we[cc, where, :], preferred_element_type=F32)
                if fresh_total:
                    acc_c[side, t] = both
                else:
                    acc_c[side, t] += both

    def c_copy(cc, o):
        return remote(
            stage_c.at[cc, o], landed_c.at[cc, sp], tx.at[c_tx], c_rx.at[cc],
            {"sp": o, "tp": mate_tp},
        )

    def c_finish(cc):
        pair_rate = hint_in[1:2, w_cols(cc)]
        query = hint_in[0:1, w_cols(cc)]
        total = jnp.zeros((HD, LANES), F32)
        for side, column in ((0, sp), (1, y_peer)):
            state = jnp.zeros((HD, LANES), F32)
            for t in range(parts):
                at = slice(t * size, (t + 1) * size)
                key = (
                    rotated(acc_c[side, t, :, :LANES], cos_ref[side, at], sin_ref[side, at])
                    * HD**-0.5
                ).astype(BF16)
                fade = jnp.exp(to_end[at] * pair_rate)
                weighted = (key.astype(F32) * fade).astype(BF16)
                state = state + outer(weighted, acc_c[side, t, :, LANES:].astype(BF16))
            total = total + state * jnp.exp(
                pair_rate * (span * (n_sp - 1 - column)).astype(F32)
            )
        spread = jnp.where(pick[:, :LANES], query, 0.0).astype(BF16)
        spread = jnp.dot(
            spread, jnp.where(same[:LANES, :LANES], 1.0, 0.0).astype(BF16),
            preferred_element_type=F32,
        )
        read = jnp.sum(total * spread, axis=0, keepdims=True)
        for o in range(n_sp):
            stage_c[cc, o, 0:keep] = total[o * keep : (o + 1) * keep]
            stage_c[cc, o, keep : keep + 1] = read
        for o in range(n_sp):
            c_copy(cc, o).start()

    order = middle_order(main, moved)
    steps = end_int * (len(main) * (chips - 1)) + (1 - end_int) * len(order)

    def decode(n):
        kind = end_int * (n // len(main)) + (1 - end_int) * one_of(n, [o[0] for o in order])
        s = end_int * (n % len(main)) + (1 - end_int) * one_of(n, [o[1] for o in order])
        c = (
            (kind == 0).astype(jnp.int32) * mate
            + (kind == 1).astype(jnp.int32) * second
            + (kind == 2).astype(jnp.int32) * third
        )
        return kind, c, s

    first_w = 2 * len(moved) + 1
    c_at = len(order) - 4
    last = len(order) - 1

    def w_pair(cc, g):
        arrived(we.at[cc, w_part(g, None)], w_sem(cc, g, 0, None))
        for kv in range(2):
            w_pass(cc, g, kv).start()

    def w_relay(g, r, kv):
        arrived(w_place(1, g, kv, r), w_sem(1, g, kv, r))
        w_pass(1, g, kv, r).start()

    def w_own(cc, g, fresh_total=False):
        c_add(cc, row_x * groups + g, fresh_total)

    def w_peer(cc, g):
        p = (1 - row_x) * groups + g
        arrived(we.at[cc, w_rows(p)], w_peer_sem(cc, g))
        c_add(cc, p, False)

    def y_pass(c, j):
        arrived(xc.at[2 * c + k, j], ry.at[c * parts + j])
        y_share(c, j).start()

    @pl.loop(0, len(order) + 1)
    def _(n):
        kind, c, s = decode(n)
        is_moved = s >= moved[0]

        @pl.when(mid & (n == last - 1))
        def _():
            w_relay(1, 0, 1)

        @pl.when(mid & (n == last))
        def _():
            w_relay(1, 1, 1)

        @pl.when(n < steps)
        def _():
            x_arrived(2 * c + k, s)

            @pl.when(mid & (kind == 0))
            def _():
                to_other(c, s).start()

            @pl.when(mid & (kind > 0) & (s < moved[0]))
            def _():
                to_mate(c, s).start()

            @pl.when(mid & is_moved)
            def _():
                y_send(c, s - moved[0]).start()

            to_partner(c, s).start()

        @pl.when(mid & (n == last - 2))
        def _():
            w_relay(1, 0, 0)

        @pl.when(mid & (n == last - 1))
        def _():
            w_relay(1, 1, 0)

        @pl.when(mid & (n == last))
        def _():
            w_relay(2, 0, 0)

        @pl.when(mid & (n >= first_w) & (n < first_w + groups))
        def _():
            w_pair(0, n - first_w)

        @pl.when(mid & (n == first_w + groups))
        def _():
            w_pair(1, 0)

        @pl.when(mid & (n >= 3) & (n < 3 + parts))
        def _():
            y_pass(z, n - 3)

        @pl.when(mid & (n >= 6) & (n < 6 + 2 * parts))
        def _():
            m = n - 6
            y_pass((m % 2) * second + (1 - m % 2) * mate, m // 2)

        @pl.when(mid & (n >= c_at - parts) & (n < c_at))
        def _():
            y_pass(third, n - (c_at - parts))

        @pl.when(n < steps)
        def _():
            add(2 * c + k, s, False)

        @pl.when(mid & (n == last))
        def _():
            w_relay(2, 0, 1)

        kind_b, c_b, s_b = decode(n - 1)

        @pl.when((n >= 1) & (n <= steps))
        def _():
            x_arrived(2 * c_b + 1 - k, s_b)
            add(2 * c_b + 1 - k, s_b, False)

            @pl.when(mid & (n == last + 1))
            def _():
                w_relay(2, 1, 1)

            @pl.when(kind_b == 2)
            def _():
                finish(s_b)

        @pl.when(mid & (n == last))
        def _():
            w_relay(2, 1, 0)

        early = n - (c_at - 5)

        @pl.when(mid & (early == 0))
        def _():
            arrived(xc.at[pl.ds(0, chips - 1)], ry.at[chips * parts])
            arrived(we.at[0, pl.ds(0, groups * feat)], w_peer_sem(0, 0))
            acc_c[...] = jnp.zeros(acc_c.shape, F32)

        @pl.when(mid & (early >= 0) & (early < 6))
        def _():
            turn = early // 2
            cx = (
                (turn == 0).astype(jnp.int32) * z
                + (turn == 1).astype(jnp.int32) * mate
                + (turn == 2).astype(jnp.int32) * second
            )
            c_add(0, 2 * cx + early % 2, False)

        @pl.when(mid & (n == c_at))
        def _():
            arrived(xc.at[0], ry.at[chips * parts + 1])

            @pl.loop(0, 2)
            def _(m):
                c_add(0, 2 * third + m, False)

            hint_copy.wait_recv()
            pl.semaphore_wait(ready.at[1], 1)
            c_finish(0)

    @pl.when(mid)
    def _():
        w_own(1, 0, True)
        w_peer(1, 0)
        w_relay(3, 0, 0)
        w_own(1, 1)
        w_peer(1, 1)
        w_relay(3, 0, 1)
        w_own(1, 2)
        w_relay(3, 1, 0)
        w_relay(3, 1, 1)
        w_peer(1, 2)
        w_own(1, 3)
        for s in range(moved_seq):
            arrived(landed.at[s, pl.ds(0, 2)], rs_rx.at[s])
            for side in range(2):
                stage[s, 2 * row_y + side] += landed[s, side]
            x_half(s).start()
        w_peer(1, 3)
        c_finish(1)

    def gather(s):
        arrived(landed.at[s, pl.ds(0, n_sp - 1)], rs_rx.at[s])
        total = None
        for j in range(n_sp):
            term = jnp.where(sp == j, totals[s], landed[s, j])
            total = term if total is None else total + term
        totals[s] = total

    sent(nx.at[pl.ds(0, chips)], n_share_tx)

    @pl.when(end)
    def _():
        pl.semaphore_wait(ready.at[1], 1)
        sent(nx.at[0], n_tx)
        sent(hint, hint_tx)
        sent(x.at[0], to_mate_tx)
        sent(x.at[pl.ds(0, chips), pl.ds(0, len(main))], share_tx)
        sent(we.at[pl.ds(0, chunks), pl.ds(0, groups * feat)], w_tx)
        sent(stage.at[pl.ds(0, moved_seq), pl.ds(0, n_sp - 1)], rs_tx)

    @pl.when(mid)
    def _():
        sent(nx.at[pl.ds(0, 5)], n_tx)
        sent(x.at[pl.ds(0, chips - 1), pl.ds(0, len(main))], to_mate_tx)
        sent(x.at[pl.ds(0, 2)], to_other_tx)
        sent(x.at[pl.ds(0, chips)], share_tx)
        sent(xc.at[pl.ds(0, chips)], y_tx)
        sent(xc.at[pl.ds(0, chips)], y_share_tx)
        sent(we.at[pl.ds(0, chunks), pl.ds(0, groups * feat)], w_pass_tx)
        sent(stage.at[:, pl.ds(0, n_sp - 1)], rs_tx)

    @pl.when(mid)
    def _():
        for s in range(moved_seq):
            arrived(landed.at[s, 2], rs_rx.at[seqs + s])
            totals[s] = stage[s, sp] + landed[s, 2]
        gather(moved_seq)

    @pl.when(end)
    def _():
        for s in range(moved_seq):
            gather(s)
        for cc in range(chunks):
            arrived(landed_c.at[cc], c_rx.at[cc])
            for side in range(2):
                at = slice(side * half + cc * LANES, side * half + (cc + 1) * LANES)
                totals[moved_seq, :, at] = landed_c[cc, 2 * side] + landed_c[cc, 2 * side + 1]

    for s in range(seqs):
        read = totals[s, keep : keep + 1]
        totals[s, keep : keep + 1] = read * rows_ref[1:2] + own_term[s : s + 1]

    @pl.when(mid)
    def _():
        sent(stage_c, c_tx)


def solution(mesh):
    n_sp, n_tp = mesh.shape["sp"], mesh.shape["tp"]

    def body(tokens, new_token, query_weight, key_weight, value_weight, log_decay):
        seqs, span, feat = tokens.shape
        width, inner = key_weight.shape
        heads = inner // HD
        keep = HD // n_sp
        rows = -(-(keep + 1) // 8) * 8
        chips = n_tp // 2
        half = HD // 2
        parts = max(1, 8 // chips)
        pieces = seqs * parts
        size = span // parts
        inverse = jnp.asarray(np.tile(inverse_angles(), LANES // half)[None])
        anywhere = pl.BlockSpec(memory_space=pl.ANY)
        vmem = pl.BlockSpec(memory_space=pltpu.VMEM)
        dma = pltpu.SemaphoreType.DMA
        moves = chips == 4 and n_sp == 4 and seqs > 1 and inner == 4 * LANES
        tokens_in = [
            pltpu.VMEM((n_tp, pieces, size, feat), BF16),
            pltpu.VMEM((n_tp, seqs, feat), BF16),
        ]
        weights_in = [pltpu.VMEM((width, inner), BF16)] * 3
        totals = [pltpu.VMEM((pieces, size, inner), F32)] * 2
        ends = [
            pltpu.VMEM((8, inner), F32),
            pltpu.VMEM((seqs, HD, inner), F32),
            pltpu.VMEM((NEW_ROWS, inner), F32),
            pltpu.VMEM((HD, inner), F32),
            pltpu.VMEM((seqs, n_sp, rows, inner), F32),
            pltpu.VMEM((seqs, n_sp, rows, inner), F32),
        ]
        if moves:
            chunks = inner // 2 // LANES
            groups = n_tp // 2
            call = moved_kernel
            scratch = (
                tokens_in[:1]
                + [pltpu.VMEM((n_tp, parts, size, feat), BF16)]
                + tokens_in[1:]
                + weights_in
                + [pltpu.VMEM((chunks, width, 2 * LANES), BF16)]
                + totals
                + [
                    pltpu.VMEM((2, parts, size, 2 * LANES), F32),
                    pltpu.VMEM((2, span, LANES), F32),
                    pltpu.VMEM((2, span, LANES), F32),
                    pltpu.VMEM((span, inner), F32),
                ]
                + ends
                + [
                    pltpu.VMEM((8, inner), F32),
                    pltpu.VMEM((8, inner), F32),
                    pltpu.VMEM((chunks, n_sp, rows, LANES), F32),
                    pltpu.VMEM((chunks, n_sp, rows, LANES), F32),
                    dma((pieces + 1,)),
                    dma((3,)),
                    dma((n_tp, pieces)),
                    dma((chips + 1,)),
                    dma((chips * parts + 2,)),
                    dma((6 * groups - 2,)),
                    dma((12,)),
                    dma((1,)),
                    dma((2 * seqs,)),
                    dma((chunks,)),
                    pltpu.SemaphoreType.REGULAR((2,)),
                ]
            )
        else:
            call = kernel
            scratch = (
                tokens_in
                + weights_in
                + totals
                + [
                    pltpu.VMEM((span, LANES), F32),
                    pltpu.VMEM((span, LANES), F32),
                    pltpu.VMEM((span, inner), F32),
                ]
                + ends
                + [
                    pltpu.VMEM((seqs, rows, inner), F32),
                    dma((pieces + 1,)),
                    dma((3,)),
                    dma((n_tp, pieces)),
                    dma((n_tp,)),
                    dma((2, chips, pieces)),
                    dma((chips, pieces)),
                    dma((2, chips)),
                    dma((chips,)),
                    dma((seqs, n_sp)),
                    dma((seqs, n_sp)),
                ]
            )
        out_shape = (
            jax.ShapeDtypeStruct((seqs, heads, keep, HD), BF16),
            jax.ShapeDtypeStruct((seqs, inner), BF16),
        )
        shared = dict(
            scratch_shapes=scratch,
            name="retention",
        )
        args = (
            tokens, new_token.reshape(seqs, feat), query_weight, key_weight, value_weight
        )
        args = tuple(pltpu.with_memory_space_constraint(a, pltpu.HBM) for a in args)
        smem = pl.BlockSpec(memory_space=pltpu.SMEM)
        limit = (53 if moves else 60) * 1024 * 1024
        params = pltpu.CompilerParams(
            collective_id=0, has_side_effects=True, vmem_limit_bytes=limit
        )
        call = functools.partial(call, n_sp, n_tp, parts)
        if not moves:
            return pl.pallas_call(
                call,
                out_shape=out_shape,
                in_specs=[anywhere] * 5 + [vmem, smem],
                out_specs=(vmem, vmem),
                compiler_params=params,
                **shared,
            )(*args, inverse, log_decay)
        sums = pl.pallas_call(
            call,
            out_shape=jax.ShapeDtypeStruct((seqs, rows, inner), F32),
            in_specs=[anywhere] * 5 + [smem],
            out_specs=vmem,
            compiler_params=params,
            **shared,
        )(*args, pltpu.with_memory_space_constraint(log_decay, pltpu.HBM))
        return pl.pallas_call(
            outputs,
            out_shape=out_shape,
            in_specs=[vmem],
            out_specs=(vmem, vmem),
            compiler_params=pltpu.CompilerParams(vmem_limit_bytes=4 * 1024 * 1024),
            name="outputs",
        )(sums)

    return jax.shard_map(
        body,
        mesh=mesh,
        in_specs=(
            P(None, "sp", "tp"),
            P(None, None, "tp"),
            P(None, "tp"),
            P(None, "tp"),
            P(None, "tp"),
            P("tp"),
        ),
        out_specs=(P(None, "tp", "sp", None), P(None, "tp")),
        check_vma=False,
    )
```

```python
import functools

import jax
import jax.numpy as jnp
import numpy as np
from jax import lax
from jax.experimental import pallas as pl
from jax.experimental.pallas import tpu as pltpu
from jax.sharding import PartitionSpec as P

HD = 64
LANES = 128
NEW_ROWS = 8
F32 = jnp.float32
BF16 = jnp.bfloat16


def inverse_angles():
    half = HD // 2
    return np.float32(10000.0) ** (-np.arange(half, dtype=np.float32) / half)


def lane_iota(shape):
    return lax.broadcasted_iota(jnp.int32, shape, len(shape) - 1)


def rotated(block, cosine, sine):
    half = HD // 2
    low = lane_iota(block.shape) % HD < half
    swapped = jnp.where(
        low, pltpu.roll(block, LANES - half, 1), pltpu.roll(block, half, 1)
    )
    return block * cosine + swapped * sine


def kernel(
    n_sp, n_tp, parts,
    tokens, fresh, wq_hbm, wk_hbm, wv_hbm, inverse_ref, decay_ref,
    state_out, read_out,
    x, nx, wq, wk, wv, acc_k, acc_v, cos_ref, sin_ref, fade_ref, rows_ref,
    q_spread, own_term, sums, stage, landed, totals,
    load_sem, weight_sem, rx, rn, fwd, share, nfwd, nshare, rs_tx, rs_rx,
):
    seqs, span, feat = tokens.shape
    inner = wk.shape[1]
    heads = inner // HD
    chips = n_tp // 2
    pieces = seqs * parts
    size = span // parts
    keep = HD // n_sp
    sp = lax.axis_index("sp")
    tp = lax.axis_index("tp")
    z, k = tp // 2, tp % 2
    MESH = pl.DeviceIdType.MESH

    def to_tp(index):
        return {"tp": index}

    partner = z * 2 + 1 - k
    own_loads = [
        pltpu.make_async_copy(
            tokens.at[s // parts, pl.ds(s % parts * size, size)], x.at[tp, s], load_sem.at[s]
        )
        for s in range(pieces)
    ]
    new_load = pltpu.make_async_copy(fresh, nx.at[tp], load_sem.at[pieces])
    new_load.start()
    for copy in own_loads:
        copy.start()
    weight_loads = [
        pltpu.make_async_copy(a, b, weight_sem.at[i])
        for i, (a, b) in enumerate(((wk_hbm, wk), (wv_hbm, wv), (wq_hbm, wq)))
    ]

    barrier = pltpu.get_barrier_semaphore()

    @pl.when(z > 0)
    def _():
        pl.semaphore_signal(barrier, inc=1, device_id=to_tp(tp - 2), device_id_type=MESH)

    @pl.when(z < chips - 1)
    def _():
        pl.semaphore_signal(barrier, inc=1, device_id=to_tp(tp + 2), device_id_type=MESH)

    pl.semaphore_signal(barrier, inc=1, device_id=to_tp(partner), device_id_type=MESH)
    for o in range(1, n_sp):
        pl.semaphore_signal(
            barrier, inc=1, device_id={"sp": lax.rem(sp + o, n_sp)}, device_id_type=MESH
        )
    pl.semaphore_wait(
        barrier, n_sp + (z > 0).astype(jnp.int32) + (z < chips - 1).astype(jnp.int32)
    )

    def x_copy(c, s, sem, target):
        p = 2 * c + k
        return pltpu.make_async_remote_copy(
            x.at[p, s], x.at[p, s], sem, rx.at[p, s], device_id=to_tp(target), device_id_type=MESH
        )

    def n_copy(c, sem, target):
        p = 2 * c + k
        return pltpu.make_async_remote_copy(
            nx.at[p], nx.at[p], sem, rn.at[p], device_id=to_tp(target), device_id_type=MESH
        )

    def x_arrived(p, s):
        pltpu.make_async_remote_copy(
            x.at[p, s], x.at[p, s], share.at[0, 0], rx.at[p, s],
            device_id=to_tp(partner), device_id_type=MESH,
        ).wait_recv()

    def n_arrived(p):
        pltpu.make_async_remote_copy(
            nx.at[p], nx.at[p], nshare.at[0], rn.at[p],
            device_id=to_tp(partner), device_id_type=MESH,
        ).wait_recv()

    new_load.wait()
    n_up = n_copy(z, nfwd.at[0, z], tp + 2)
    n_down = n_copy(z, nfwd.at[1, z], tp - 2)
    n_side = n_copy(z, nshare.at[z], partner)

    @pl.when(z < chips - 1)
    def _():
        n_up.start()

    @pl.when(z > 0)
    def _():
        n_down.start()

    n_side.start()
    for s in range(pieces):
        own_loads[s].wait()

        @pl.when(z < chips - 1)
        def _(s=s):
            x_copy(z, s, fwd.at[0, z, s], tp + 2).start()

        @pl.when(z > 0)
        def _(s=s):
            x_copy(z, s, fwd.at[1, z, s], tp - 2).start()

        x_copy(z, s, share.at[z, s], partner).start()

    for copy in weight_loads:
        copy.start()

    row = lax.broadcasted_iota(jnp.int32, (span, LANES), 0)
    within = lane_iota((1, LANES)) % HD
    first_half = jnp.where(within < HD // 2, -1.0, 1.0).astype(F32)
    inverse = inverse_ref[...]
    angles = (sp * span + row).astype(F32) * inverse
    cos_ref[...] = jnp.cos(angles)
    sin_ref[...] = jnp.sin(angles) * first_half
    new_angles = jnp.full((NEW_ROWS, LANES), n_sp * span, F32) * inverse
    new_cos = jnp.cos(new_angles)
    new_sin = jnp.sin(new_angles) * first_half
    head_of = lane_iota((1, inner)) // HD
    rate = jnp.zeros((1, inner), F32)
    for h in range(heads):
        rate = jnp.where(head_of == h, decay_ref[h], rate)
    to_end = (span - 1 - lax.broadcasted_iota(jnp.int32, (span, 1), 0)).astype(F32)
    fade_ref[...] = jnp.exp(to_end * rate)
    rows_ref[0:1] = jnp.exp(rate * (span * (n_sp - 1 - sp)).astype(F32))
    rows_ref[1:2] = jnp.exp(rate)

    for copy in weight_loads:
        copy.wait()

    def add(p, s, fresh_total):
        block = x[p, s]
        where = pl.ds(pl.multiple_of(p * feat, feat), feat)
        part_k = jnp.dot(block, wk[where, :], preferred_element_type=F32)
        part_v = jnp.dot(block, wv[where, :], preferred_element_type=F32)
        if fresh_total:
            acc_k[s] = part_k
            acc_v[s] = part_v
        else:
            acc_k[s] += part_k
            acc_v[s] += part_v

    @pl.loop(0, pieces)
    def _(s):
        add(tp, s, True)
        x_arrived(partner, s)
        add(partner, s, False)

    n_arrived(partner)

    def project_new():
        def piece(p, totals):
            where = pl.ds(pl.multiple_of(p * feat, feat), feat)
            block = jnp.concatenate(
                [nx[p].astype(F32), jnp.zeros((NEW_ROWS - seqs, feat), F32)], axis=0
            ).astype(BF16)
            return tuple(
                t + jnp.dot(block, w[where, :], preferred_element_type=F32)
                for t, w in zip(totals, (wk, wv, wq))
            )

        zero = jnp.zeros((NEW_ROWS, inner), F32)
        new_k, new_v, new_q = lax.fori_loop(0, n_tp, piece, (zero, zero, zero))
        keys, queries = [], []
        for j in range(inner // LANES):
            at = slice(j * LANES, (j + 1) * LANES)
            keys.append((rotated(new_k[:, at], new_cos, new_sin) * HD**-0.5).astype(BF16))
            queries.append(rotated(new_q[:, at], new_cos, new_sin).astype(BF16))
        key = jnp.concatenate(keys, axis=1).astype(F32)
        query = jnp.concatenate(queries, axis=1).astype(F32)
        value = new_v.astype(BF16).astype(F32)
        same = (
            lax.broadcasted_iota(jnp.int32, (inner, inner), 0) // HD
            == lax.broadcasted_iota(jnp.int32, (inner, inner), 1) // HD
        )
        product = query * key
        for h in range(heads):
            at = slice(h * HD, (h + 1) * HD)
            own_term[:, at] = jnp.sum(product[:, at], axis=-1, keepdims=True) * value[:, at]
        pick = lax.broadcasted_iota(jnp.int32, (HD, inner), 0) == lane_iota((HD, inner)) % HD
        for s in range(seqs):
            spread = jnp.where(pick, query[s : s + 1], 0.0).astype(BF16)
            q_spread[s] = jnp.dot(
                spread, jnp.where(same, 1.0, 0.0).astype(BF16), preferred_element_type=F32
            )

    def rs_copy(s, o):
        peer = lax.rem(sp + o, n_sp)
        return pltpu.make_async_remote_copy(
            stage.at[s, peer], landed.at[s, sp], rs_tx.at[s, peer], rs_rx.at[s, sp],
            device_id={"sp": peer}, device_id_type=MESH,
        )

    def finish(i):
        s, part = i // parts, i % parts
        where = pl.ds(pl.multiple_of(part * size, size), size)
        cosine, sine = cos_ref[where, :], sin_ref[where, :]
        lane = lane_iota((HD, LANES))
        for j in range(inner // LANES):
            at = slice(j * LANES, (j + 1) * LANES)
            key = (rotated(acc_k[i, :, at], cosine, sine) * HD**-0.5).astype(BF16)
            weighted = (key.astype(F32) * fade_ref[where, at]).astype(BF16)
            value = acc_v[i, :, at].astype(BF16)
            both = lax.dot_general(
                weighted, value, (((0,), (0,)), ((), ())), preferred_element_type=F32
            )
            state = jnp.where(lane < HD, both[:HD], both[HD:])
            sums[:, at] = jnp.where(part == 0, state, sums[:, at] + state)

        @pl.when(part == parts - 1)
        def _():
            scaled = sums[...] * rows_ref[0:1]
            read = jnp.sum(scaled * q_spread[s], axis=0, keepdims=True)
            for o in range(n_sp):
                stage[s, o, 0:keep] = scaled[o * keep : (o + 1) * keep]
                stage[s, o, keep : keep + 1] = read
            for o in range(1, n_sp):
                rs_copy(s, o).start()
            totals[s] = stage[s, sp]

    far = jnp.maximum(z, chips - 1 - z)

    def decode(i):
        d = i // (2 * pieces) + 1
        s = (i // 2) % pieces
        step = 2 * (i % 2) - 1
        c = z + step * d
        return d, s, step, c, (c >= 0) & (c < chips)

    def onward(step):
        nxt = z - step
        return nxt, (nxt >= 0) & (nxt < chips), (step + 1) // 2

    @pl.loop(0, 2 * pieces * (chips - 1))
    def _(i):
        d, s, step, c, valid = decode(i)
        nxt, pass_on, way = onward(step)

        @pl.when(valid)
        def _():
            @pl.when(s == 0)
            def _():
                n_arrived(2 * c + k)

                @pl.when(pass_on)
                def _():
                    n_copy(c, nfwd.at[way, c], 2 * nxt + k).start()

                n_copy(c, nshare.at[c], partner).start()

            x_arrived(2 * c + k, s)

            @pl.when(pass_on)
            def _():
                x_copy(c, s, fwd.at[way, c, s], 2 * nxt + k).start()

            x_copy(c, s, share.at[c, s], partner).start()
            add(2 * c + k, s, False)

            @pl.when(s == 0)
            def _():
                n_arrived(2 * c + 1 - k)

            x_arrived(2 * c + 1 - k, s)
            add(2 * c + 1 - k, s, False)

        last = (d == far) & (step == 1)

        @pl.when(last & (s == 0))
        def _():
            project_new()

        @pl.when(last)
        def _():
            finish(s)

    raws = []
    for s in range(seqs):
        for o in range(1, n_sp):
            src = lax.rem(sp + o, n_sp)
            pltpu.make_async_remote_copy(
                stage.at[s, src], landed.at[s, src], rs_tx.at[s, src], rs_rx.at[s, src],
                device_id={"sp": src}, device_id_type=MESH,
            ).wait_recv()
        total = None
        for j in range(n_sp):
            term = jnp.where(sp == j, totals[s], landed[s, j])
            total = term if total is None else total + term
        kept = total[0:keep].astype(BF16)
        for h in range(heads):
            state_out[s, h] = kept[:, h * HD : (h + 1) * HD]
        raws.append(total[keep : keep + 1] * rows_ref[1:2] + own_term[s : s + 1])
    raw = jnp.concatenate(raws, axis=0)
    for h in range(heads):
        at = slice(h * HD, (h + 1) * HD)
        head = raw[:, at]
        centered = head - jnp.mean(head, axis=-1, keepdims=True)
        spread = jnp.mean(centered * centered, axis=-1, keepdims=True)
        read_out[:, at] = (centered * lax.rsqrt(spread + 1e-05)).astype(BF16)

    @pl.when(z < chips - 1)
    def _():
        n_up.wait_send()

    @pl.when(z > 0)
    def _():
        n_down.wait_send()

    n_side.wait_send()
    for s in range(seqs):
        for o in range(1, n_sp):
            rs_copy(s, o).wait_send()
    for s in range(pieces):
        @pl.when(z < chips - 1)
        def _(s=s):
            x_copy(z, s, fwd.at[0, z, s], tp + 2).wait_send()

        @pl.when(z > 0)
        def _(s=s):
            x_copy(z, s, fwd.at[1, z, s], tp - 2).wait_send()

        x_copy(z, s, share.at[z, s], partner).wait_send()

    @pl.loop(0, 2 * pieces * (chips - 1))
    def _(i):
        d, s, step, c, valid = decode(i)
        nxt, pass_on, way = onward(step)

        @pl.when(valid)
        def _():
            @pl.when(s == 0)
            def _():
                @pl.when(pass_on)
                def _():
                    n_copy(c, nfwd.at[way, c], 2 * nxt + k).wait_send()

                n_copy(c, nshare.at[c], partner).wait_send()

            @pl.when(pass_on)
            def _():
                x_copy(c, s, fwd.at[way, c, s], 2 * nxt + k).wait_send()

            x_copy(c, s, share.at[c, s], partner).wait_send()


def one_of(n, values):
    total = 0
    for k, value in enumerate(values):
        if value:
            total = total + (n == k).astype(jnp.int32) * value
    return total


def middle_order(main, moved):
    near = [(0, i) for i in main]
    far = [(2, i) for i in moved + main]
    order = [(kind, i) for i in moved for kind in (0, 1)]
    order += [(1, i) for i in main]
    for at in range(max(len(near), len(far))):
        order += far[at : at + 1] + near[at : at + 1]
    return order


def outputs(totals, state_out, read_out):
    seqs, heads, keep, _ = state_out.shape
    raws = []
    for s in range(seqs):
        kept = totals[s, 0:keep].astype(BF16)
        for h in range(heads):
            state_out[s, h] = kept[:, h * HD : (h + 1) * HD]
        raws.append(totals[s, keep : keep + 1])
    raw = jnp.concatenate(raws, axis=0)
    for h in range(heads):
        at = slice(h * HD, (h + 1) * HD)
        head = raw[:, at]
        centered = head - jnp.mean(head, axis=-1, keepdims=True)
        spread = jnp.mean(centered * centered, axis=-1, keepdims=True)
        read_out[:, at] = (centered * lax.rsqrt(spread + 1e-05)).astype(BF16)


def moved_kernel(
    n_sp, n_tp, parts,
    tokens, fresh, wq_hbm, wk_hbm, wv_hbm, decay_ref,
    totals,
    x, xc, nx, wq, wk, wv, we, acc_k, acc_v, acc_c, cos_ref, sin_ref, fade_ref, rows_ref,
    q_spread, own_term, sums, stage, landed, hint, hint_in, stage_c, landed_c,
    load_sem, weight_sem, rx, rn, ry, rw, tx, hint_rx, rs_rx, c_rx, ready,
):
    seqs, span, feat = tokens.shape
    inner = wk.shape[1]
    heads = inner // HD
    half = inner // 2
    chunks = half // LANES
    chips = n_tp // 2
    pieces = seqs * parts
    size = span // parts
    keep = HD // n_sp
    groups = n_tp // 2
    moved_seq = seqs - 1
    to_mate_tx, to_other_tx, share_tx, n_tx, n_share_tx, y_tx, y_share_tx, w_tx, w_pass_tx = range(9)
    hint_tx, rs_tx, c_tx = range(9, 12)
    main = list(range(moved_seq * parts))
    moved = list(range(moved_seq * parts, pieces))
    sp = lax.axis_index("sp")
    tp = lax.axis_index("tp")
    z, k = tp // 2, tp % 2
    row_y, row_x = sp // 2, sp % 2
    x_peer = sp + 1 - 2 * row_x
    y_peer = sp + 2 - 4 * row_y
    MESH = pl.DeviceIdType.MESH
    end_int = (z == 0).astype(jnp.int32) + (z == chips - 1).astype(jnp.int32)
    end = end_int > 0
    mid = end_int == 0
    partner = z * 2 + 1 - k
    mate = z + 1 - 2 * (z % 2)
    mate_tp = 2 * mate + k
    other = chips - 1 - z
    other_tp = 2 * other + k
    second = end_int * (chips - 1 - mate) + (1 - end_int) * (chips - 1 - z)
    third = end_int * (chips - 1 - z) + (1 - end_int) * (chips - 1 - mate)

    own_loads = {
        s: pltpu.make_async_copy(
            tokens.at[s // parts, pl.ds(s % parts * size, size)], x.at[tp, s], load_sem.at[s]
        )
        for s in range(pieces)
    }
    new_load = pltpu.make_async_copy(fresh, nx.at[tp], load_sem.at[pieces])
    new_load.start()
    for s in moved + main:
        own_loads[s].start()
    weight_loads = [
        pltpu.make_async_copy(a, b, weight_sem.at[i])
        for i, (a, b) in enumerate(((wk_hbm, wk), (wv_hbm, wv), (wq_hbm, wq)))
    ]

    barrier = pltpu.get_barrier_semaphore()
    for target in ({"tp": partner}, {"tp": mate_tp}, {"sp": x_peer}, {"sp": y_peer}):
        pl.semaphore_signal(barrier, inc=1, device_id=target, device_id_type=MESH)

    @pl.when(mid)
    def _():
        pl.semaphore_signal(barrier, inc=1, device_id={"tp": other_tp}, device_id_type=MESH)

    pl.semaphore_wait(barrier, 5 - end_int)
    for target in ({"sp": x_peer}, {"sp": y_peer}):
        pl.semaphore_signal(ready.at[0], inc=1, device_id=target, device_id_type=MESH)

    def remote(source, dest, send, recv, target):
        return pltpu.make_async_remote_copy(
            source, dest, send, recv, device_id=target, device_id_type=MESH
        )

    def sent(ref, kind):
        remote(ref, ref, tx.at[kind], hint_rx.at[0], {"tp": partner}).wait_send()

    def arrived(ref, sem):
        remote(ref, ref, tx.at[0], sem, {"tp": partner}).wait_recv()

    def x_copy(c, s, kind, target):
        here = x.at[2 * c + k, s]
        return remote(here, here, tx.at[kind], rx.at[2 * c + k, s], {"tp": target})

    def to_mate(c, s):
        return x_copy(c, s, to_mate_tx, mate_tp)

    def to_other(c, s):
        return x_copy(c, s, to_other_tx, other_tp)

    def to_partner(c, s):
        return x_copy(c, s, share_tx, partner)

    def x_arrived(p, s):
        arrived(x.at[p, s], rx.at[p, s])

    def y_send(c, j):
        p = 2 * c + k
        return remote(
            x.at[p, moved[0] + j], xc.at[p, j], tx.at[y_tx], ry.at[c * parts + j], {"sp": y_peer}
        )

    def y_share(c, j):
        here = xc.at[2 * c + k, j]
        late = (c == third).astype(jnp.int32)
        return remote(
            here, here, tx.at[y_share_tx], ry.at[chips * parts + late], {"tp": partner}
        )

    def w_rows(p):
        return pl.ds(pl.multiple_of(p * feat, feat), feat)

    def w_cols(cc):
        return pl.ds(pl.multiple_of(row_y * half + cc * LANES, LANES), LANES)

    def w_part(g, r):
        if r is None:
            return w_rows(row_x * groups + g)
        start = (row_x * groups + g) * feat + r * (feat // 2)
        return pl.ds(pl.multiple_of(start, feat // 2), feat // 2)

    def w_place(cc, g, kv, r):
        return we.at[cc, w_part(g, r), pl.ds(kv * LANES, LANES)]

    def w_sem(cc, g, kv, r):
        if r is None:
            return rw.at[cc * groups + g]
        return rw.at[groups + 1 + 4 * (g - 1) + 2 * r + kv]

    def w_peer_sem(cc, g):
        return rw.at[5 * groups - 3 + cc * (1 + g)]

    def w_send(cc, g, kv, r=None):
        mine = (wk, wv)[kv].at[w_part(g, r), w_cols(cc)]
        return remote(
            mine, w_place(cc, g, kv, r), tx.at[w_tx], w_sem(cc, g, kv, r), {"tp": mate_tp}
        )

    def w_pass(cc, g, kv, r=None):
        here = w_place(cc, g, kv, r)
        return remote(here, here, tx.at[w_pass_tx], w_peer_sem(cc, g), {"sp": x_peer})

    def n_copy(c, kind, sem, target):
        here = nx.at[2 * c + k]
        return remote(here, here, tx.at[kind], sem, {"tp": target})

    def n_to(c, target):
        n_copy(c, n_tx, rn.at[c], target).start()

    def n_share(c):
        n_copy(c, n_share_tx, rn.at[chips], partner).start()

    def n_arrived(c):
        arrived(nx.at[2 * c + k], rn.at[c])

    hint_copy = remote(hint, hint_in, tx.at[hint_tx], hint_rx.at[0], {"tp": mate_tp})

    new_load.wait()
    n_to(z, mate_tp)
    n_share(z)

    @pl.when(mid)
    def _():
        n_to(z, other_tp)

    for s in moved + main:
        own_loads[s].wait()

    def send_moved(j):
        s = moved[j]

        @pl.when(mid)
        def _():
            to_other(z, s).start()
            y_send(z, j).start()
            to_partner(z, s).start()

        @pl.when(end)
        def _():
            to_mate(z, s).start()

    send_moved(0)
    to_partner(z, main[0]).start()

    @pl.when(mid)
    def _():
        to_mate(z, main[0]).start()

    for copy in weight_loads:
        copy.start()

    @pl.when(mid)
    def _():
        n_arrived(mate)
        n_to(mate, other_tp)
        n_share(mate)
        n_arrived(other)
        n_to(other, mate_tp)
        n_share(other)

    for j in range(1, parts):
        send_moved(j)
    for s in main[1:]:
        to_partner(z, s).start()

    @pl.when(mid)
    def _():
        for s in main[1:2]:
            to_mate(z, s).start()
        for s in main:
            to_other(z, s).start()

    row = lax.broadcasted_iota(jnp.int32, (span, LANES), 0)
    within = lane_iota((1, LANES)) % HD
    first_half = jnp.where(within < HD // 2, -1.0, 1.0).astype(F32)
    inverse = jnp.zeros((1, LANES), F32)
    for j, step in enumerate(inverse_angles()):
        inverse = jnp.where(within % (HD // 2) == j, float(step), inverse)

    def tables(slot, column):
        angles = (column * span + row).astype(F32) * inverse
        cos_ref[slot] = jnp.cos(angles)
        sin_ref[slot] = jnp.sin(angles) * first_half

    for copy in weight_loads[:2]:
        copy.wait()

    @pl.when(end)
    def _():
        for cc, g in [(0, g) for g in range(groups)] + [(1, 0)]:
            for kv in range(2):
                w_send(cc, g, kv).start()

    tables(0, sp)

    @pl.when(mid)
    def _():
        tables(1, y_peer)

    new_angles = jnp.full((NEW_ROWS, LANES), n_sp * span, F32) * inverse
    new_cos = jnp.cos(new_angles)
    new_sin = jnp.sin(new_angles) * first_half
    head_of = lane_iota((1, inner)) // HD
    rate = jnp.zeros((1, inner), F32)
    for h in range(heads):
        rate = jnp.where(head_of == h, decay_ref[h], rate)
    to_end = (span - 1 - lax.broadcasted_iota(jnp.int32, (span, 1), 0)).astype(F32)
    fade_ref[...] = jnp.exp(to_end * rate)
    rows_ref[0:1] = jnp.exp(rate * (span * (n_sp - 1 - sp)).astype(F32))
    rows_ref[1:2] = jnp.exp(rate)
    hint[...] = jnp.zeros(hint.shape, F32)
    hint[1:2] = rate
    weight_loads[2].wait()

    def add(p, s, fresh_total):
        block = x[p, s]
        where = w_rows(p)
        part_k = jnp.dot(block, wk[where, :], preferred_element_type=F32)
        part_v = jnp.dot(block, wv[where, :], preferred_element_type=F32)
        if fresh_total:
            acc_k[s] = part_k
            acc_v[s] = part_v
        else:
            acc_k[s] += part_k
            acc_v[s] += part_v

    same = (
        lax.broadcasted_iota(jnp.int32, (inner, inner), 0) // HD
        == lax.broadcasted_iota(jnp.int32, (inner, inner), 1) // HD
    )
    pick = lax.broadcasted_iota(jnp.int32, (HD, inner), 0) == lane_iota((HD, inner)) % HD

    @pl.when(mid)
    def _():
        n_arrived(third)
        n_to(third, mate_tp)
        n_share(third)
        for s in main[2:]:
            to_mate(z, s).start()

    own_pieces = end_int * len(main) + (1 - end_int) * pieces

    @pl.loop(0, pieces)
    def _(i):
        s = lax.rem(i + (1 - end_int) * len(main), pieces)

        @pl.when(i < own_pieces)
        def _():
            add(tp, s, True)

        @pl.when(i < own_pieces)
        def _():
            x_arrived(partner, s)
            add(partner, s, False)

    @pl.when(end)
    def _():
        for c in (mate, second, third):
            n_arrived(c)
            n_share(c)

    arrived(nx.at[pl.ds(0, chips)], rn.at[chips])

    def project_new():
        def piece(p, totals):
            where = w_rows(p)
            block = jnp.concatenate(
                [nx[p].astype(F32), jnp.zeros((NEW_ROWS - seqs, feat), F32)], axis=0
            ).astype(BF16)
            return tuple(
                t + jnp.dot(block, w[where, :], preferred_element_type=F32)
                for t, w in zip(totals, (wk, wv, wq))
            )

        zero = jnp.zeros((NEW_ROWS, inner), F32)
        new_k, new_v, new_q = lax.fori_loop(0, n_tp, piece, (zero, zero, zero))
        keys, queries = [], []
        for j in range(inner // LANES):
            at = slice(j * LANES, (j + 1) * LANES)
            keys.append((rotated(new_k[:, at], new_cos, new_sin) * HD**-0.5).astype(BF16))
            queries.append(rotated(new_q[:, at], new_cos, new_sin).astype(BF16))
        key = jnp.concatenate(keys, axis=1).astype(F32)
        query = jnp.concatenate(queries, axis=1).astype(F32)
        value = new_v.astype(BF16).astype(F32)
        product = query * key
        for h in range(heads):
            at = slice(h * HD, (h + 1) * HD)
            own_term[:, at] = jnp.sum(product[:, at], axis=-1, keepdims=True) * value[:, at]
        hint[0:1] = query[moved_seq : moved_seq + 1]
        for s in range(seqs):
            spread = jnp.where(pick, query[s : s + 1], 0.0).astype(BF16)
            q_spread[s] = jnp.dot(
                spread, jnp.where(same, 1.0, 0.0).astype(BF16), preferred_element_type=F32
            )

    project_new()

    @pl.when(end)
    def _():
        hint_copy.start()
        for s in main:
            to_mate(z, s).start()
        for g in range(1, groups):
            for r in range(2):
                for kv in range(2):
                    w_send(1, g, kv, r).start()

    def rs_copy(s, o):
        peer = lax.rem(sp + o, n_sp)
        return remote(
            stage.at[s, peer], landed.at[s, sp], tx.at[rs_tx], rs_rx.at[s], {"sp": peer}
        )

    pl.semaphore_wait(ready.at[0], 2)
    pl.semaphore_signal(ready.at[1], inc=1, device_id={"sp": x_peer}, device_id_type=MESH)

    def y_half(s):
        return remote(
            stage.at[s, pl.ds(2 - 2 * row_y, 2)], landed.at[s, pl.ds(0, 2)],
            tx.at[rs_tx], rs_rx.at[s], {"sp": y_peer},
        )

    def x_half(s):
        return remote(
            stage.at[s, x_peer], landed.at[s, 2], tx.at[rs_tx], rs_rx.at[seqs + s], {"sp": x_peer}
        )

    def outer(weighted, value):
        both = lax.dot_general(
            weighted, value, (((0,), (0,)), ((), ())), preferred_element_type=F32
        )
        return jnp.where(lane_iota((HD, LANES)) < HD, both[:HD], both[HD:])

    def finish(i):
        s, part = i // parts, i % parts
        where = pl.ds(pl.multiple_of(part * size, size), size)
        cosine, sine = cos_ref[0, where, :], sin_ref[0, where, :]
        for j in range(inner // LANES):
            at = slice(j * LANES, (j + 1) * LANES)
            key = (rotated(acc_k[i, :, at], cosine, sine) * HD**-0.5).astype(BF16)
            weighted = (key.astype(F32) * fade_ref[where, at]).astype(BF16)
            value = acc_v[i, :, at].astype(BF16)
            state = outer(weighted, value)
            sums[:, at] = jnp.where(part == 0, state, sums[:, at] + state)

        @pl.when(part == parts - 1)
        def _():
            scaled = sums[...] * rows_ref[0:1]
            read = jnp.sum(scaled * q_spread[s], axis=0, keepdims=True)
            for o in range(n_sp):
                stage[s, o, 0:keep] = scaled[o * keep : (o + 1) * keep]
                stage[s, o, keep : keep + 1] = read
            totals[s] = stage[s, sp]

            @pl.when(end | (s == moved_seq))
            def _():
                for o in range(1, n_sp):
                    rs_copy(s, o).start()

            @pl.when(mid & (s < moved_seq))
            def _():
                y_half(s).start()

    def c_add(cc, p, fresh_total):
        where = w_rows(p)
        for t in range(parts):
            for side, block in ((0, x[p, moved[0] + t]), (1, xc[p, t])):
                both = jnp.dot(block, we[cc, where, :], preferred_element_type=F32)
                if fresh_total:
                    acc_c[side, t] = both
                else:
                    acc_c[side, t] += both

    def c_copy(cc, o):
        return remote(
            stage_c.at[cc, o], landed_c.at[cc, sp], tx.at[c_tx], c_rx.at[cc],
            {"sp": o, "tp": mate_tp},
        )

    def c_finish(cc):
        pair_rate = hint_in[1:2, w_cols(cc)]
        query = hint_in[0:1, w_cols(cc)]
        total = jnp.zeros((HD, LANES), F32)
        for side, column in ((0, sp), (1, y_peer)):
            state = jnp.zeros((HD, LANES), F32)
            for t in range(parts):
                at = slice(t * size, (t + 1) * size)
                key = (
                    rotated(acc_c[side, t, :, :LANES], cos_ref[side, at], sin_ref[side, at])
                    * HD**-0.5
                ).astype(BF16)
                fade = jnp.exp(to_end[at] * pair_rate)
                weighted = (key.astype(F32) * fade).astype(BF16)
                state = state + outer(weighted, acc_c[side, t, :, LANES:].astype(BF16))
            total = total + state * jnp.exp(
                pair_rate * (span * (n_sp - 1 - column)).astype(F32)
            )
        spread = jnp.where(pick[:, :LANES], query, 0.0).astype(BF16)
        spread = jnp.dot(
            spread, jnp.where(same[:LANES, :LANES], 1.0, 0.0).astype(BF16),
            preferred_element_type=F32,
        )
        read = jnp.sum(total * spread, axis=0, keepdims=True)
        for o in range(n_sp):
            stage_c[cc, o, 0:keep] = total[o * keep : (o + 1) * keep]
            stage_c[cc, o, keep : keep + 1] = read
        for o in range(n_sp):
            c_copy(cc, o).start()

    order = middle_order(main, moved)
    steps = end_int * (len(main) * (chips - 1)) + (1 - end_int) * len(order)

    def decode(n):
        kind = end_int * (n // len(main)) + (1 - end_int) * one_of(n, [o[0] for o in order])
        s = end_int * (n % len(main)) + (1 - end_int) * one_of(n, [o[1] for o in order])
        c = (
            (kind == 0).astype(jnp.int32) * mate
            + (kind == 1).astype(jnp.int32) * second
            + (kind == 2).astype(jnp.int32) * third
        )
        return kind, c, s

    first_w = 2 * len(moved) + 1
    c_at = len(order) - 4
    last = len(order) - 1

    def w_pair(cc, g):
        arrived(we.at[cc, w_part(g, None)], w_sem(cc, g, 0, None))
        for kv in range(2):
            w_pass(cc, g, kv).start()

    def w_relay(g, r, kv):
        arrived(w_place(1, g, kv, r), w_sem(1, g, kv, r))
        w_pass(1, g, kv, r).start()

    def w_own(cc, g, fresh_total=False):
        c_add(cc, row_x * groups + g, fresh_total)

    def w_peer(cc, g):
        p = (1 - row_x) * groups + g
        arrived(we.at[cc, w_rows(p)], w_peer_sem(cc, g))
        c_add(cc, p, False)

    def y_pass(c, j):
        arrived(xc.at[2 * c + k, j], ry.at[c * parts + j])
        y_share(c, j).start()

    @pl.loop(0, len(order) + 1)
    def _(n):
        kind, c, s = decode(n)
        is_moved = s >= moved[0]
        kind_b, c_b, s_b = decode(n - 1)

        @pl.when(end & (n >= 1) & (n <= steps))
        def _():
            x_arrived(2 * c_b + 1 - k, s_b)
            add(2 * c_b + 1 - k, s_b, False)

            @pl.when(kind_b == 2)
            def _():
                finish(s_b)

        @pl.when(mid & (n == last - 1))
        def _():
            w_relay(1, 0, 1)

        @pl.when(mid & (n == last))
        def _():
            w_relay(1, 1, 1)

        @pl.when(n < steps)
        def _():
            x_arrived(2 * c + k, s)

            @pl.when(mid & (kind == 0))
            def _():
                to_other(c, s).start()

            @pl.when(mid & (kind > 0) & (s < moved[0]))
            def _():
                to_mate(c, s).start()

            @pl.when(mid & is_moved)
            def _():
                y_send(c, s - moved[0]).start()

            to_partner(c, s).start()

        @pl.when(mid & (n == last - 2))
        def _():
            w_relay(1, 0, 0)

        @pl.when(mid & (n == last - 1))
        def _():
            w_relay(1, 1, 0)

        @pl.when(mid & (n == last))
        def _():
            w_relay(2, 0, 0)

        @pl.when(mid & (n >= first_w) & (n < first_w + groups))
        def _():
            w_pair(0, n - first_w)

        @pl.when(mid & (n == first_w + groups))
        def _():
            w_pair(1, 0)

        @pl.when(mid & (n >= 3) & (n < 3 + parts))
        def _():
            y_pass(z, n - 3)

        @pl.when(mid & (n >= 6) & (n < 6 + 2 * parts))
        def _():
            m = n - 6
            y_pass((m % 2) * second + (1 - m % 2) * mate, m // 2)

        @pl.when(mid & (n >= c_at - parts) & (n < c_at))
        def _():
            y_pass(third, n - (c_at - parts))

        @pl.when(n < steps)
        def _():
            add(2 * c + k, s, False)

        @pl.when(mid & (n == last))
        def _():
            w_relay(2, 0, 1)

        @pl.when(mid & (n >= 1))
        def _():
            x_arrived(2 * c_b + 1 - k, s_b)
            add(2 * c_b + 1 - k, s_b, False)

            @pl.when(n == last + 1)
            def _():
                w_relay(2, 1, 1)

            @pl.when(kind_b == 2)
            def _():
                finish(s_b)

        @pl.when(mid & (n == last))
        def _():
            w_relay(2, 1, 0)

        early = n - (c_at - 5)

        @pl.when(mid & (early == 0))
        def _():
            arrived(xc.at[pl.ds(0, chips - 1)], ry.at[chips * parts])
            arrived(we.at[0, pl.ds(0, groups * feat)], w_peer_sem(0, 0))
            acc_c[...] = jnp.zeros(acc_c.shape, F32)

        @pl.when(mid & (early >= 0) & (early < 6))
        def _():
            turn = early // 2
            cx = (
                (turn == 0).astype(jnp.int32) * z
                + (turn == 1).astype(jnp.int32) * mate
                + (turn == 2).astype(jnp.int32) * second
            )
            c_add(0, 2 * cx + early % 2, False)

        @pl.when(mid & (n == c_at))
        def _():
            arrived(xc.at[0], ry.at[chips * parts + 1])

            @pl.loop(0, 2)
            def _(m):
                c_add(0, 2 * third + m, False)

            hint_copy.wait_recv()
            pl.semaphore_wait(ready.at[1], 1)
            c_finish(0)

    @pl.when(mid)
    def _():
        w_own(1, 0, True)
        w_peer(1, 0)
        w_relay(3, 0, 0)
        w_own(1, 1)
        w_peer(1, 1)
        w_relay(3, 0, 1)
        w_own(1, 2)
        w_relay(3, 1, 0)
        w_relay(3, 1, 1)
        w_peer(1, 2)
        w_own(1, 3)
        for s in range(moved_seq):
            arrived(landed.at[s, pl.ds(0, 2)], rs_rx.at[s])
            for side in range(2):
                stage[s, 2 * row_y + side] += landed[s, side]
        w_peer(1, 3)
        for s in range(moved_seq):
            x_half(s).start()
        c_finish(1)

    def gather(s):
        arrived(landed.at[s, pl.ds(0, n_sp - 1)], rs_rx.at[s])
        total = None
        for j in range(n_sp):
            term = jnp.where(sp == j, totals[s], landed[s, j])
            total = term if total is None else total + term
        totals[s] = total

    sent(nx.at[pl.ds(0, chips)], n_share_tx)

    @pl.when(end)
    def _():
        pl.semaphore_wait(ready.at[1], 1)
        sent(nx.at[0], n_tx)
        sent(hint, hint_tx)
        sent(x.at[0], to_mate_tx)
        sent(x.at[pl.ds(0, chips), pl.ds(0, len(main))], share_tx)
        sent(we.at[pl.ds(0, chunks), pl.ds(0, groups * feat)], w_tx)
        sent(stage.at[pl.ds(0, moved_seq), pl.ds(0, n_sp - 1)], rs_tx)

    @pl.when(mid)
    def _():
        sent(nx.at[pl.ds(0, 5)], n_tx)
        sent(x.at[pl.ds(0, chips - 1), pl.ds(0, len(main))], to_mate_tx)
        sent(x.at[pl.ds(0, 2)], to_other_tx)
        sent(x.at[pl.ds(0, chips)], share_tx)
        sent(xc.at[pl.ds(0, chips)], y_tx)
        sent(xc.at[pl.ds(0, chips)], y_share_tx)
        sent(we.at[pl.ds(0, chunks), pl.ds(0, groups * feat)], w_pass_tx)
        sent(stage.at[:, pl.ds(0, n_sp - 1)], rs_tx)

    @pl.when(mid)
    def _():
        for s in range(moved_seq):
            arrived(landed.at[s, 2], rs_rx.at[seqs + s])
            totals[s] = stage[s, sp] + landed[s, 2]
        gather(moved_seq)

    @pl.when(end)
    def _():
        for s in range(moved_seq):
            gather(s)
        for cc in range(chunks):
            arrived(landed_c.at[cc], c_rx.at[cc])
            for side in range(2):
                at = slice(side * half + cc * LANES, side * half + (cc + 1) * LANES)
                totals[moved_seq, :, at] = landed_c[cc, 2 * side] + landed_c[cc, 2 * side + 1]

    for s in range(seqs):
        read = totals[s, keep : keep + 1]
        totals[s, keep : keep + 1] = read * rows_ref[1:2] + own_term[s : s + 1]

    @pl.when(mid)
    def _():
        sent(stage_c, c_tx)


def solution(mesh):
    n_sp, n_tp = mesh.shape["sp"], mesh.shape["tp"]

    def body(tokens, new_token, query_weight, key_weight, value_weight, log_decay):
        seqs, span, feat = tokens.shape
        width, inner = key_weight.shape
        heads = inner // HD
        keep = HD // n_sp
        rows = -(-(keep + 1) // 8) * 8
        chips = n_tp // 2
        half = HD // 2
        parts = max(1, 8 // chips)
        pieces = seqs * parts
        size = span // parts
        inverse = jnp.asarray(np.tile(inverse_angles(), LANES // half)[None])
        anywhere = pl.BlockSpec(memory_space=pl.ANY)
        vmem = pl.BlockSpec(memory_space=pltpu.VMEM)
        dma = pltpu.SemaphoreType.DMA
        moves = chips == 4 and n_sp == 4 and seqs > 1 and inner == 4 * LANES
        tokens_in = [
            pltpu.VMEM((n_tp, pieces, size, feat), BF16),
            pltpu.VMEM((n_tp, seqs, feat), BF16),
        ]
        weights_in = [pltpu.VMEM((width, inner), BF16)] * 3
        totals = [pltpu.VMEM((pieces, size, inner), F32)] * 2
        ends = [
            pltpu.VMEM((8, inner), F32),
            pltpu.VMEM((seqs, HD, inner), F32),
            pltpu.VMEM((NEW_ROWS, inner), F32),
            pltpu.VMEM((HD, inner), F32),
            pltpu.VMEM((seqs, n_sp, rows, inner), F32),
            pltpu.VMEM((seqs, n_sp, rows, inner), F32),
        ]
        if moves:
            chunks = inner // 2 // LANES
            groups = n_tp // 2
            call = moved_kernel
            scratch = (
                tokens_in[:1]
                + [pltpu.VMEM((n_tp, parts, size, feat), BF16)]
                + tokens_in[1:]
                + weights_in
                + [pltpu.VMEM((chunks, width, 2 * LANES), BF16)]
                + totals
                + [
                    pltpu.VMEM((2, parts, size, 2 * LANES), F32),
                    pltpu.VMEM((2, span, LANES), F32),
                    pltpu.VMEM((2, span, LANES), F32),
                    pltpu.VMEM((span, inner), F32),
                ]
                + ends
                + [
                    pltpu.VMEM((8, inner), F32),
                    pltpu.VMEM((8, inner), F32),
                    pltpu.VMEM((chunks, n_sp, rows, LANES), F32),
                    pltpu.VMEM((chunks, n_sp, rows, LANES), F32),
                    dma((pieces + 1,)),
                    dma((3,)),
                    dma((n_tp, pieces)),
                    dma((chips + 1,)),
                    dma((chips * parts + 2,)),
                    dma((6 * groups - 2,)),
                    dma((12,)),
                    dma((1,)),
                    dma((2 * seqs,)),
                    dma((chunks,)),
                    pltpu.SemaphoreType.REGULAR((2,)),
                ]
            )
        else:
            call = kernel
            scratch = (
                tokens_in
                + weights_in
                + totals
                + [
                    pltpu.VMEM((span, LANES), F32),
                    pltpu.VMEM((span, LANES), F32),
                    pltpu.VMEM((span, inner), F32),
                ]
                + ends
                + [
                    pltpu.VMEM((seqs, rows, inner), F32),
                    dma((pieces + 1,)),
                    dma((3,)),
                    dma((n_tp, pieces)),
                    dma((n_tp,)),
                    dma((2, chips, pieces)),
                    dma((chips, pieces)),
                    dma((2, chips)),
                    dma((chips,)),
                    dma((seqs, n_sp)),
                    dma((seqs, n_sp)),
                ]
            )
        out_shape = (
            jax.ShapeDtypeStruct((seqs, heads, keep, HD), BF16),
            jax.ShapeDtypeStruct((seqs, inner), BF16),
        )
        shared = dict(
            scratch_shapes=scratch,
            name="retention",
        )
        args = (
            tokens, new_token.reshape(seqs, feat), query_weight, key_weight, value_weight
        )
        args = tuple(pltpu.with_memory_space_constraint(a, pltpu.HBM) for a in args)
        smem = pl.BlockSpec(memory_space=pltpu.SMEM)
        limit = (53 if moves else 60) * 1024 * 1024
        params = pltpu.CompilerParams(
            collective_id=0, has_side_effects=True, vmem_limit_bytes=limit
        )
        call = functools.partial(call, n_sp, n_tp, parts)
        if not moves:
            return pl.pallas_call(
                call,
                out_shape=out_shape,
                in_specs=[anywhere] * 5 + [vmem, smem],
                out_specs=(vmem, vmem),
                compiler_params=params,
                **shared,
            )(*args, inverse, log_decay)
        sums = pl.pallas_call(
            call,
            out_shape=jax.ShapeDtypeStruct((seqs, rows, inner), F32),
            in_specs=[anywhere] * 5 + [smem],
            out_specs=vmem,
            compiler_params=params,
            **shared,
        )(*args, pltpu.with_memory_space_constraint(log_decay, pltpu.HBM))
        return pl.pallas_call(
            outputs,
            out_shape=out_shape,
            in_specs=[vmem],
            out_specs=(vmem, vmem),
            compiler_params=pltpu.CompilerParams(vmem_limit_bytes=4 * 1024 * 1024),
            name="outputs",
        )(sums)

    return jax.shard_map(
        body,
        mesh=mesh,
        in_specs=(
            P(None, "sp", "tp"),
            P(None, None, "tp"),
            P(None, "tp"),
            P(None, "tp"),
            P(None, "tp"),
            P("tp"),
        ),
        out_specs=(P(None, "tp", "sp", None), P(None, "tp")),
        check_vma=False,
    )
```

```python
import functools

import jax
import jax.numpy as jnp
import numpy as np
from jax import lax
from jax.experimental import pallas as pl
from jax.experimental.pallas import tpu as pltpu
from jax.sharding import PartitionSpec as P

HD = 64
LANES = 128
NEW_ROWS = 8
F32 = jnp.float32
BF16 = jnp.bfloat16


def inverse_angles():
    half = HD // 2
    return np.float32(10000.0) ** (-np.arange(half, dtype=np.float32) / half)


def lane_iota(shape):
    return lax.broadcasted_iota(jnp.int32, shape, len(shape) - 1)


def rotated(block, cosine, sine):
    half = HD // 2
    low = lane_iota(block.shape) % HD < half
    swapped = jnp.where(
        low, pltpu.roll(block, LANES - half, 1), pltpu.roll(block, half, 1)
    )
    return block * cosine + swapped * sine


def kernel(
    n_sp, n_tp, parts,
    tokens, fresh, wq_hbm, wk_hbm, wv_hbm, inverse_ref, decay_ref,
    state_out, read_out,
    x, nx, wq, wk, wv, acc_k, acc_v, cos_ref, sin_ref, fade_ref, rows_ref,
    q_spread, own_term, sums, stage, landed, totals,
    load_sem, weight_sem, rx, rn, fwd, share, nfwd, nshare, rs_tx, rs_rx,
):
    seqs, span, feat = tokens.shape
    inner = wk.shape[1]
    heads = inner // HD
    chips = n_tp // 2
    pieces = seqs * parts
    size = span // parts
    keep = HD // n_sp
    sp = lax.axis_index("sp")
    tp = lax.axis_index("tp")
    z, k = tp // 2, tp % 2
    MESH = pl.DeviceIdType.MESH

    def to_tp(index):
        return {"tp": index}

    partner = z * 2 + 1 - k
    own_loads = [
        pltpu.make_async_copy(
            tokens.at[s // parts, pl.ds(s % parts * size, size)], x.at[tp, s], load_sem.at[s]
        )
        for s in range(pieces)
    ]
    new_load = pltpu.make_async_copy(fresh, nx.at[tp], load_sem.at[pieces])
    new_load.start()
    for copy in own_loads:
        copy.start()
    weight_loads = [
        pltpu.make_async_copy(a, b, weight_sem.at[i])
        for i, (a, b) in enumerate(((wk_hbm, wk), (wv_hbm, wv), (wq_hbm, wq)))
    ]

    barrier = pltpu.get_barrier_semaphore()

    @pl.when(z > 0)
    def _():
        pl.semaphore_signal(barrier, inc=1, device_id=to_tp(tp - 2), device_id_type=MESH)

    @pl.when(z < chips - 1)
    def _():
        pl.semaphore_signal(barrier, inc=1, device_id=to_tp(tp + 2), device_id_type=MESH)

    pl.semaphore_signal(barrier, inc=1, device_id=to_tp(partner), device_id_type=MESH)
    for o in range(1, n_sp):
        pl.semaphore_signal(
            barrier, inc=1, device_id={"sp": lax.rem(sp + o, n_sp)}, device_id_type=MESH
        )
    pl.semaphore_wait(
        barrier, n_sp + (z > 0).astype(jnp.int32) + (z < chips - 1).astype(jnp.int32)
    )

    def x_copy(c, s, sem, target):
        p = 2 * c + k
        return pltpu.make_async_remote_copy(
            x.at[p, s], x.at[p, s], sem, rx.at[p, s], device_id=to_tp(target), device_id_type=MESH
        )

    def n_copy(c, sem, target):
        p = 2 * c + k
        return pltpu.make_async_remote_copy(
            nx.at[p], nx.at[p], sem, rn.at[p], device_id=to_tp(target), device_id_type=MESH
        )

    def x_arrived(p, s):
        pltpu.make_async_remote_copy(
            x.at[p, s], x.at[p, s], share.at[0, 0], rx.at[p, s],
            device_id=to_tp(partner), device_id_type=MESH,
        ).wait_recv()

    def n_arrived(p):
        pltpu.make_async_remote_copy(
            nx.at[p], nx.at[p], nshare.at[0], rn.at[p],
            device_id=to_tp(partner), device_id_type=MESH,
        ).wait_recv()

    new_load.wait()
    n_up = n_copy(z, nfwd.at[0, z], tp + 2)
    n_down = n_copy(z, nfwd.at[1, z], tp - 2)
    n_side = n_copy(z, nshare.at[z], partner)

    @pl.when(z < chips - 1)
    def _():
        n_up.start()

    @pl.when(z > 0)
    def _():
        n_down.start()

    n_side.start()
    for s in range(pieces):
        own_loads[s].wait()

        @pl.when(z < chips - 1)
        def _(s=s):
            x_copy(z, s, fwd.at[0, z, s], tp + 2).start()

        @pl.when(z > 0)
        def _(s=s):
            x_copy(z, s, fwd.at[1, z, s], tp - 2).start()

        x_copy(z, s, share.at[z, s], partner).start()

    for copy in weight_loads:
        copy.start()

    row = lax.broadcasted_iota(jnp.int32, (span, LANES), 0)
    within = lane_iota((1, LANES)) % HD
    first_half = jnp.where(within < HD // 2, -1.0, 1.0).astype(F32)
    inverse = inverse_ref[...]
    angles = (sp * span + row).astype(F32) * inverse
    cos_ref[...] = jnp.cos(angles)
    sin_ref[...] = jnp.sin(angles) * first_half
    new_angles = jnp.full((NEW_ROWS, LANES), n_sp * span, F32) * inverse
    new_cos = jnp.cos(new_angles)
    new_sin = jnp.sin(new_angles) * first_half
    head_of = lane_iota((1, inner)) // HD
    rate = jnp.zeros((1, inner), F32)
    for h in range(heads):
        rate = jnp.where(head_of == h, decay_ref[h], rate)
    to_end = (span - 1 - lax.broadcasted_iota(jnp.int32, (span, 1), 0)).astype(F32)
    fade_ref[...] = jnp.exp(to_end * rate)
    rows_ref[0:1] = jnp.exp(rate * (span * (n_sp - 1 - sp)).astype(F32))
    rows_ref[1:2] = jnp.exp(rate)

    for copy in weight_loads:
        copy.wait()

    def add(p, s, fresh_total):
        block = x[p, s]
        where = pl.ds(pl.multiple_of(p * feat, feat), feat)
        part_k = jnp.dot(block, wk[where, :], preferred_element_type=F32)
        part_v = jnp.dot(block, wv[where, :], preferred_element_type=F32)
        if fresh_total:
            acc_k[s] = part_k
            acc_v[s] = part_v
        else:
            acc_k[s] += part_k
            acc_v[s] += part_v

    @pl.loop(0, pieces)
    def _(s):
        add(tp, s, True)
        x_arrived(partner, s)
        add(partner, s, False)

    n_arrived(partner)

    def project_new():
        def piece(p, totals):
            where = pl.ds(pl.multiple_of(p * feat, feat), feat)
            block = jnp.concatenate(
                [nx[p].astype(F32), jnp.zeros((NEW_ROWS - seqs, feat), F32)], axis=0
            ).astype(BF16)
            return tuple(
                t + jnp.dot(block, w[where, :], preferred_element_type=F32)
                for t, w in zip(totals, (wk, wv, wq))
            )

        zero = jnp.zeros((NEW_ROWS, inner), F32)
        new_k, new_v, new_q = lax.fori_loop(0, n_tp, piece, (zero, zero, zero))
        keys, queries = [], []
        for j in range(inner // LANES):
            at = slice(j * LANES, (j + 1) * LANES)
            keys.append((rotated(new_k[:, at], new_cos, new_sin) * HD**-0.5).astype(BF16))
            queries.append(rotated(new_q[:, at], new_cos, new_sin).astype(BF16))
        key = jnp.concatenate(keys, axis=1).astype(F32)
        query = jnp.concatenate(queries, axis=1).astype(F32)
        value = new_v.astype(BF16).astype(F32)
        same = (
            lax.broadcasted_iota(jnp.int32, (inner, inner), 0) // HD
            == lax.broadcasted_iota(jnp.int32, (inner, inner), 1) // HD
        )
        product = query * key
        for h in range(heads):
            at = slice(h * HD, (h + 1) * HD)
            own_term[:, at] = jnp.sum(product[:, at], axis=-1, keepdims=True) * value[:, at]
        pick = lax.broadcasted_iota(jnp.int32, (HD, inner), 0) == lane_iota((HD, inner)) % HD
        for s in range(seqs):
            spread = jnp.where(pick, query[s : s + 1], 0.0).astype(BF16)
            q_spread[s] = jnp.dot(
                spread, jnp.where(same, 1.0, 0.0).astype(BF16), preferred_element_type=F32
            )

    def rs_copy(s, o):
        peer = lax.rem(sp + o, n_sp)
        return pltpu.make_async_remote_copy(
            stage.at[s, peer], landed.at[s, sp], rs_tx.at[s, peer], rs_rx.at[s, sp],
            device_id={"sp": peer}, device_id_type=MESH,
        )

    def finish(i):
        s, part = i // parts, i % parts
        where = pl.ds(pl.multiple_of(part * size, size), size)
        cosine, sine = cos_ref[where, :], sin_ref[where, :]
        lane = lane_iota((HD, LANES))
        for j in range(inner // LANES):
            at = slice(j * LANES, (j + 1) * LANES)
            key = (rotated(acc_k[i, :, at], cosine, sine) * HD**-0.5).astype(BF16)
            weighted = (key.astype(F32) * fade_ref[where, at]).astype(BF16)
            value = acc_v[i, :, at].astype(BF16)
            both = lax.dot_general(
                weighted, value, (((0,), (0,)), ((), ())), preferred_element_type=F32
            )
            state = jnp.where(lane < HD, both[:HD], both[HD:])
            sums[:, at] = jnp.where(part == 0, state, sums[:, at] + state)

        @pl.when(part == parts - 1)
        def _():
            scaled = sums[...] * rows_ref[0:1]
            read = jnp.sum(scaled * q_spread[s], axis=0, keepdims=True)
            for o in range(n_sp):
                stage[s, o, 0:keep] = scaled[o * keep : (o + 1) * keep]
                stage[s, o, keep : keep + 1] = read
            for o in range(1, n_sp):
                rs_copy(s, o).start()
            totals[s] = stage[s, sp]

    far = jnp.maximum(z, chips - 1 - z)

    def decode(i):
        d = i // (2 * pieces) + 1
        s = (i // 2) % pieces
        step = 2 * (i % 2) - 1
        c = z + step * d
        return d, s, step, c, (c >= 0) & (c < chips)

    def onward(step):
        nxt = z - step
        return nxt, (nxt >= 0) & (nxt < chips), (step + 1) // 2

    @pl.loop(0, 2 * pieces * (chips - 1))
    def _(i):
        d, s, step, c, valid = decode(i)
        nxt, pass_on, way = onward(step)

        @pl.when(valid)
        def _():
            @pl.when(s == 0)
            def _():
                n_arrived(2 * c + k)

                @pl.when(pass_on)
                def _():
                    n_copy(c, nfwd.at[way, c], 2 * nxt + k).start()

                n_copy(c, nshare.at[c], partner).start()

            x_arrived(2 * c + k, s)

            @pl.when(pass_on)
            def _():
                x_copy(c, s, fwd.at[way, c, s], 2 * nxt + k).start()

            x_copy(c, s, share.at[c, s], partner).start()
            add(2 * c + k, s, False)

            @pl.when(s == 0)
            def _():
                n_arrived(2 * c + 1 - k)

            x_arrived(2 * c + 1 - k, s)
            add(2 * c + 1 - k, s, False)

        last = (d == far) & (step == 1)

        @pl.when(last & (s == 0))
        def _():
            project_new()

        @pl.when(last)
        def _():
            finish(s)

    raws = []
    for s in range(seqs):
        for o in range(1, n_sp):
            src = lax.rem(sp + o, n_sp)
            pltpu.make_async_remote_copy(
                stage.at[s, src], landed.at[s, src], rs_tx.at[s, src], rs_rx.at[s, src],
                device_id={"sp": src}, device_id_type=MESH,
            ).wait_recv()
        total = None
        for j in range(n_sp):
            term = jnp.where(sp == j, totals[s], landed[s, j])
            total = term if total is None else total + term
        kept = total[0:keep].astype(BF16)
        for h in range(heads):
            state_out[s, h] = kept[:, h * HD : (h + 1) * HD]
        raws.append(total[keep : keep + 1] * rows_ref[1:2] + own_term[s : s + 1])
    raw = jnp.concatenate(raws, axis=0)
    for h in range(heads):
        at = slice(h * HD, (h + 1) * HD)
        head = raw[:, at]
        centered = head - jnp.mean(head, axis=-1, keepdims=True)
        spread = jnp.mean(centered * centered, axis=-1, keepdims=True)
        read_out[:, at] = (centered * lax.rsqrt(spread + 1e-05)).astype(BF16)

    @pl.when(z < chips - 1)
    def _():
        n_up.wait_send()

    @pl.when(z > 0)
    def _():
        n_down.wait_send()

    n_side.wait_send()
    for s in range(seqs):
        for o in range(1, n_sp):
            rs_copy(s, o).wait_send()
    for s in range(pieces):
        @pl.when(z < chips - 1)
        def _(s=s):
            x_copy(z, s, fwd.at[0, z, s], tp + 2).wait_send()

        @pl.when(z > 0)
        def _(s=s):
            x_copy(z, s, fwd.at[1, z, s], tp - 2).wait_send()

        x_copy(z, s, share.at[z, s], partner).wait_send()

    @pl.loop(0, 2 * pieces * (chips - 1))
    def _(i):
        d, s, step, c, valid = decode(i)
        nxt, pass_on, way = onward(step)

        @pl.when(valid)
        def _():
            @pl.when(s == 0)
            def _():
                @pl.when(pass_on)
                def _():
                    n_copy(c, nfwd.at[way, c], 2 * nxt + k).wait_send()

                n_copy(c, nshare.at[c], partner).wait_send()

            @pl.when(pass_on)
            def _():
                x_copy(c, s, fwd.at[way, c, s], 2 * nxt + k).wait_send()

            x_copy(c, s, share.at[c, s], partner).wait_send()


def one_of(n, values):
    total = 0
    for k, value in enumerate(values):
        if value:
            total = total + (n == k).astype(jnp.int32) * value
    return total


def middle_order(main, moved):
    near = [(0, i) for i in main]
    far = [(2, i) for i in moved + main]
    order = [(kind, i) for i in moved for kind in (0, 1)]
    order += [(1, i) for i in main]
    for at in range(max(len(near), len(far))):
        order += far[at : at + 1] + near[at : at + 1]
    return order


def outputs(totals, state_out, read_out, state, read, sem):
    seqs, heads, keep, _ = state_out.shape
    raws = []
    for s in range(seqs):
        kept = totals[s, 0:keep].astype(BF16)
        for h in range(heads):
            state[s, h] = kept[:, h * HD : (h + 1) * HD]
        raws.append(totals[s, keep : keep + 1])
    state_copy = pltpu.make_async_copy(state, state_out, sem.at[0])
    state_copy.start()
    raw = jnp.concatenate(raws, axis=0)
    for h in range(heads):
        at = slice(h * HD, (h + 1) * HD)
        head = raw[:, at]
        centered = head - jnp.mean(head, axis=-1, keepdims=True)
        spread = jnp.mean(centered * centered, axis=-1, keepdims=True)
        read[:, at] = (centered * lax.rsqrt(spread + 1e-05)).astype(BF16)
    read_copy = pltpu.make_async_copy(read, read_out, sem.at[1])
    read_copy.start()
    state_copy.wait()
    read_copy.wait()


def moved_kernel(
    n_sp, n_tp, parts,
    tokens, fresh, wq_hbm, wk_hbm, wv_hbm, decay_ref,
    totals,
    x, xc, nx, wq, wk, wv, we, acc_k, acc_v, acc_c, cos_ref, sin_ref, fade_ref, rows_ref,
    q_spread, own_term, sums, stage, landed, hint, hint_in, stage_c, landed_c,
    load_sem, weight_sem, rx, rn, ry, rw, tx, hint_rx, rs_rx, c_rx, ready,
):
    seqs, span, feat = tokens.shape
    inner = wk.shape[1]
    heads = inner // HD
    half = inner // 2
    chips = n_tp // 2
    pieces = seqs * parts
    size = span // parts
    keep = HD // n_sp
    units = n_tp
    early = n_tp - 3
    moved_seq = seqs - 1
    to_mate_tx, to_other_tx, share_tx, n_tx, n_share_tx, token_tx, token_share_tx, w_tx = range(8)
    hint_tx, rs_tx, c_tx = range(8, 11)
    main = list(range(moved_seq * parts))
    moved = list(range(moved_seq * parts, pieces))
    sp = lax.axis_index("sp")
    tp = lax.axis_index("tp")
    z, k = tp // 2, tp % 2
    row_y, row_x = sp // 2, sp % 2
    x_peer = sp + 1 - 2 * row_x
    y_peer = sp + 2 - 4 * row_y
    columns = (sp, x_peer, y_peer, x_peer + y_peer - sp)
    MESH = pl.DeviceIdType.MESH
    end_int = (z == 0).astype(jnp.int32) + (z == chips - 1).astype(jnp.int32)
    end = end_int > 0
    mid = end_int == 0
    partner = z * 2 + 1 - k
    mate = z + 1 - 2 * (z % 2)
    mate_tp = 2 * mate + k
    other = chips - 1 - z
    other_tp = 2 * other + k
    second = end_int * (chips - 1 - mate) + (1 - end_int) * (chips - 1 - z)
    third = end_int * (chips - 1 - z) + (1 - end_int) * (chips - 1 - mate)

    own_loads = {
        s: pltpu.make_async_copy(
            tokens.at[s // parts, pl.ds(s % parts * size, size)], x.at[tp, s], load_sem.at[s]
        )
        for s in range(pieces)
    }
    new_load = pltpu.make_async_copy(fresh, nx.at[tp], load_sem.at[pieces])
    new_load.start()
    for s in moved + main:
        own_loads[s].start()
    weight_loads = [
        pltpu.make_async_copy(a, b, weight_sem.at[i])
        for i, (a, b) in enumerate(((wk_hbm, wk), (wv_hbm, wv), (wq_hbm, wq)))
    ]

    barrier = pltpu.get_barrier_semaphore()
    for target in ({"tp": partner}, {"tp": mate_tp}, {"sp": x_peer}, {"sp": y_peer}):
        pl.semaphore_signal(barrier, inc=1, device_id=target, device_id_type=MESH)

    @pl.when(mid)
    def _():
        pl.semaphore_signal(barrier, inc=1, device_id={"tp": other_tp}, device_id_type=MESH)

    pl.semaphore_wait(barrier, 5 - end_int)
    for target in ({"sp": x_peer}, {"sp": y_peer}):
        pl.semaphore_signal(ready.at[0], inc=1, device_id=target, device_id_type=MESH)

    def remote(source, dest, send, recv, target):
        return pltpu.make_async_remote_copy(
            source, dest, send, recv, device_id=target, device_id_type=MESH
        )

    def sent(ref, kind):
        remote(ref, ref, tx.at[kind], hint_rx.at[0], {"tp": partner}).wait_send()

    def arrived(ref, sem):
        remote(ref, ref, tx.at[0], sem, {"tp": partner}).wait_recv()

    def x_copy(c, s, kind, target):
        here = x.at[2 * c + k, s]
        return remote(here, here, tx.at[kind], rx.at[2 * c + k, s], {"tp": target})

    def to_mate(c, s):
        return x_copy(c, s, to_mate_tx, mate_tp)

    def to_other(c, s):
        return x_copy(c, s, to_other_tx, other_tp)

    def to_partner(c, s):
        return x_copy(c, s, share_tx, partner)

    def x_arrived(p, s):
        arrived(x.at[p, s], rx.at[p, s])

    def token_send(c, j):
        here = x.at[2 * c + k, moved[0] + j]
        for slot, target in ((0, x_peer), (1, y_peer)):
            remote(
                here, xc.at[slot, 2 * c + k, j], tx.at[token_tx],
                ry.at[(slot * chips + c) * parts + j], {"sp": target},
            ).start()

    def token_pass(slot, c, j):
        p = 2 * c + k
        here = xc.at[slot, p, j]
        arrived(here, ry.at[(slot * chips + c) * parts + j])
        if slot < 2 and slot == j % 2:
            remote(
                here, xc.at[2, p, j], tx.at[token_tx],
                ry.at[(2 * chips + c) * parts + j], {"sp": y_peer if slot == 0 else x_peer},
            ).start()
        remote(
            here, here, tx.at[token_share_tx], ry.at[3 * chips * parts + c], {"tp": partner}
        ).start()

    def w_rows(p):
        return pl.ds(pl.multiple_of(p * feat, feat), feat)

    def w_cols():
        return pl.ds(pl.multiple_of(row_y * half + row_x * LANES, LANES), LANES)

    def w_sem(u, kv):
        return rw.at[u + (kv if u == units - 1 else 0)]

    def w_send(u, kv):
        rows = w_rows(2 * (mate, z, second, third)[u // 2] + u % 2)
        return remote(
            (wk, wv)[kv].at[rows, w_cols()], we.at[rows, pl.ds(kv * LANES, LANES)],
            tx.at[w_tx], w_sem(u, kv), {"tp": mate_tp},
        )

    def n_copy(c, kind, sem, target):
        here = nx.at[2 * c + k]
        return remote(here, here, tx.at[kind], sem, {"tp": target})

    def n_to(c, target):
        n_copy(c, n_tx, rn.at[c], target).start()

    def n_share(c):
        n_copy(c, n_share_tx, rn.at[chips], partner).start()

    def n_arrived(c):
        arrived(nx.at[2 * c + k], rn.at[c])

    hint_copy = remote(hint, hint_in, tx.at[hint_tx], hint_rx.at[0], {"tp": mate_tp})

    new_load.wait()
    n_to(z, mate_tp)
    n_share(z)

    @pl.when(mid)
    def _():
        n_to(z, other_tp)

    for s in moved + main:
        own_loads[s].wait()

    def send_moved(j):
        s = moved[j]

        @pl.when(mid)
        def _():
            to_other(z, s).start()
            token_send(z, j)
            to_partner(z, s).start()

        @pl.when(end)
        def _():
            to_mate(z, s).start()

    send_moved(0)
    to_partner(z, main[0]).start()

    @pl.when(mid)
    def _():
        to_mate(z, main[0]).start()

    for copy in weight_loads:
        copy.start()

    @pl.when(mid)
    def _():
        n_arrived(mate)
        n_to(mate, other_tp)
        n_share(mate)
        n_arrived(other)
        n_to(other, mate_tp)
        n_share(other)

    for j in range(1, parts):
        send_moved(j)
    for s in main[1:]:
        to_partner(z, s).start()

    @pl.when(mid)
    def _():
        for s in main[1:2]:
            to_mate(z, s).start()
        for s in main:
            to_other(z, s).start()

    row = lax.broadcasted_iota(jnp.int32, (span, LANES), 0)
    within = lane_iota((1, LANES)) % HD
    first_half = jnp.where(within < HD // 2, -1.0, 1.0).astype(F32)
    inverse = jnp.zeros((1, LANES), F32)
    for j, step in enumerate(inverse_angles()):
        inverse = jnp.where(within % (HD // 2) == j, float(step), inverse)

    def tables(slot, column):
        angles = (column * span + row).astype(F32) * inverse
        cos_ref[slot] = jnp.cos(angles)
        sin_ref[slot] = jnp.sin(angles) * first_half

    for copy in weight_loads[:2]:
        copy.wait()

    @pl.when(end)
    def _():
        for u in range(early):
            for kv in range(2):
                w_send(u, kv).start()

    tables(0, sp)

    @pl.when(mid)
    def _():
        for slot in range(1, len(columns)):
            tables(slot, columns[slot])

    new_angles = jnp.full((NEW_ROWS, LANES), n_sp * span, F32) * inverse
    new_cos = jnp.cos(new_angles)
    new_sin = jnp.sin(new_angles) * first_half
    head_of = lane_iota((1, inner)) // HD
    rate = jnp.zeros((1, inner), F32)
    for h in range(heads):
        rate = jnp.where(head_of == h, decay_ref[h], rate)
    to_end = (span - 1 - lax.broadcasted_iota(jnp.int32, (span, 1), 0)).astype(F32)
    fade_ref[...] = jnp.exp(to_end * rate)
    rows_ref[0:1] = jnp.exp(rate * (span * (n_sp - 1 - sp)).astype(F32))
    rows_ref[1:2] = jnp.exp(rate)
    hint[...] = jnp.zeros(hint.shape, F32)
    hint[1:2] = rate
    weight_loads[2].wait()

    def add(p, s, fresh_total):
        block = x[p, s]
        where = w_rows(p)
        part_k = jnp.dot(block, wk[where, :], preferred_element_type=F32)
        part_v = jnp.dot(block, wv[where, :], preferred_element_type=F32)
        if fresh_total:
            acc_k[s] = part_k
            acc_v[s] = part_v
        else:
            acc_k[s] += part_k
            acc_v[s] += part_v

    same = (
        lax.broadcasted_iota(jnp.int32, (inner, inner), 0) // HD
        == lax.broadcasted_iota(jnp.int32, (inner, inner), 1) // HD
    )
    pick = lax.broadcasted_iota(jnp.int32, (HD, inner), 0) == lane_iota((HD, inner)) % HD

    @pl.when(mid)
    def _():
        n_arrived(third)
        n_to(third, mate_tp)
        n_share(third)
        for s in main[2:]:
            to_mate(z, s).start()

    own_pieces = end_int * len(main) + (1 - end_int) * pieces

    @pl.loop(0, pieces)
    def _(i):
        s = lax.rem(i + (1 - end_int) * len(main), pieces)

        @pl.when(i < own_pieces)
        def _():
            add(tp, s, True)

        @pl.when(i < own_pieces)
        def _():
            x_arrived(partner, s)
            add(partner, s, False)

    @pl.when(end)
    def _():
        for c in (mate, second, third):
            n_arrived(c)
            n_share(c)

    arrived(nx.at[pl.ds(0, chips)], rn.at[chips])

    def project_new():
        def piece(p, totals):
            where = w_rows(p)
            block = jnp.concatenate(
                [nx[p].astype(F32), jnp.zeros((NEW_ROWS - seqs, feat), F32)], axis=0
            ).astype(BF16)
            return tuple(
                t + jnp.dot(block, w[where, :], preferred_element_type=F32)
                for t, w in zip(totals, (wk, wv, wq))
            )

        zero = jnp.zeros((NEW_ROWS, inner), F32)
        new_k, new_v, new_q = lax.fori_loop(0, n_tp, piece, (zero, zero, zero))
        keys, queries = [], []
        for j in range(inner // LANES):
            at = slice(j * LANES, (j + 1) * LANES)
            keys.append((rotated(new_k[:, at], new_cos, new_sin) * HD**-0.5).astype(BF16))
            queries.append(rotated(new_q[:, at], new_cos, new_sin).astype(BF16))
        key = jnp.concatenate(keys, axis=1).astype(F32)
        query = jnp.concatenate(queries, axis=1).astype(F32)
        value = new_v.astype(BF16).astype(F32)
        product = query * key
        for h in range(heads):
            at = slice(h * HD, (h + 1) * HD)
            own_term[:, at] = jnp.sum(product[:, at], axis=-1, keepdims=True) * value[:, at]
        hint[0:1] = query[moved_seq : moved_seq + 1]
        for s in range(seqs):
            spread = jnp.where(pick, query[s : s + 1], 0.0).astype(BF16)
            q_spread[s] = jnp.dot(
                spread, jnp.where(same, 1.0, 0.0).astype(BF16), preferred_element_type=F32
            )

    project_new()

    @pl.when(end)
    def _():
        hint_copy.start()
        for s in main:
            to_mate(z, s).start()
        for u in range(early, units):
            for kv in range(2):
                w_send(u, kv).start()

    def rs_copy(s, o):
        peer = lax.rem(sp + o, n_sp)
        return remote(
            stage.at[s, peer], landed.at[s, sp], tx.at[rs_tx], rs_rx.at[s], {"sp": peer}
        )

    pl.semaphore_wait(ready.at[0], 2)
    pl.semaphore_signal(ready.at[1], inc=1, device_id={"sp": x_peer}, device_id_type=MESH)

    def y_half(s):
        return remote(
            stage.at[s, pl.ds(2 - 2 * row_y, 2)], landed.at[s, pl.ds(0, 2)],
            tx.at[rs_tx], rs_rx.at[s], {"sp": y_peer},
        )

    def x_half(s):
        return remote(
            stage.at[s, x_peer], landed.at[s, 2], tx.at[rs_tx], rs_rx.at[seqs + s], {"sp": x_peer}
        )

    def outer(weighted, value):
        both = lax.dot_general(
            weighted, value, (((0,), (0,)), ((), ())), preferred_element_type=F32
        )
        return jnp.where(lane_iota((HD, LANES)) < HD, both[:HD], both[HD:])

    def finish(i):
        s, part = i // parts, i % parts
        where = pl.ds(pl.multiple_of(part * size, size), size)
        cosine, sine = cos_ref[0, where, :], sin_ref[0, where, :]
        for j in range(inner // LANES):
            at = slice(j * LANES, (j + 1) * LANES)
            key = (rotated(acc_k[i, :, at], cosine, sine) * HD**-0.5).astype(BF16)
            weighted = (key.astype(F32) * fade_ref[where, at]).astype(BF16)
            value = acc_v[i, :, at].astype(BF16)
            state = outer(weighted, value)
            sums[:, at] = jnp.where(part == 0, state, sums[:, at] + state)

        @pl.when(part == parts - 1)
        def _():
            scaled = sums[...] * rows_ref[0:1]
            read = jnp.sum(scaled * q_spread[s], axis=0, keepdims=True)
            for o in range(n_sp):
                stage[s, o, 0:keep] = scaled[o * keep : (o + 1) * keep]
                stage[s, o, keep : keep + 1] = read
            totals[s] = stage[s, sp]

            @pl.when(end | (s == moved_seq))
            def _():
                for o in range(1, n_sp):
                    rs_copy(s, o).start()

            @pl.when(mid & (s < moved_seq))
            def _():
                y_half(s).start()

    def c_add(u, cx, at, halves):
        p = 2 * cx + u % 2
        for kv in halves:
            arrived(we.at[w_rows(p), at], w_sem(u, kv))
        for t in range(parts):
            for slot in range(len(columns)):
                block = x[p, moved[0] + t] if slot == 0 else xc[slot - 1, p, t]
                both = jnp.dot(block, we[w_rows(p), at], preferred_element_type=F32)
                if u == 0:
                    acc_c[slot, t, :, at] = both
                else:
                    acc_c[slot, t, :, at] += both

    def unit(u):
        c_add(u, (z, mate, second, third)[u // 2], slice(0, 2 * LANES), (0,))

    def c_copy(o):
        return remote(
            stage_c.at[o], landed_c.at[sp], tx.at[c_tx], c_rx.at[0], {"sp": o, "tp": mate_tp}
        )

    def key_rows(slot, t):
        return pl.ds((slot * parts + t) * size, size)

    def c_keys():
        pair_rate = hint_in[1:2, w_cols()]
        for t in range(parts):
            at = slice(t * size, (t + 1) * size)
            fade = jnp.exp(to_end[at] * pair_rate)
            for slot in range(len(columns)):
                key = (
                    rotated(acc_c[slot, t, :, :LANES], cos_ref[slot, at], sin_ref[slot, at])
                    * HD**-0.5
                ).astype(BF16)
                wq[key_rows(slot, t), 0:LANES] = (key.astype(F32) * fade).astype(BF16)

    def c_states():
        pair_rate = hint_in[1:2, w_cols()]
        query = hint_in[0:1, w_cols()]
        total = jnp.zeros((HD, LANES), F32)
        for slot, column in enumerate(columns):
            state = jnp.zeros((HD, LANES), F32)
            for t in range(parts):
                state = state + outer(wq[key_rows(slot, t), 0:LANES], acc_c[slot, t, :, LANES:].astype(BF16))
            total = total + state * jnp.exp(
                pair_rate * (span * (n_sp - 1 - column)).astype(F32)
            )
        spread = jnp.where(pick[:, :LANES], query, 0.0).astype(BF16)
        spread = jnp.dot(
            spread, jnp.where(same[:LANES, :LANES], 1.0, 0.0).astype(BF16),
            preferred_element_type=F32,
        )
        read = jnp.sum(total * spread, axis=0, keepdims=True)
        for o in range(n_sp):
            stage_c[o, 0:keep] = total[o * keep : (o + 1) * keep]
            stage_c[o, keep : keep + 1] = read
        for o in range(n_sp):
            c_copy(o).start()

    order = middle_order(main, moved)
    steps = end_int * (len(main) * (chips - 1)) + (1 - end_int) * len(order)

    def decode(n):
        kind = end_int * (n // len(main)) + (1 - end_int) * one_of(n, [o[0] for o in order])
        s = end_int * (n % len(main)) + (1 - end_int) * one_of(n, [o[1] for o in order])
        c = (
            (kind == 0).astype(jnp.int32) * mate
            + (kind == 1).astype(jnp.int32) * second
            + (kind == 2).astype(jnp.int32) * third
        )
        return kind, c, s

    last = len(order) - 1
    passes = (
        (0, ((0, 0, 0), (1, 0, 0))),
        (1, ((0, 0, 1), (1, 0, 1))),
        (5, ((0, 1, 0), (1, 1, 0))),
        (7, ((2, 0, 0), (2, 0, 1), (0, 2, 0), (1, 2, 0))),
        (8, ((0, 1, 1), (1, 1, 1))),
        (9, ((0, 2, 1), (1, 2, 1))),
        (13, ((2, 1, 0), (2, 1, 1))),
        (15, ((2, 2, 0), (2, 2, 1), (0, 3, 0), (1, 3, 0))),
        (17, ((0, 3, 1), (1, 3, 1))),
    )
    adds = ((8, 0), (9, 1), (14, 2), (15, 3), (16, 4))

    def chip(kind):
        return (z, mate, second, third)[kind]

    def shared(kind):
        arrived(xc.at[0, pl.ds(0, 3)], ry.at[3 * chips * parts + chip(kind)])

    @pl.loop(0, len(order) + 1)
    def _(n):
        kind, c, s = decode(n)
        is_moved = s >= moved[0]
        kind_b, c_b, s_b = decode(n - 1)

        @pl.when(end & (n >= 1) & (n <= steps))
        def _():
            x_arrived(2 * c_b + 1 - k, s_b)
            add(2 * c_b + 1 - k, s_b, False)

            @pl.when(kind_b == 2)
            def _():
                finish(s_b)

        @pl.when(n < steps)
        def _():
            x_arrived(2 * c + k, s)

            @pl.when(mid & (kind == 0))
            def _():
                to_other(c, s).start()

            @pl.when(mid & (kind > 0) & (s < moved[0]))
            def _():
                to_mate(c, s).start()

            @pl.when(mid & is_moved)
            def _():
                token_send(c, s - moved[0])

            to_partner(c, s).start()

        for step, events in passes:

            @pl.when(mid & (n == step))
            def _(events=events):
                for slot, kind, j in events:
                    token_pass(slot, chip(kind), j)

        @pl.when(n < steps)
        def _():
            add(2 * c + k, s, False)

        @pl.when(mid & (n >= 1))
        def _():
            x_arrived(2 * c_b + 1 - k, s_b)
            add(2 * c_b + 1 - k, s_b, False)

            @pl.when(kind_b == 2)
            def _():
                finish(s_b)

        for step, u in adds:

            @pl.when(mid & (n == step))
            def _(u=u):
                if u % 2 == 0:
                    shared(u // 2)
                unit(u)

    @pl.when(mid)
    def _():
        hint_copy.wait_recv()
        pl.semaphore_wait(ready.at[1], 1)
        unit(early)
        for j in range(parts):
            token_pass(2, third, j)
        shared(3)
        unit(units - 2)
        for s in range(moved_seq):
            arrived(landed.at[s, pl.ds(0, 2)], rs_rx.at[s])
            for side in range(2):
                stage[s, 2 * row_y + side] += landed[s, side]
            x_half(s).start()
        c_add(units - 1, third, slice(0, LANES), (0,))
        c_keys()
        c_add(units - 1, third, slice(LANES, 2 * LANES), (1,))
        c_states()

    def gather(s):
        arrived(landed.at[s, pl.ds(0, n_sp - 1)], rs_rx.at[s])
        total = None
        for j in range(n_sp):
            term = jnp.where(sp == j, totals[s], landed[s, j])
            total = term if total is None else total + term
        totals[s] = total

    sent(nx.at[pl.ds(0, chips)], n_share_tx)

    @pl.when(end)
    def _():
        pl.semaphore_wait(ready.at[1], 1)
        sent(nx.at[0], n_tx)
        sent(hint, hint_tx)
        sent(x.at[0], to_mate_tx)
        sent(x.at[pl.ds(0, chips), pl.ds(0, len(main))], share_tx)
        sent(we, w_tx)
        sent(stage.at[pl.ds(0, moved_seq), pl.ds(0, n_sp - 1)], rs_tx)

    @pl.when(mid)
    def _():
        sent(nx.at[pl.ds(0, 5)], n_tx)
        sent(x.at[pl.ds(0, chips - 1), pl.ds(0, len(main))], to_mate_tx)
        sent(x.at[pl.ds(0, 2)], to_other_tx)
        sent(x.at[pl.ds(0, chips)], share_tx)
        sent(xc.at[:, pl.ds(0, chips)], token_tx)
        sent(xc.at[:, pl.ds(0, chips)], token_share_tx)
        sent(stage.at[:, pl.ds(0, n_sp - 1)], rs_tx)

    @pl.when(mid)
    def _():
        for s in range(moved_seq):
            arrived(landed.at[s, 2], rs_rx.at[seqs + s])
            totals[s] = stage[s, sp] + landed[s, 2]
        gather(moved_seq)

    @pl.when(end)
    def _():
        for s in range(moved_seq):
            gather(s)
        arrived(landed_c, c_rx.at[0])
        for o in range(n_sp):
            start = (o // 2) * half + (o % 2) * LANES
            totals[moved_seq, :, start : start + LANES] = landed_c[o]

    for s in range(seqs):
        read = totals[s, keep : keep + 1]
        totals[s, keep : keep + 1] = read * rows_ref[1:2] + own_term[s : s + 1]

    @pl.when(mid)
    def _():
        sent(stage_c, c_tx)


def solution(mesh):
    n_sp, n_tp = mesh.shape["sp"], mesh.shape["tp"]

    def body(tokens, new_token, query_weight, key_weight, value_weight, log_decay):
        seqs, span, feat = tokens.shape
        width, inner = key_weight.shape
        heads = inner // HD
        keep = HD // n_sp
        rows = -(-(keep + 1) // 8) * 8
        chips = n_tp // 2
        half = HD // 2
        parts = max(1, 8 // chips)
        pieces = seqs * parts
        size = span // parts
        inverse = jnp.asarray(np.tile(inverse_angles(), LANES // half)[None])
        anywhere = pl.BlockSpec(memory_space=pl.ANY)
        vmem = pl.BlockSpec(memory_space=pltpu.VMEM)
        dma = pltpu.SemaphoreType.DMA
        moves = chips == 4 and n_sp == 4 and seqs > 1 and inner == 4 * LANES
        tokens_in = [
            pltpu.VMEM((n_tp, pieces, size, feat), BF16),
            pltpu.VMEM((n_tp, seqs, feat), BF16),
        ]
        weights_in = [pltpu.VMEM((width, inner), BF16)] * 3
        totals = [pltpu.VMEM((pieces, size, inner), F32)] * 2
        ends = [
            pltpu.VMEM((8, inner), F32),
            pltpu.VMEM((seqs, HD, inner), F32),
            pltpu.VMEM((NEW_ROWS, inner), F32),
            pltpu.VMEM((HD, inner), F32),
            pltpu.VMEM((seqs, n_sp, rows, inner), F32),
            pltpu.VMEM((seqs, n_sp, rows, inner), F32),
        ]
        if moves:
            call = moved_kernel
            scratch = (
                tokens_in[:1]
                + [pltpu.VMEM((3, n_tp, parts, size, feat), BF16)]
                + tokens_in[1:]
                + weights_in
                + [pltpu.VMEM((width, 2 * LANES), BF16)]
                + totals
                + [
                    pltpu.VMEM((n_sp, parts, size, 2 * LANES), F32),
                    pltpu.VMEM((n_sp, span, LANES), F32),
                    pltpu.VMEM((n_sp, span, LANES), F32),
                    pltpu.VMEM((span, inner), F32),
                ]
                + ends
                + [
                    pltpu.VMEM((8, inner), F32),
                    pltpu.VMEM((8, inner), F32),
                    pltpu.VMEM((n_sp, rows, LANES), F32),
                    pltpu.VMEM((n_sp, rows, LANES), F32),
                    dma((pieces + 1,)),
                    dma((3,)),
                    dma((n_tp, pieces)),
                    dma((chips + 1,)),
                    dma((3 * chips * parts + chips,)),
                    dma((n_tp + 1,)),
                    dma((11,)),
                    dma((1,)),
                    dma((2 * seqs,)),
                    dma((1,)),
                    pltpu.SemaphoreType.REGULAR((2,)),
                ]
            )
        else:
            call = kernel
            scratch = (
                tokens_in
                + weights_in
                + totals
                + [
                    pltpu.VMEM((span, LANES), F32),
                    pltpu.VMEM((span, LANES), F32),
                    pltpu.VMEM((span, inner), F32),
                ]
                + ends
                + [
                    pltpu.VMEM((seqs, rows, inner), F32),
                    dma((pieces + 1,)),
                    dma((3,)),
                    dma((n_tp, pieces)),
                    dma((n_tp,)),
                    dma((2, chips, pieces)),
                    dma((chips, pieces)),
                    dma((2, chips)),
                    dma((chips,)),
                    dma((seqs, n_sp)),
                    dma((seqs, n_sp)),
                ]
            )
        out_shape = (
            jax.ShapeDtypeStruct((seqs, heads, keep, HD), BF16),
            jax.ShapeDtypeStruct((seqs, inner), BF16),
        )
        shared = dict(
            scratch_shapes=scratch,
            name="retention",
        )
        args = (
            tokens, new_token.reshape(seqs, feat), query_weight, key_weight, value_weight
        )
        args = tuple(pltpu.with_memory_space_constraint(a, pltpu.HBM) for a in args)
        smem = pl.BlockSpec(memory_space=pltpu.SMEM)
        limit = (215 if moves else 240) * 256 * 1024
        params = pltpu.CompilerParams(
            collective_id=0, has_side_effects=True, vmem_limit_bytes=limit
        )
        call = functools.partial(call, n_sp, n_tp, parts)
        if not moves:
            return pl.pallas_call(
                call,
                out_shape=out_shape,
                in_specs=[anywhere] * 5 + [vmem, smem],
                out_specs=(vmem, vmem),
                compiler_params=params,
                **shared,
            )(*args, inverse, log_decay)
        sums = pl.pallas_call(
            call,
            out_shape=jax.ShapeDtypeStruct((seqs, rows, inner), F32),
            in_specs=[anywhere] * 5 + [smem],
            out_specs=vmem,
            compiler_params=params,
            **shared,
        )(*args, pltpu.with_memory_space_constraint(log_decay, pltpu.HBM))
        return pl.pallas_call(
            outputs,
            out_shape=out_shape,
            in_specs=[vmem],
            out_specs=(anywhere, anywhere),
            scratch_shapes=[pltpu.VMEM(out.shape, BF16) for out in out_shape] + [dma((2,))],
            compiler_params=pltpu.CompilerParams(vmem_limit_bytes=4 * 1024 * 1024),
            name="outputs",
        )(sums)

    return jax.shard_map(
        body,
        mesh=mesh,
        in_specs=(
            P(None, "sp", "tp"),
            P(None, None, "tp"),
            P(None, "tp"),
            P(None, "tp"),
            P(None, "tp"),
            P("tp"),
        ),
        out_specs=(P(None, "tp", "sp", None), P(None, "tp")),
        check_vma=False,
    )
```

```python
import functools

import jax
import jax.numpy as jnp
import numpy as np
from jax import lax
from jax.experimental import pallas as pl
from jax.experimental.pallas import tpu as pltpu
from jax.sharding import PartitionSpec as P

HD = 64
LANES = 128
NEW_ROWS = 8
F32 = jnp.float32
BF16 = jnp.bfloat16


def inverse_angles():
    half = HD // 2
    return np.float32(10000.0) ** (-np.arange(half, dtype=np.float32) / half)


def lane_iota(shape):
    return lax.broadcasted_iota(jnp.int32, shape, len(shape) - 1)


def rotated(block, cosine, sine):
    half = HD // 2
    low = lane_iota(block.shape) % HD < half
    swapped = jnp.where(
        low, pltpu.roll(block, LANES - half, 1), pltpu.roll(block, half, 1)
    )
    return block * cosine + swapped * sine


def kernel(
    n_sp, n_tp, parts,
    tokens, fresh, wq_hbm, wk_hbm, wv_hbm, inverse_ref, decay_ref,
    state_out, read_out,
    x, nx, wq, wk, wv, acc_k, acc_v, cos_ref, sin_ref, fade_ref, rows_ref,
    q_spread, own_term, sums, stage, landed, totals,
    load_sem, weight_sem, rx, rn, fwd, share, nfwd, nshare, rs_tx, rs_rx,
):
    seqs, span, feat = tokens.shape
    inner = wk.shape[1]
    heads = inner // HD
    chips = n_tp // 2
    pieces = seqs * parts
    size = span // parts
    keep = HD // n_sp
    sp = lax.axis_index("sp")
    tp = lax.axis_index("tp")
    z, k = tp // 2, tp % 2
    MESH = pl.DeviceIdType.MESH

    def to_tp(index):
        return {"tp": index}

    partner = z * 2 + 1 - k
    own_loads = [
        pltpu.make_async_copy(
            tokens.at[s // parts, pl.ds(s % parts * size, size)], x.at[tp, s], load_sem.at[s]
        )
        for s in range(pieces)
    ]
    new_load = pltpu.make_async_copy(fresh, nx.at[tp], load_sem.at[pieces])
    new_load.start()
    for copy in own_loads:
        copy.start()
    weight_loads = [
        pltpu.make_async_copy(a, b, weight_sem.at[i])
        for i, (a, b) in enumerate(((wk_hbm, wk), (wv_hbm, wv), (wq_hbm, wq)))
    ]

    barrier = pltpu.get_barrier_semaphore()

    @pl.when(z > 0)
    def _():
        pl.semaphore_signal(barrier, inc=1, device_id=to_tp(tp - 2), device_id_type=MESH)

    @pl.when(z < chips - 1)
    def _():
        pl.semaphore_signal(barrier, inc=1, device_id=to_tp(tp + 2), device_id_type=MESH)

    pl.semaphore_signal(barrier, inc=1, device_id=to_tp(partner), device_id_type=MESH)
    for o in range(1, n_sp):
        pl.semaphore_signal(
            barrier, inc=1, device_id={"sp": lax.rem(sp + o, n_sp)}, device_id_type=MESH
        )
    pl.semaphore_wait(
        barrier, n_sp + (z > 0).astype(jnp.int32) + (z < chips - 1).astype(jnp.int32)
    )

    def x_copy(c, s, sem, target):
        p = 2 * c + k
        return pltpu.make_async_remote_copy(
            x.at[p, s], x.at[p, s], sem, rx.at[p, s], device_id=to_tp(target), device_id_type=MESH
        )

    def n_copy(c, sem, target):
        p = 2 * c + k
        return pltpu.make_async_remote_copy(
            nx.at[p], nx.at[p], sem, rn.at[p], device_id=to_tp(target), device_id_type=MESH
        )

    def x_arrived(p, s):
        pltpu.make_async_remote_copy(
            x.at[p, s], x.at[p, s], share.at[0, 0], rx.at[p, s],
            device_id=to_tp(partner), device_id_type=MESH,
        ).wait_recv()

    def n_arrived(p):
        pltpu.make_async_remote_copy(
            nx.at[p], nx.at[p], nshare.at[0], rn.at[p],
            device_id=to_tp(partner), device_id_type=MESH,
        ).wait_recv()

    new_load.wait()
    n_up = n_copy(z, nfwd.at[0, z], tp + 2)
    n_down = n_copy(z, nfwd.at[1, z], tp - 2)
    n_side = n_copy(z, nshare.at[z], partner)

    @pl.when(z < chips - 1)
    def _():
        n_up.start()

    @pl.when(z > 0)
    def _():
        n_down.start()

    n_side.start()
    for s in range(pieces):
        own_loads[s].wait()

        @pl.when(z < chips - 1)
        def _(s=s):
            x_copy(z, s, fwd.at[0, z, s], tp + 2).start()

        @pl.when(z > 0)
        def _(s=s):
            x_copy(z, s, fwd.at[1, z, s], tp - 2).start()

        x_copy(z, s, share.at[z, s], partner).start()

    for copy in weight_loads:
        copy.start()

    row = lax.broadcasted_iota(jnp.int32, (span, LANES), 0)
    within = lane_iota((1, LANES)) % HD
    first_half = jnp.where(within < HD // 2, -1.0, 1.0).astype(F32)
    inverse = inverse_ref[...]
    angles = (sp * span + row).astype(F32) * inverse
    cos_ref[...] = jnp.cos(angles)
    sin_ref[...] = jnp.sin(angles) * first_half
    new_angles = jnp.full((NEW_ROWS, LANES), n_sp * span, F32) * inverse
    new_cos = jnp.cos(new_angles)
    new_sin = jnp.sin(new_angles) * first_half
    head_of = lane_iota((1, inner)) // HD
    rate = jnp.zeros((1, inner), F32)
    for h in range(heads):
        rate = jnp.where(head_of == h, decay_ref[h], rate)
    to_end = (span - 1 - lax.broadcasted_iota(jnp.int32, (span, 1), 0)).astype(F32)
    fade_ref[...] = jnp.exp(to_end * rate)
    rows_ref[0:1] = jnp.exp(rate * (span * (n_sp - 1 - sp)).astype(F32))
    rows_ref[1:2] = jnp.exp(rate)

    for copy in weight_loads:
        copy.wait()

    def add(p, s, fresh_total):
        block = x[p, s]
        where = pl.ds(pl.multiple_of(p * feat, feat), feat)
        part_k = jnp.dot(block, wk[where, :], preferred_element_type=F32)
        part_v = jnp.dot(block, wv[where, :], preferred_element_type=F32)
        if fresh_total:
            acc_k[s] = part_k
            acc_v[s] = part_v
        else:
            acc_k[s] += part_k
            acc_v[s] += part_v

    @pl.loop(0, pieces)
    def _(s):
        add(tp, s, True)
        x_arrived(partner, s)
        add(partner, s, False)

    n_arrived(partner)

    def project_new():
        def piece(p, totals):
            where = pl.ds(pl.multiple_of(p * feat, feat), feat)
            block = jnp.concatenate(
                [nx[p].astype(F32), jnp.zeros((NEW_ROWS - seqs, feat), F32)], axis=0
            ).astype(BF16)
            return tuple(
                t + jnp.dot(block, w[where, :], preferred_element_type=F32)
                for t, w in zip(totals, (wk, wv, wq))
            )

        zero = jnp.zeros((NEW_ROWS, inner), F32)
        new_k, new_v, new_q = lax.fori_loop(0, n_tp, piece, (zero, zero, zero))
        keys, queries = [], []
        for j in range(inner // LANES):
            at = slice(j * LANES, (j + 1) * LANES)
            keys.append((rotated(new_k[:, at], new_cos, new_sin) * HD**-0.5).astype(BF16))
            queries.append(rotated(new_q[:, at], new_cos, new_sin).astype(BF16))
        key = jnp.concatenate(keys, axis=1).astype(F32)
        query = jnp.concatenate(queries, axis=1).astype(F32)
        value = new_v.astype(BF16).astype(F32)
        same = (
            lax.broadcasted_iota(jnp.int32, (inner, inner), 0) // HD
            == lax.broadcasted_iota(jnp.int32, (inner, inner), 1) // HD
        )
        product = query * key
        for h in range(heads):
            at = slice(h * HD, (h + 1) * HD)
            own_term[:, at] = jnp.sum(product[:, at], axis=-1, keepdims=True) * value[:, at]
        pick = lax.broadcasted_iota(jnp.int32, (HD, inner), 0) == lane_iota((HD, inner)) % HD
        for s in range(seqs):
            spread = jnp.where(pick, query[s : s + 1], 0.0).astype(BF16)
            q_spread[s] = jnp.dot(
                spread, jnp.where(same, 1.0, 0.0).astype(BF16), preferred_element_type=F32
            )

    def rs_copy(s, o):
        peer = lax.rem(sp + o, n_sp)
        return pltpu.make_async_remote_copy(
            stage.at[s, peer], landed.at[s, sp], rs_tx.at[s, peer], rs_rx.at[s, sp],
            device_id={"sp": peer}, device_id_type=MESH,
        )

    def finish(i):
        s, part = i // parts, i % parts
        where = pl.ds(pl.multiple_of(part * size, size), size)
        cosine, sine = cos_ref[where, :], sin_ref[where, :]
        lane = lane_iota((HD, LANES))
        for j in range(inner // LANES):
            at = slice(j * LANES, (j + 1) * LANES)
            key = (rotated(acc_k[i, :, at], cosine, sine) * HD**-0.5).astype(BF16)
            weighted = (key.astype(F32) * fade_ref[where, at]).astype(BF16)
            value = acc_v[i, :, at].astype(BF16)
            both = lax.dot_general(
                weighted, value, (((0,), (0,)), ((), ())), preferred_element_type=F32
            )
            state = jnp.where(lane < HD, both[:HD], both[HD:])
            sums[:, at] = jnp.where(part == 0, state, sums[:, at] + state)

        @pl.when(part == parts - 1)
        def _():
            scaled = sums[...] * rows_ref[0:1]
            read = jnp.sum(scaled * q_spread[s], axis=0, keepdims=True)
            for o in range(n_sp):
                stage[s, o, 0:keep] = scaled[o * keep : (o + 1) * keep]
                stage[s, o, keep : keep + 1] = read
            for o in range(1, n_sp):
                rs_copy(s, o).start()
            totals[s] = stage[s, sp]

    far = jnp.maximum(z, chips - 1 - z)

    def decode(i):
        d = i // (2 * pieces) + 1
        s = (i // 2) % pieces
        step = 2 * (i % 2) - 1
        c = z + step * d
        return d, s, step, c, (c >= 0) & (c < chips)

    def onward(step):
        nxt = z - step
        return nxt, (nxt >= 0) & (nxt < chips), (step + 1) // 2

    @pl.loop(0, 2 * pieces * (chips - 1))
    def _(i):
        d, s, step, c, valid = decode(i)
        nxt, pass_on, way = onward(step)

        @pl.when(valid)
        def _():
            @pl.when(s == 0)
            def _():
                n_arrived(2 * c + k)

                @pl.when(pass_on)
                def _():
                    n_copy(c, nfwd.at[way, c], 2 * nxt + k).start()

                n_copy(c, nshare.at[c], partner).start()

            x_arrived(2 * c + k, s)

            @pl.when(pass_on)
            def _():
                x_copy(c, s, fwd.at[way, c, s], 2 * nxt + k).start()

            x_copy(c, s, share.at[c, s], partner).start()
            add(2 * c + k, s, False)

            @pl.when(s == 0)
            def _():
                n_arrived(2 * c + 1 - k)

            x_arrived(2 * c + 1 - k, s)
            add(2 * c + 1 - k, s, False)

        last = (d == far) & (step == 1)

        @pl.when(last & (s == 0))
        def _():
            project_new()

        @pl.when(last)
        def _():
            finish(s)

    raws = []
    for s in range(seqs):
        for o in range(1, n_sp):
            src = lax.rem(sp + o, n_sp)
            pltpu.make_async_remote_copy(
                stage.at[s, src], landed.at[s, src], rs_tx.at[s, src], rs_rx.at[s, src],
                device_id={"sp": src}, device_id_type=MESH,
            ).wait_recv()
        total = None
        for j in range(n_sp):
            term = jnp.where(sp == j, totals[s], landed[s, j])
            total = term if total is None else total + term
        kept = total[0:keep].astype(BF16)
        for h in range(heads):
            state_out[s, h] = kept[:, h * HD : (h + 1) * HD]
        raws.append(total[keep : keep + 1] * rows_ref[1:2] + own_term[s : s + 1])
    raw = jnp.concatenate(raws, axis=0)
    for h in range(heads):
        at = slice(h * HD, (h + 1) * HD)
        head = raw[:, at]
        centered = head - jnp.mean(head, axis=-1, keepdims=True)
        spread = jnp.mean(centered * centered, axis=-1, keepdims=True)
        read_out[:, at] = (centered * lax.rsqrt(spread + 1e-05)).astype(BF16)

    @pl.when(z < chips - 1)
    def _():
        n_up.wait_send()

    @pl.when(z > 0)
    def _():
        n_down.wait_send()

    n_side.wait_send()
    for s in range(seqs):
        for o in range(1, n_sp):
            rs_copy(s, o).wait_send()
    for s in range(pieces):
        @pl.when(z < chips - 1)
        def _(s=s):
            x_copy(z, s, fwd.at[0, z, s], tp + 2).wait_send()

        @pl.when(z > 0)
        def _(s=s):
            x_copy(z, s, fwd.at[1, z, s], tp - 2).wait_send()

        x_copy(z, s, share.at[z, s], partner).wait_send()

    @pl.loop(0, 2 * pieces * (chips - 1))
    def _(i):
        d, s, step, c, valid = decode(i)
        nxt, pass_on, way = onward(step)

        @pl.when(valid)
        def _():
            @pl.when(s == 0)
            def _():
                @pl.when(pass_on)
                def _():
                    n_copy(c, nfwd.at[way, c], 2 * nxt + k).wait_send()

                n_copy(c, nshare.at[c], partner).wait_send()

            @pl.when(pass_on)
            def _():
                x_copy(c, s, fwd.at[way, c, s], 2 * nxt + k).wait_send()

            x_copy(c, s, share.at[c, s], partner).wait_send()


def one_of(n, values):
    total = 0
    for k, value in enumerate(values):
        if value:
            total = total + (n == k).astype(jnp.int32) * value
    return total


def middle_order(main, moved):
    near = [(0, i) for i in main]
    far = [(2, i) for i in moved + main]
    order = [(kind, i) for i in moved for kind in (0, 1)]
    order += [(1, i) for i in main]
    for at in range(max(len(near), len(far))):
        order += far[at : at + 1] + near[at : at + 1]
    return order


def outputs(totals, state_out, read_out, state, read, sem):
    seqs, heads, keep, _ = state_out.shape
    raws = []
    for s in range(seqs):
        kept = totals[s, 0:keep].astype(BF16)
        for h in range(heads):
            state[s, h] = kept[:, h * HD : (h + 1) * HD]
        raws.append(totals[s, keep : keep + 1])
    state_copy = pltpu.make_async_copy(state, state_out, sem.at[0])
    state_copy.start()
    raw = jnp.concatenate(raws, axis=0)
    for h in range(heads):
        at = slice(h * HD, (h + 1) * HD)
        head = raw[:, at]
        centered = head - jnp.mean(head, axis=-1, keepdims=True)
        spread = jnp.mean(centered * centered, axis=-1, keepdims=True)
        read[:, at] = (centered * lax.rsqrt(spread + 1e-05)).astype(BF16)
    read_copy = pltpu.make_async_copy(read, read_out, sem.at[1])
    read_copy.start()
    state_copy.wait()
    read_copy.wait()


def moved_kernel(
    n_sp, n_tp, parts,
    tokens, fresh, wq_hbm, wk_hbm, wv_hbm, decay_ref,
    totals,
    x, xc, nx, wq, wk, wv, we, acc_k, acc_v, acc_c, cos_ref, sin_ref, fade_ref, rows_ref,
    q_spread, own_term, sums, stage, landed, hint, hint_in, stage_c, landed_c,
    load_sem, weight_sem, rx, rn, ry, rw, tx, hint_rx, rs_rx, c_rx, ready,
):
    seqs, span, feat = tokens.shape
    inner = wk.shape[1]
    heads = inner // HD
    half = inner // 2
    chips = n_tp // 2
    pieces = seqs * parts
    size = span // parts
    keep = HD // n_sp
    units = n_tp
    early = n_tp - 3
    moved_seq = seqs - 1
    to_mate_tx, to_other_tx, share_tx, n_tx, n_share_tx, token_tx, token_share_tx, w_tx = range(8)
    hint_tx, rs_tx, c_tx = range(8, 11)
    main = list(range(moved_seq * parts))
    moved = list(range(moved_seq * parts, pieces))
    sp = lax.axis_index("sp")
    tp = lax.axis_index("tp")
    z, k = tp // 2, tp % 2
    row_y, row_x = sp // 2, sp % 2
    x_peer = sp + 1 - 2 * row_x
    y_peer = sp + 2 - 4 * row_y
    columns = (sp, x_peer, y_peer, x_peer + y_peer - sp)
    MESH = pl.DeviceIdType.MESH
    end_int = (z == 0).astype(jnp.int32) + (z == chips - 1).astype(jnp.int32)
    end = end_int > 0
    mid = end_int == 0
    partner = z * 2 + 1 - k
    mate = z + 1 - 2 * (z % 2)
    mate_tp = 2 * mate + k
    other = chips - 1 - z
    other_tp = 2 * other + k
    second = end_int * (chips - 1 - mate) + (1 - end_int) * (chips - 1 - z)
    third = end_int * (chips - 1 - z) + (1 - end_int) * (chips - 1 - mate)

    own_loads = {
        s: pltpu.make_async_copy(
            tokens.at[s // parts, pl.ds(s % parts * size, size)], x.at[tp, s], load_sem.at[s]
        )
        for s in range(pieces)
    }
    new_load = pltpu.make_async_copy(fresh, nx.at[tp], load_sem.at[pieces])
    new_load.start()
    for s in moved + main:
        own_loads[s].start()
    weight_loads = [
        pltpu.make_async_copy(a, b, weight_sem.at[i])
        for i, (a, b) in enumerate(((wk_hbm, wk), (wv_hbm, wv), (wq_hbm, wq)))
    ]

    barrier = pltpu.get_barrier_semaphore()
    for target in ({"tp": partner}, {"tp": mate_tp}, {"sp": x_peer}, {"sp": y_peer}):
        pl.semaphore_signal(barrier, inc=1, device_id=target, device_id_type=MESH)

    @pl.when(mid)
    def _():
        pl.semaphore_signal(barrier, inc=1, device_id={"tp": other_tp}, device_id_type=MESH)

    pl.semaphore_wait(barrier, 5 - end_int)
    for target in ({"sp": x_peer}, {"sp": y_peer}):
        pl.semaphore_signal(ready.at[0], inc=1, device_id=target, device_id_type=MESH)

    def remote(source, dest, send, recv, target):
        return pltpu.make_async_remote_copy(
            source, dest, send, recv, device_id=target, device_id_type=MESH
        )

    def sent(ref, kind):
        remote(ref, ref, tx.at[kind], hint_rx.at[0], {"tp": partner}).wait_send()

    def arrived(ref, sem):
        remote(ref, ref, tx.at[0], sem, {"tp": partner}).wait_recv()

    def x_copy(c, s, kind, target):
        here = x.at[2 * c + k, s]
        return remote(here, here, tx.at[kind], rx.at[2 * c + k, s], {"tp": target})

    def to_mate(c, s):
        return x_copy(c, s, to_mate_tx, mate_tp)

    def to_other(c, s):
        return x_copy(c, s, to_other_tx, other_tp)

    def to_partner(c, s):
        return x_copy(c, s, share_tx, partner)

    def x_arrived(p, s):
        arrived(x.at[p, s], rx.at[p, s])

    def token_send(c, j):
        here = x.at[2 * c + k, moved[0] + j]
        for slot, target in ((0, x_peer), (1, y_peer)):
            remote(
                here, xc.at[slot, 2 * c + k, j], tx.at[token_tx],
                ry.at[(slot * chips + c) * parts + j], {"sp": target},
            ).start()

    def token_pass(slot, c, j):
        p = 2 * c + k
        here = xc.at[slot, p, j]
        arrived(here, ry.at[(slot * chips + c) * parts + j])
        if slot < 2 and slot == j % 2:
            remote(
                here, xc.at[2, p, j], tx.at[token_tx],
                ry.at[(2 * chips + c) * parts + j], {"sp": y_peer if slot == 0 else x_peer},
            ).start()
        remote(
            here, here, tx.at[token_share_tx], ry.at[3 * chips * parts + c], {"tp": partner}
        ).start()

    def w_rows(p):
        return pl.ds(pl.multiple_of(p * feat, feat), feat)

    def w_cols():
        return pl.ds(pl.multiple_of(row_y * half + row_x * LANES, LANES), LANES)

    def w_sem(u, kv):
        return rw.at[u + (kv if u == units - 1 else 0)]

    def w_send(u, kv):
        rows = w_rows(2 * (mate, z, second, third)[u // 2] + u % 2)
        return remote(
            (wk, wv)[kv].at[rows, w_cols()], we.at[rows, pl.ds(kv * LANES, LANES)],
            tx.at[w_tx], w_sem(u, kv), {"tp": mate_tp},
        )

    def n_copy(c, kind, sem, target):
        here = nx.at[2 * c + k]
        return remote(here, here, tx.at[kind], sem, {"tp": target})

    def n_to(c, target):
        n_copy(c, n_tx, rn.at[c], target).start()

    def n_share(c):
        n_copy(c, n_share_tx, rn.at[chips], partner).start()

    def n_arrived(c):
        arrived(nx.at[2 * c + k], rn.at[c])

    hint_copy = remote(hint, hint_in, tx.at[hint_tx], hint_rx.at[0], {"tp": mate_tp})

    new_load.wait()
    n_to(z, mate_tp)
    n_share(z)

    @pl.when(mid)
    def _():
        n_to(z, other_tp)

    for s in moved + main:
        own_loads[s].wait()

    def send_moved(j):
        s = moved[j]

        @pl.when(mid)
        def _():
            to_other(z, s).start()
            token_send(z, j)
            to_partner(z, s).start()

        @pl.when(end)
        def _():
            to_mate(z, s).start()

    send_moved(0)
    to_partner(z, main[0]).start()

    @pl.when(mid)
    def _():
        to_mate(z, main[0]).start()

    for copy in weight_loads:
        copy.start()

    @pl.when(mid)
    def _():
        n_arrived(mate)
        n_to(mate, other_tp)
        n_share(mate)
        n_arrived(other)
        n_to(other, mate_tp)
        n_share(other)

    for j in range(1, parts):
        send_moved(j)
    for s in main[1:]:
        to_partner(z, s).start()

    @pl.when(mid)
    def _():
        for s in main[1:2]:
            to_mate(z, s).start()
        for s in main:
            to_other(z, s).start()

    row = lax.broadcasted_iota(jnp.int32, (span, LANES), 0)
    within = lane_iota((1, LANES)) % HD
    first_half = jnp.where(within < HD // 2, -1.0, 1.0).astype(F32)
    inverse = jnp.zeros((1, LANES), F32)
    for j, step in enumerate(inverse_angles()):
        inverse = jnp.where(within % (HD // 2) == j, float(step), inverse)

    def tables(slot, column):
        angles = (column * span + row).astype(F32) * inverse
        cos_ref[slot] = jnp.cos(angles)
        sin_ref[slot] = jnp.sin(angles) * first_half

    for copy in weight_loads[:2]:
        copy.wait()

    @pl.when(end)
    def _():
        for u in range(early):
            for kv in range(2):
                w_send(u, kv).start()

    tables(0, sp)

    @pl.when(mid)
    def _():
        for slot in range(1, len(columns)):
            tables(slot, columns[slot])

    new_angles = jnp.full((NEW_ROWS, LANES), n_sp * span, F32) * inverse
    new_cos = jnp.cos(new_angles)
    new_sin = jnp.sin(new_angles) * first_half
    head_of = lane_iota((1, inner)) // HD
    rate = jnp.zeros((1, inner), F32)
    for h in range(heads):
        rate = jnp.where(head_of == h, decay_ref[h], rate)
    to_end = (span - 1 - lax.broadcasted_iota(jnp.int32, (span, 1), 0)).astype(F32)
    fade_ref[...] = jnp.exp(to_end * rate)
    rows_ref[0:1] = jnp.exp(rate * (span * (n_sp - 1 - sp)).astype(F32))
    rows_ref[1:2] = jnp.exp(rate)
    hint[...] = jnp.zeros(hint.shape, F32)
    hint[1:2] = rate
    weight_loads[2].wait()

    def add(p, s, fresh_total):
        block = x[p, s]
        where = w_rows(p)
        part_k = jnp.dot(block, wk[where, :], preferred_element_type=F32)
        part_v = jnp.dot(block, wv[where, :], preferred_element_type=F32)
        if fresh_total:
            acc_k[s] = part_k
            acc_v[s] = part_v
        else:
            acc_k[s] += part_k
            acc_v[s] += part_v

    same = (
        lax.broadcasted_iota(jnp.int32, (inner, inner), 0) // HD
        == lax.broadcasted_iota(jnp.int32, (inner, inner), 1) // HD
    )
    pick = lax.broadcasted_iota(jnp.int32, (HD, inner), 0) == lane_iota((HD, inner)) % HD

    @pl.when(mid)
    def _():
        n_arrived(third)
        n_to(third, mate_tp)
        n_share(third)
        for s in main[2:]:
            to_mate(z, s).start()

    own_pieces = end_int * len(main) + (1 - end_int) * pieces

    @pl.loop(0, pieces)
    def _(i):
        s = lax.rem(i + (1 - end_int) * len(main), pieces)

        @pl.when(i < own_pieces)
        def _():
            add(tp, s, True)

        @pl.when(i < own_pieces)
        def _():
            x_arrived(partner, s)
            add(partner, s, False)

    @pl.when(end)
    def _():
        for c in (mate, second, third):
            n_arrived(c)
            n_share(c)

    arrived(nx.at[pl.ds(0, chips)], rn.at[chips])

    def project_new():
        def piece(p, totals):
            where = w_rows(p)
            block = jnp.concatenate(
                [nx[p].astype(F32), jnp.zeros((NEW_ROWS - seqs, feat), F32)], axis=0
            ).astype(BF16)
            return tuple(
                t + jnp.dot(block, w[where, :], preferred_element_type=F32)
                for t, w in zip(totals, (wk, wv, wq))
            )

        zero = jnp.zeros((NEW_ROWS, inner), F32)
        new_k, new_v, new_q = lax.fori_loop(0, n_tp, piece, (zero, zero, zero))
        keys, queries = [], []
        for j in range(inner // LANES):
            at = slice(j * LANES, (j + 1) * LANES)
            keys.append((rotated(new_k[:, at], new_cos, new_sin) * HD**-0.5).astype(BF16))
            queries.append(rotated(new_q[:, at], new_cos, new_sin).astype(BF16))
        key = jnp.concatenate(keys, axis=1).astype(F32)
        query = jnp.concatenate(queries, axis=1).astype(F32)
        value = new_v.astype(BF16).astype(F32)
        product = query * key
        for h in range(heads):
            at = slice(h * HD, (h + 1) * HD)
            own_term[:, at] = jnp.sum(product[:, at], axis=-1, keepdims=True) * value[:, at]
        hint[0:1] = query[moved_seq : moved_seq + 1]
        for s in range(seqs):
            spread = jnp.where(pick, query[s : s + 1], 0.0).astype(BF16)
            q_spread[s] = jnp.dot(
                spread, jnp.where(same, 1.0, 0.0).astype(BF16), preferred_element_type=F32
            )

    project_new()

    @pl.when(end)
    def _():
        hint_copy.start()
        for s in main:
            to_mate(z, s).start()
        final = units - 1
        for u in range(early, final - 1):
            for kv in range(2):
                w_send(u, kv).start()
        for u, kv in ((final, 0), (final - 1, 0), (final - 1, 1), (final, 1)):
            w_send(u, kv).start()

    def rs_copy(s, o):
        peer = lax.rem(sp + o, n_sp)
        return remote(
            stage.at[s, peer], landed.at[s, sp], tx.at[rs_tx], rs_rx.at[s], {"sp": peer}
        )

    pl.semaphore_wait(ready.at[0], 2)
    pl.semaphore_signal(ready.at[1], inc=1, device_id={"sp": x_peer}, device_id_type=MESH)

    def y_half(s):
        return remote(
            stage.at[s, pl.ds(2 - 2 * row_y, 2)], landed.at[s, pl.ds(0, 2)],
            tx.at[rs_tx], rs_rx.at[s], {"sp": y_peer},
        )

    def x_half(s):
        return remote(
            stage.at[s, x_peer], landed.at[s, 2], tx.at[rs_tx], rs_rx.at[seqs + s], {"sp": x_peer}
        )

    def outer(weighted, value):
        both = lax.dot_general(
            weighted, value, (((0,), (0,)), ((), ())), preferred_element_type=F32
        )
        return jnp.where(lane_iota((HD, LANES)) < HD, both[:HD], both[HD:])

    def finish(i):
        s, part = i // parts, i % parts
        where = pl.ds(pl.multiple_of(part * size, size), size)
        cosine, sine = cos_ref[0, where, :], sin_ref[0, where, :]
        for j in range(inner // LANES):
            at = slice(j * LANES, (j + 1) * LANES)
            key = (rotated(acc_k[i, :, at], cosine, sine) * HD**-0.5).astype(BF16)
            weighted = (key.astype(F32) * fade_ref[where, at]).astype(BF16)
            value = acc_v[i, :, at].astype(BF16)
            state = outer(weighted, value)
            sums[:, at] = jnp.where(part == 0, state, sums[:, at] + state)

        @pl.when(part == parts - 1)
        def _():
            scaled = sums[...] * rows_ref[0:1]
            read = jnp.sum(scaled * q_spread[s], axis=0, keepdims=True)
            for o in range(n_sp):
                stage[s, o, 0:keep] = scaled[o * keep : (o + 1) * keep]
                stage[s, o, keep : keep + 1] = read
            totals[s] = stage[s, sp]

            @pl.when(end | (s == moved_seq))
            def _():
                for o in range(1, n_sp):
                    rs_copy(s, o).start()

            @pl.when(mid & (s < moved_seq))
            def _():
                y_half(s).start()

    def c_add(u, cx, at, halves):
        p = 2 * cx + u % 2
        for kv in halves:
            arrived(we.at[w_rows(p), at], w_sem(u, kv))
        for t in range(parts):
            for slot in range(len(columns)):
                block = x[p, moved[0] + t] if slot == 0 else xc[slot - 1, p, t]
                both = jnp.dot(block, we[w_rows(p), at], preferred_element_type=F32)
                if u == 0:
                    acc_c[slot, t, :, at] = both
                else:
                    acc_c[slot, t, :, at] += both

    def unit(u):
        c_add(u, (z, mate, second, third)[u // 2], slice(0, 2 * LANES), (0,))

    def c_copy(o):
        return remote(
            stage_c.at[o], landed_c.at[sp], tx.at[c_tx], c_rx.at[0], {"sp": o, "tp": mate_tp}
        )

    def key_rows(slot, t):
        return pl.ds((slot * parts + t) * size, size)

    def c_keys():
        pair_rate = hint_in[1:2, w_cols()]
        for t in range(parts):
            at = slice(t * size, (t + 1) * size)
            fade = jnp.exp(to_end[at] * pair_rate)
            for slot in range(len(columns)):
                key = (
                    rotated(acc_c[slot, t, :, :LANES], cos_ref[slot, at], sin_ref[slot, at])
                    * HD**-0.5
                ).astype(BF16)
                wq[key_rows(slot, t), 0:LANES] = (key.astype(F32) * fade).astype(BF16)

    def c_states():
        pair_rate = hint_in[1:2, w_cols()]
        query = hint_in[0:1, w_cols()]
        total = jnp.zeros((HD, LANES), F32)
        for slot, column in enumerate(columns):
            state = jnp.zeros((HD, LANES), F32)
            for t in range(parts):
                state = state + outer(wq[key_rows(slot, t), 0:LANES], acc_c[slot, t, :, LANES:].astype(BF16))
            total = total + state * jnp.exp(
                pair_rate * (span * (n_sp - 1 - column)).astype(F32)
            )
        spread = jnp.where(pick[:, :LANES], query, 0.0).astype(BF16)
        spread = jnp.dot(
            spread, jnp.where(same[:LANES, :LANES], 1.0, 0.0).astype(BF16),
            preferred_element_type=F32,
        )
        read = jnp.sum(total * spread, axis=0, keepdims=True)
        for o in range(n_sp):
            stage_c[o, 0:keep] = total[o * keep : (o + 1) * keep]
            stage_c[o, keep : keep + 1] = read
        for o in range(n_sp):
            c_copy(o).start()

    order = middle_order(main, moved)
    steps = end_int * (len(main) * (chips - 1)) + (1 - end_int) * len(order)

    def decode(n):
        kind = end_int * (n // len(main)) + (1 - end_int) * one_of(n, [o[0] for o in order])
        s = end_int * (n % len(main)) + (1 - end_int) * one_of(n, [o[1] for o in order])
        c = (
            (kind == 0).astype(jnp.int32) * mate
            + (kind == 1).astype(jnp.int32) * second
            + (kind == 2).astype(jnp.int32) * third
        )
        return kind, c, s

    last = len(order) - 1
    passes = (
        (0, ((0, 0, 0), (1, 0, 0))),
        (1, ((0, 0, 1), (1, 0, 1))),
        (5, ((0, 1, 0), (1, 1, 0))),
        (7, ((2, 0, 0), (2, 0, 1), (0, 2, 0), (1, 2, 0))),
        (8, ((0, 1, 1), (1, 1, 1))),
        (9, ((0, 2, 1), (1, 2, 1))),
        (13, ((2, 1, 0), (2, 1, 1))),
        (15, ((2, 2, 0), (2, 2, 1), (0, 3, 0), (1, 3, 0))),
        (17, ((0, 3, 1), (1, 3, 1))),
    )
    adds = ((8, 0), (9, 1), (14, 2), (15, 3), (16, 4))

    def chip(kind):
        return (z, mate, second, third)[kind]

    def shared(kind):
        arrived(xc.at[0, pl.ds(0, 3)], ry.at[3 * chips * parts + chip(kind)])

    @pl.loop(0, len(order) + 1)
    def _(n):
        kind, c, s = decode(n)
        is_moved = s >= moved[0]
        kind_b, c_b, s_b = decode(n - 1)

        @pl.when(end & (n >= 1) & (n <= steps))
        def _():
            x_arrived(2 * c_b + 1 - k, s_b)
            add(2 * c_b + 1 - k, s_b, False)

            @pl.when(kind_b == 2)
            def _():
                finish(s_b)

        @pl.when(n < steps)
        def _():
            x_arrived(2 * c + k, s)

            @pl.when(mid & (kind == 0))
            def _():
                to_other(c, s).start()

            @pl.when(mid & (kind > 0) & (s < moved[0]))
            def _():
                to_mate(c, s).start()

            @pl.when(mid & is_moved)
            def _():
                token_send(c, s - moved[0])

            to_partner(c, s).start()

        for step, events in passes:

            @pl.when(mid & (n == step))
            def _(events=events):
                for slot, kind, j in events:
                    token_pass(slot, chip(kind), j)

        @pl.when(n < steps)
        def _():
            add(2 * c + k, s, False)

        @pl.when(mid & (n >= 1))
        def _():
            x_arrived(2 * c_b + 1 - k, s_b)
            add(2 * c_b + 1 - k, s_b, False)

            @pl.when(kind_b == 2)
            def _():
                finish(s_b)

        for step, u in adds:

            @pl.when(mid & (n == step))
            def _(u=u):
                if u % 2 == 0:
                    shared(u // 2)
                unit(u)

    @pl.when(mid)
    def _():
        hint_copy.wait_recv()
        pl.semaphore_wait(ready.at[1], 1)
        unit(early)
        for j in range(parts):
            token_pass(2, third, j)
        shared(3)
        c_add(units - 1, third, slice(0, LANES), (0,))
        unit(units - 2)
        c_keys()
        for s in range(moved_seq):
            arrived(landed.at[s, pl.ds(0, 2)], rs_rx.at[s])
            for side in range(2):
                stage[s, 2 * row_y + side] += landed[s, side]
            x_half(s).start()
        c_add(units - 1, third, slice(LANES, 2 * LANES), (1,))
        c_states()

    def gather(s):
        arrived(landed.at[s, pl.ds(0, n_sp - 1)], rs_rx.at[s])
        total = None
        for j in range(n_sp):
            term = jnp.where(sp == j, totals[s], landed[s, j])
            total = term if total is None else total + term
        totals[s] = total

    sent(nx.at[pl.ds(0, chips)], n_share_tx)

    @pl.when(end)
    def _():
        pl.semaphore_wait(ready.at[1], 1)
        sent(nx.at[0], n_tx)
        sent(hint, hint_tx)
        sent(x.at[0], to_mate_tx)
        sent(x.at[pl.ds(0, chips), pl.ds(0, len(main))], share_tx)
        sent(we, w_tx)
        sent(stage.at[pl.ds(0, moved_seq), pl.ds(0, n_sp - 1)], rs_tx)

    @pl.when(mid)
    def _():
        sent(nx.at[pl.ds(0, 5)], n_tx)
        sent(x.at[pl.ds(0, chips - 1), pl.ds(0, len(main))], to_mate_tx)
        sent(x.at[pl.ds(0, 2)], to_other_tx)
        sent(x.at[pl.ds(0, chips)], share_tx)
        sent(xc.at[:, pl.ds(0, chips)], token_tx)
        sent(xc.at[:, pl.ds(0, chips)], token_share_tx)
        sent(stage.at[:, pl.ds(0, n_sp - 1)], rs_tx)

    @pl.when(mid)
    def _():
        for s in range(moved_seq):
            arrived(landed.at[s, 2], rs_rx.at[seqs + s])
            totals[s] = stage[s, sp] + landed[s, 2]
        gather(moved_seq)

    @pl.when(end)
    def _():
        for s in range(moved_seq):
            gather(s)
        arrived(landed_c, c_rx.at[0])
        for o in range(n_sp):
            start = (o // 2) * half + (o % 2) * LANES
            totals[moved_seq, :, start : start + LANES] = landed_c[o]

    for s in range(seqs):
        read = totals[s, keep : keep + 1]
        totals[s, keep : keep + 1] = read * rows_ref[1:2] + own_term[s : s + 1]

    @pl.when(mid)
    def _():
        sent(stage_c, c_tx)


def solution(mesh):
    n_sp, n_tp = mesh.shape["sp"], mesh.shape["tp"]

    def body(tokens, new_token, query_weight, key_weight, value_weight, log_decay):
        seqs, span, feat = tokens.shape
        width, inner = key_weight.shape
        heads = inner // HD
        keep = HD // n_sp
        rows = -(-(keep + 1) // 8) * 8
        chips = n_tp // 2
        half = HD // 2
        parts = max(1, 8 // chips)
        pieces = seqs * parts
        size = span // parts
        inverse = jnp.asarray(np.tile(inverse_angles(), LANES // half)[None])
        anywhere = pl.BlockSpec(memory_space=pl.ANY)
        vmem = pl.BlockSpec(memory_space=pltpu.VMEM)
        dma = pltpu.SemaphoreType.DMA
        moves = chips == 4 and n_sp == 4 and seqs > 1 and inner == 4 * LANES
        tokens_in = [
            pltpu.VMEM((n_tp, pieces, size, feat), BF16),
            pltpu.VMEM((n_tp, seqs, feat), BF16),
        ]
        weights_in = [pltpu.VMEM((width, inner), BF16)] * 3
        totals = [pltpu.VMEM((pieces, size, inner), F32)] * 2
        ends = [
            pltpu.VMEM((8, inner), F32),
            pltpu.VMEM((seqs, HD, inner), F32),
            pltpu.VMEM((NEW_ROWS, inner), F32),
            pltpu.VMEM((HD, inner), F32),
            pltpu.VMEM((seqs, n_sp, rows, inner), F32),
            pltpu.VMEM((seqs, n_sp, rows, inner), F32),
        ]
        if moves:
            call = moved_kernel
            scratch = (
                tokens_in[:1]
                + [pltpu.VMEM((3, n_tp, parts, size, feat), BF16)]
                + tokens_in[1:]
                + weights_in
                + [pltpu.VMEM((width, 2 * LANES), BF16)]
                + totals
                + [
                    pltpu.VMEM((n_sp, parts, size, 2 * LANES), F32),
                    pltpu.VMEM((n_sp, span, LANES), F32),
                    pltpu.VMEM((n_sp, span, LANES), F32),
                    pltpu.VMEM((span, inner), F32),
                ]
                + ends
                + [
                    pltpu.VMEM((8, inner), F32),
                    pltpu.VMEM((8, inner), F32),
                    pltpu.VMEM((n_sp, rows, LANES), F32),
                    pltpu.VMEM((n_sp, rows, LANES), F32),
                    dma((pieces + 1,)),
                    dma((3,)),
                    dma((n_tp, pieces)),
                    dma((chips + 1,)),
                    dma((3 * chips * parts + chips,)),
                    dma((n_tp + 1,)),
                    dma((11,)),
                    dma((1,)),
                    dma((2 * seqs,)),
                    dma((1,)),
                    pltpu.SemaphoreType.REGULAR((2,)),
                ]
            )
        else:
            call = kernel
            scratch = (
                tokens_in
                + weights_in
                + totals
                + [
                    pltpu.VMEM((span, LANES), F32),
                    pltpu.VMEM((span, LANES), F32),
                    pltpu.VMEM((span, inner), F32),
                ]
                + ends
                + [
                    pltpu.VMEM((seqs, rows, inner), F32),
                    dma((pieces + 1,)),
                    dma((3,)),
                    dma((n_tp, pieces)),
                    dma((n_tp,)),
                    dma((2, chips, pieces)),
                    dma((chips, pieces)),
                    dma((2, chips)),
                    dma((chips,)),
                    dma((seqs, n_sp)),
                    dma((seqs, n_sp)),
                ]
            )
        out_shape = (
            jax.ShapeDtypeStruct((seqs, heads, keep, HD), BF16),
            jax.ShapeDtypeStruct((seqs, inner), BF16),
        )
        shared = dict(
            scratch_shapes=scratch,
            name="retention",
        )
        args = (
            tokens, new_token.reshape(seqs, feat), query_weight, key_weight, value_weight
        )
        args = tuple(pltpu.with_memory_space_constraint(a, pltpu.HBM) for a in args)
        smem = pl.BlockSpec(memory_space=pltpu.SMEM)
        limit = (215 if moves else 240) * 256 * 1024
        params = pltpu.CompilerParams(
            collective_id=0, has_side_effects=True, vmem_limit_bytes=limit
        )
        call = functools.partial(call, n_sp, n_tp, parts)
        if not moves:
            return pl.pallas_call(
                call,
                out_shape=out_shape,
                in_specs=[anywhere] * 5 + [vmem, smem],
                out_specs=(vmem, vmem),
                compiler_params=params,
                **shared,
            )(*args, inverse, log_decay)
        sums = pl.pallas_call(
            call,
            out_shape=jax.ShapeDtypeStruct((seqs, rows, inner), F32),
            in_specs=[anywhere] * 5 + [smem],
            out_specs=vmem,
            compiler_params=params,
            **shared,
        )(*args, pltpu.with_memory_space_constraint(log_decay, pltpu.HBM))
        return pl.pallas_call(
            outputs,
            out_shape=out_shape,
            in_specs=[vmem],
            out_specs=(anywhere, anywhere),
            scratch_shapes=[pltpu.VMEM(out.shape, BF16) for out in out_shape] + [dma((2,))],
            compiler_params=pltpu.CompilerParams(vmem_limit_bytes=4 * 1024 * 1024),
            name="outputs",
        )(sums)

    return jax.shard_map(
        body,
        mesh=mesh,
        in_specs=(
            P(None, "sp", "tp"),
            P(None, None, "tp"),
            P(None, "tp"),
            P(None, "tp"),
            P(None, "tp"),
            P("tp"),
        ),
        out_specs=(P(None, "tp", "sp", None), P(None, "tp")),
        check_vma=False,
    )
```

```python
import functools

import jax
import jax.numpy as jnp
import numpy as np
from jax import lax
from jax.experimental import pallas as pl
from jax.experimental.pallas import tpu as pltpu
from jax.sharding import PartitionSpec as P

HD = 64
LANES = 128
NEW_ROWS = 8
F32 = jnp.float32
BF16 = jnp.bfloat16


def inverse_angles():
    half = HD // 2
    return np.float32(10000.0) ** (-np.arange(half, dtype=np.float32) / half)


def lane_iota(shape):
    return lax.broadcasted_iota(jnp.int32, shape, len(shape) - 1)


def rotated(block, cosine, sine):
    half = HD // 2
    low = lane_iota(block.shape) % HD < half
    swapped = jnp.where(
        low, pltpu.roll(block, LANES - half, 1), pltpu.roll(block, half, 1)
    )
    return block * cosine + swapped * sine


def kernel(
    n_sp, n_tp, parts,
    tokens, fresh, wq_hbm, wk_hbm, wv_hbm, inverse_ref, decay_ref,
    state_out, read_out,
    x, nx, wq, wk, wv, acc_k, acc_v, cos_ref, sin_ref, fade_ref, rows_ref,
    q_spread, own_term, sums, stage, landed, totals,
    load_sem, weight_sem, rx, rn, fwd, share, nfwd, nshare, rs_tx, rs_rx,
):
    seqs, span, feat = tokens.shape
    inner = wk.shape[1]
    heads = inner // HD
    chips = n_tp // 2
    pieces = seqs * parts
    size = span // parts
    keep = HD // n_sp
    sp = lax.axis_index("sp")
    tp = lax.axis_index("tp")
    z, k = tp // 2, tp % 2
    MESH = pl.DeviceIdType.MESH

    def to_tp(index):
        return {"tp": index}

    partner = z * 2 + 1 - k
    own_loads = [
        pltpu.make_async_copy(
            tokens.at[s // parts, pl.ds(s % parts * size, size)], x.at[tp, s], load_sem.at[s]
        )
        for s in range(pieces)
    ]
    new_load = pltpu.make_async_copy(fresh, nx.at[tp], load_sem.at[pieces])
    new_load.start()
    for copy in own_loads:
        copy.start()
    weight_loads = [
        pltpu.make_async_copy(a, b, weight_sem.at[i])
        for i, (a, b) in enumerate(((wk_hbm, wk), (wv_hbm, wv), (wq_hbm, wq)))
    ]

    barrier = pltpu.get_barrier_semaphore()

    @pl.when(z > 0)
    def _():
        pl.semaphore_signal(barrier, inc=1, device_id=to_tp(tp - 2), device_id_type=MESH)

    @pl.when(z < chips - 1)
    def _():
        pl.semaphore_signal(barrier, inc=1, device_id=to_tp(tp + 2), device_id_type=MESH)

    pl.semaphore_signal(barrier, inc=1, device_id=to_tp(partner), device_id_type=MESH)
    for o in range(1, n_sp):
        pl.semaphore_signal(
            barrier, inc=1, device_id={"sp": lax.rem(sp + o, n_sp)}, device_id_type=MESH
        )
    pl.semaphore_wait(
        barrier, n_sp + (z > 0).astype(jnp.int32) + (z < chips - 1).astype(jnp.int32)
    )

    def x_copy(c, s, sem, target):
        p = 2 * c + k
        return pltpu.make_async_remote_copy(
            x.at[p, s], x.at[p, s], sem, rx.at[p, s], device_id=to_tp(target), device_id_type=MESH
        )

    def n_copy(c, sem, target):
        p = 2 * c + k
        return pltpu.make_async_remote_copy(
            nx.at[p], nx.at[p], sem, rn.at[p], device_id=to_tp(target), device_id_type=MESH
        )

    def x_arrived(p, s):
        pltpu.make_async_remote_copy(
            x.at[p, s], x.at[p, s], share.at[0, 0], rx.at[p, s],
            device_id=to_tp(partner), device_id_type=MESH,
        ).wait_recv()

    def n_arrived(p):
        pltpu.make_async_remote_copy(
            nx.at[p], nx.at[p], nshare.at[0], rn.at[p],
            device_id=to_tp(partner), device_id_type=MESH,
        ).wait_recv()

    new_load.wait()
    n_up = n_copy(z, nfwd.at[0, z], tp + 2)
    n_down = n_copy(z, nfwd.at[1, z], tp - 2)
    n_side = n_copy(z, nshare.at[z], partner)

    @pl.when(z < chips - 1)
    def _():
        n_up.start()

    @pl.when(z > 0)
    def _():
        n_down.start()

    n_side.start()
    for s in range(pieces):
        own_loads[s].wait()

        @pl.when(z < chips - 1)
        def _(s=s):
            x_copy(z, s, fwd.at[0, z, s], tp + 2).start()

        @pl.when(z > 0)
        def _(s=s):
            x_copy(z, s, fwd.at[1, z, s], tp - 2).start()

        x_copy(z, s, share.at[z, s], partner).start()

    for copy in weight_loads:
        copy.start()

    row = lax.broadcasted_iota(jnp.int32, (span, LANES), 0)
    within = lane_iota((1, LANES)) % HD
    first_half = jnp.where(within < HD // 2, -1.0, 1.0).astype(F32)
    inverse = inverse_ref[...]
    angles = (sp * span + row).astype(F32) * inverse
    cos_ref[...] = jnp.cos(angles)
    sin_ref[...] = jnp.sin(angles) * first_half
    new_angles = jnp.full((NEW_ROWS, LANES), n_sp * span, F32) * inverse
    new_cos = jnp.cos(new_angles)
    new_sin = jnp.sin(new_angles) * first_half
    head_of = lane_iota((1, inner)) // HD
    rate = jnp.zeros((1, inner), F32)
    for h in range(heads):
        rate = jnp.where(head_of == h, decay_ref[h], rate)
    to_end = (span - 1 - lax.broadcasted_iota(jnp.int32, (span, 1), 0)).astype(F32)
    fade_ref[...] = jnp.exp(to_end * rate)
    rows_ref[0:1] = jnp.exp(rate * (span * (n_sp - 1 - sp)).astype(F32))
    rows_ref[1:2] = jnp.exp(rate)

    for copy in weight_loads:
        copy.wait()

    def add(p, s, fresh_total):
        block = x[p, s]
        where = pl.ds(pl.multiple_of(p * feat, feat), feat)
        part_k = jnp.dot(block, wk[where, :], preferred_element_type=F32)
        part_v = jnp.dot(block, wv[where, :], preferred_element_type=F32)
        if fresh_total:
            acc_k[s] = part_k
            acc_v[s] = part_v
        else:
            acc_k[s] += part_k
            acc_v[s] += part_v

    @pl.loop(0, pieces)
    def _(s):
        add(tp, s, True)
        x_arrived(partner, s)
        add(partner, s, False)

    n_arrived(partner)

    def project_new():
        def piece(p, totals):
            where = pl.ds(pl.multiple_of(p * feat, feat), feat)
            block = jnp.concatenate(
                [nx[p].astype(F32), jnp.zeros((NEW_ROWS - seqs, feat), F32)], axis=0
            ).astype(BF16)
            return tuple(
                t + jnp.dot(block, w[where, :], preferred_element_type=F32)
                for t, w in zip(totals, (wk, wv, wq))
            )

        zero = jnp.zeros((NEW_ROWS, inner), F32)
        new_k, new_v, new_q = lax.fori_loop(0, n_tp, piece, (zero, zero, zero))
        keys, queries = [], []
        for j in range(inner // LANES):
            at = slice(j * LANES, (j + 1) * LANES)
            keys.append((rotated(new_k[:, at], new_cos, new_sin) * HD**-0.5).astype(BF16))
            queries.append(rotated(new_q[:, at], new_cos, new_sin).astype(BF16))
        key = jnp.concatenate(keys, axis=1).astype(F32)
        query = jnp.concatenate(queries, axis=1).astype(F32)
        value = new_v.astype(BF16).astype(F32)
        same = (
            lax.broadcasted_iota(jnp.int32, (inner, inner), 0) // HD
            == lax.broadcasted_iota(jnp.int32, (inner, inner), 1) // HD
        )
        product = query * key
        for h in range(heads):
            at = slice(h * HD, (h + 1) * HD)
            own_term[:, at] = jnp.sum(product[:, at], axis=-1, keepdims=True) * value[:, at]
        pick = lax.broadcasted_iota(jnp.int32, (HD, inner), 0) == lane_iota((HD, inner)) % HD
        for s in range(seqs):
            spread = jnp.where(pick, query[s : s + 1], 0.0).astype(BF16)
            q_spread[s] = jnp.dot(
                spread, jnp.where(same, 1.0, 0.0).astype(BF16), preferred_element_type=F32
            )

    def rs_copy(s, o):
        peer = lax.rem(sp + o, n_sp)
        return pltpu.make_async_remote_copy(
            stage.at[s, peer], landed.at[s, sp], rs_tx.at[s, peer], rs_rx.at[s, sp],
            device_id={"sp": peer}, device_id_type=MESH,
        )

    def finish(i):
        s, part = i // parts, i % parts
        where = pl.ds(pl.multiple_of(part * size, size), size)
        cosine, sine = cos_ref[where, :], sin_ref[where, :]
        lane = lane_iota((HD, LANES))
        for j in range(inner // LANES):
            at = slice(j * LANES, (j + 1) * LANES)
            key = (rotated(acc_k[i, :, at], cosine, sine) * HD**-0.5).astype(BF16)
            weighted = (key.astype(F32) * fade_ref[where, at]).astype(BF16)
            value = acc_v[i, :, at].astype(BF16)
            both = lax.dot_general(
                weighted, value, (((0,), (0,)), ((), ())), preferred_element_type=F32
            )
            state = jnp.where(lane < HD, both[:HD], both[HD:])
            sums[:, at] = jnp.where(part == 0, state, sums[:, at] + state)

        @pl.when(part == parts - 1)
        def _():
            scaled = sums[...] * rows_ref[0:1]
            read = jnp.sum(scaled * q_spread[s], axis=0, keepdims=True)
            for o in range(n_sp):
                stage[s, o, 0:keep] = scaled[o * keep : (o + 1) * keep]
                stage[s, o, keep : keep + 1] = read
            for o in range(1, n_sp):
                rs_copy(s, o).start()
            totals[s] = stage[s, sp]

    far = jnp.maximum(z, chips - 1 - z)

    def decode(i):
        d = i // (2 * pieces) + 1
        s = (i // 2) % pieces
        step = 2 * (i % 2) - 1
        c = z + step * d
        return d, s, step, c, (c >= 0) & (c < chips)

    def onward(step):
        nxt = z - step
        return nxt, (nxt >= 0) & (nxt < chips), (step + 1) // 2

    @pl.loop(0, 2 * pieces * (chips - 1))
    def _(i):
        d, s, step, c, valid = decode(i)
        nxt, pass_on, way = onward(step)

        @pl.when(valid)
        def _():
            @pl.when(s == 0)
            def _():
                n_arrived(2 * c + k)

                @pl.when(pass_on)
                def _():
                    n_copy(c, nfwd.at[way, c], 2 * nxt + k).start()

                n_copy(c, nshare.at[c], partner).start()

            x_arrived(2 * c + k, s)

            @pl.when(pass_on)
            def _():
                x_copy(c, s, fwd.at[way, c, s], 2 * nxt + k).start()

            x_copy(c, s, share.at[c, s], partner).start()
            add(2 * c + k, s, False)

            @pl.when(s == 0)
            def _():
                n_arrived(2 * c + 1 - k)

            x_arrived(2 * c + 1 - k, s)
            add(2 * c + 1 - k, s, False)

        last = (d == far) & (step == 1)

        @pl.when(last & (s == 0))
        def _():
            project_new()

        @pl.when(last)
        def _():
            finish(s)

    raws = []
    for s in range(seqs):
        for o in range(1, n_sp):
            src = lax.rem(sp + o, n_sp)
            pltpu.make_async_remote_copy(
                stage.at[s, src], landed.at[s, src], rs_tx.at[s, src], rs_rx.at[s, src],
                device_id={"sp": src}, device_id_type=MESH,
            ).wait_recv()
        total = None
        for j in range(n_sp):
            term = jnp.where(sp == j, totals[s], landed[s, j])
            total = term if total is None else total + term
        kept = total[0:keep].astype(BF16)
        for h in range(heads):
            state_out[s, h] = kept[:, h * HD : (h + 1) * HD]
        raws.append(total[keep : keep + 1] * rows_ref[1:2] + own_term[s : s + 1])
    raw = jnp.concatenate(raws, axis=0)
    for h in range(heads):
        at = slice(h * HD, (h + 1) * HD)
        head = raw[:, at]
        centered = head - jnp.mean(head, axis=-1, keepdims=True)
        spread = jnp.mean(centered * centered, axis=-1, keepdims=True)
        read_out[:, at] = (centered * lax.rsqrt(spread + 1e-05)).astype(BF16)

    @pl.when(z < chips - 1)
    def _():
        n_up.wait_send()

    @pl.when(z > 0)
    def _():
        n_down.wait_send()

    n_side.wait_send()
    for s in range(seqs):
        for o in range(1, n_sp):
            rs_copy(s, o).wait_send()
    for s in range(pieces):
        @pl.when(z < chips - 1)
        def _(s=s):
            x_copy(z, s, fwd.at[0, z, s], tp + 2).wait_send()

        @pl.when(z > 0)
        def _(s=s):
            x_copy(z, s, fwd.at[1, z, s], tp - 2).wait_send()

        x_copy(z, s, share.at[z, s], partner).wait_send()

    @pl.loop(0, 2 * pieces * (chips - 1))
    def _(i):
        d, s, step, c, valid = decode(i)
        nxt, pass_on, way = onward(step)

        @pl.when(valid)
        def _():
            @pl.when(s == 0)
            def _():
                @pl.when(pass_on)
                def _():
                    n_copy(c, nfwd.at[way, c], 2 * nxt + k).wait_send()

                n_copy(c, nshare.at[c], partner).wait_send()

            @pl.when(pass_on)
            def _():
                x_copy(c, s, fwd.at[way, c, s], 2 * nxt + k).wait_send()

            x_copy(c, s, share.at[c, s], partner).wait_send()


def one_of(n, values):
    total = 0
    for k, value in enumerate(values):
        if value:
            total = total + (n == k).astype(jnp.int32) * value
    return total


def middle_order(main, moved):
    near = [(0, i) for i in main]
    far = [(2, i) for i in moved + main]
    order = [(kind, i) for i in moved for kind in (0, 1)]
    order += [(1, i) for i in main]
    for at in range(max(len(near), len(far))):
        order += far[at : at + 1] + near[at : at + 1]
    return order


def outputs(totals, state_out, read_out, state, read, sem):
    seqs, heads, keep, _ = state_out.shape
    raws = []
    for s in range(seqs):
        kept = totals[s, 0:keep].astype(BF16)
        for h in range(heads):
            state[s, h] = kept[:, h * HD : (h + 1) * HD]
        raws.append(totals[s, keep : keep + 1])
    state_copy = pltpu.make_async_copy(state, state_out, sem.at[0])
    state_copy.start()
    raw = jnp.concatenate(raws, axis=0)
    for h in range(heads):
        at = slice(h * HD, (h + 1) * HD)
        head = raw[:, at]
        centered = head - jnp.mean(head, axis=-1, keepdims=True)
        spread = jnp.mean(centered * centered, axis=-1, keepdims=True)
        read[:, at] = (centered * lax.rsqrt(spread + 1e-05)).astype(BF16)
    read_copy = pltpu.make_async_copy(read, read_out, sem.at[1])
    read_copy.start()
    state_copy.wait()
    read_copy.wait()


def moved_kernel(
    n_sp, n_tp, parts,
    tokens, fresh, wq_hbm, wk_hbm, wv_hbm, decay_ref,
    totals,
    x, xc, nx, wq, wk, wv, we, acc_k, acc_v, acc_c, cos_ref, sin_ref, fade_ref, rows_ref,
    q_spread, own_term, sums, stage, landed, hint, hint_in, stage_c, landed_c,
    load_sem, weight_sem, rx, rn, ry, rw, tx, hint_rx, rs_rx, c_rx, ready,
):
    seqs, span, feat = tokens.shape
    inner = wk.shape[1]
    heads = inner // HD
    half = inner // 2
    chips = n_tp // 2
    pieces = seqs * parts
    size = span // parts
    keep = HD // n_sp
    units = n_tp
    early = n_tp - 3
    moved_seq = seqs - 1
    to_mate_tx, to_other_tx, share_tx, n_tx, n_share_tx, token_tx, token_share_tx, w_tx = range(8)
    hint_tx, rs_tx, c_tx = range(8, 11)
    main = list(range(moved_seq * parts))
    moved = list(range(moved_seq * parts, pieces))
    sp = lax.axis_index("sp")
    tp = lax.axis_index("tp")
    z, k = tp // 2, tp % 2
    row_y, row_x = sp // 2, sp % 2
    x_peer = sp + 1 - 2 * row_x
    y_peer = sp + 2 - 4 * row_y
    columns = (sp, x_peer, y_peer, x_peer + y_peer - sp)
    MESH = pl.DeviceIdType.MESH
    end_int = (z == 0).astype(jnp.int32) + (z == chips - 1).astype(jnp.int32)
    end = end_int > 0
    mid = end_int == 0
    partner = z * 2 + 1 - k
    mate = z + 1 - 2 * (z % 2)
    mate_tp = 2 * mate + k
    other = chips - 1 - z
    other_tp = 2 * other + k
    second = end_int * (chips - 1 - mate) + (1 - end_int) * (chips - 1 - z)
    third = end_int * (chips - 1 - z) + (1 - end_int) * (chips - 1 - mate)

    own_loads = {
        s: pltpu.make_async_copy(
            tokens.at[s // parts, pl.ds(s % parts * size, size)], x.at[tp, s], load_sem.at[s]
        )
        for s in range(pieces)
    }
    new_load = pltpu.make_async_copy(fresh, nx.at[tp], load_sem.at[pieces])
    new_load.start()
    for s in moved + main:
        own_loads[s].start()
    weight_loads = [
        pltpu.make_async_copy(a, b, weight_sem.at[i])
        for i, (a, b) in enumerate(((wk_hbm, wk), (wv_hbm, wv), (wq_hbm, wq)))
    ]

    barrier = pltpu.get_barrier_semaphore()
    for target in ({"tp": partner}, {"tp": mate_tp}, {"sp": x_peer}, {"sp": y_peer}):
        pl.semaphore_signal(barrier, inc=1, device_id=target, device_id_type=MESH)

    @pl.when(mid)
    def _():
        pl.semaphore_signal(barrier, inc=1, device_id={"tp": other_tp}, device_id_type=MESH)

    pl.semaphore_wait(barrier, 5 - end_int)
    for target in ({"sp": x_peer}, {"sp": y_peer}):
        pl.semaphore_signal(ready.at[0], inc=1, device_id=target, device_id_type=MESH)

    def remote(source, dest, send, recv, target):
        return pltpu.make_async_remote_copy(
            source, dest, send, recv, device_id=target, device_id_type=MESH
        )

    def sent(ref, kind):
        remote(ref, ref, tx.at[kind], hint_rx.at[0], {"tp": partner}).wait_send()

    def arrived(ref, sem):
        remote(ref, ref, tx.at[0], sem, {"tp": partner}).wait_recv()

    def x_copy(c, s, kind, target):
        here = x.at[2 * c + k, s]
        return remote(here, here, tx.at[kind], rx.at[2 * c + k, s], {"tp": target})

    def to_mate(c, s):
        return x_copy(c, s, to_mate_tx, mate_tp)

    def to_other(c, s):
        return x_copy(c, s, to_other_tx, other_tp)

    def to_partner(c, s):
        return x_copy(c, s, share_tx, partner)

    def x_arrived(p, s):
        arrived(x.at[p, s], rx.at[p, s])

    def token_send(c, j):
        here = x.at[2 * c + k, moved[0] + j]
        for slot, target in ((0, x_peer), (1, y_peer)):
            remote(
                here, xc.at[slot, 2 * c + k, j], tx.at[token_tx],
                ry.at[(slot * chips + c) * parts + j], {"sp": target},
            ).start()

    def token_pass(slot, c, j):
        p = 2 * c + k
        here = xc.at[slot, p, j]
        arrived(here, ry.at[(slot * chips + c) * parts + j])
        if slot < 2 and slot == j % 2:
            remote(
                here, xc.at[2, p, j], tx.at[token_tx],
                ry.at[(2 * chips + c) * parts + j], {"sp": y_peer if slot == 0 else x_peer},
            ).start()
        remote(
            here, here, tx.at[token_share_tx], ry.at[3 * chips * parts + c], {"tp": partner}
        ).start()

    def w_rows(p):
        return pl.ds(pl.multiple_of(p * feat, feat), feat)

    def w_cols():
        return pl.ds(pl.multiple_of(row_y * half + row_x * LANES, LANES), LANES)

    def w_sem(u, kv):
        return rw.at[u + (kv if u == units - 1 else 0)]

    def w_send(u, kv):
        rows = w_rows(2 * (mate, z, second, third)[u // 2] + u % 2)
        return remote(
            (wk, wv)[kv].at[rows, w_cols()], we.at[rows, pl.ds(kv * LANES, LANES)],
            tx.at[w_tx], w_sem(u, kv), {"tp": mate_tp},
        )

    def n_copy(c, kind, sem, target):
        here = nx.at[2 * c + k]
        return remote(here, here, tx.at[kind], sem, {"tp": target})

    def n_to(c, target):
        n_copy(c, n_tx, rn.at[c], target).start()

    def n_share(c):
        n_copy(c, n_share_tx, rn.at[chips], partner).start()

    def n_arrived(c):
        arrived(nx.at[2 * c + k], rn.at[c])

    hint_copy = remote(hint, hint_in, tx.at[hint_tx], hint_rx.at[0], {"tp": mate_tp})

    new_load.wait()
    n_to(z, mate_tp)
    n_share(z)

    @pl.when(mid)
    def _():
        n_to(z, other_tp)

    for s in moved + main:
        own_loads[s].wait()

    def send_moved(j):
        s = moved[j]

        @pl.when(mid)
        def _():
            to_other(z, s).start()
            token_send(z, j)
            to_partner(z, s).start()

        @pl.when(end)
        def _():
            to_mate(z, s).start()

    send_moved(0)
    to_partner(z, main[0]).start()

    @pl.when(mid)
    def _():
        to_mate(z, main[0]).start()

    for copy in weight_loads:
        copy.start()

    @pl.when(mid)
    def _():
        n_arrived(mate)
        n_to(mate, other_tp)
        n_share(mate)
        n_arrived(other)
        n_to(other, mate_tp)
        n_share(other)

    for j in range(1, parts):
        send_moved(j)
    for s in main[1:]:
        to_partner(z, s).start()

    @pl.when(mid)
    def _():
        for s in main[1:2]:
            to_mate(z, s).start()
        for s in main:
            to_other(z, s).start()

    row = lax.broadcasted_iota(jnp.int32, (span, LANES), 0)
    within = lane_iota((1, LANES)) % HD
    first_half = jnp.where(within < HD // 2, -1.0, 1.0).astype(F32)
    inverse = jnp.zeros((1, LANES), F32)
    for j, step in enumerate(inverse_angles()):
        inverse = jnp.where(within % (HD // 2) == j, float(step), inverse)

    def tables(slot, column):
        angles = (column * span + row).astype(F32) * inverse
        cos_ref[slot] = jnp.cos(angles)
        sin_ref[slot] = jnp.sin(angles) * first_half

    for copy in weight_loads[:2]:
        copy.wait()

    @pl.when(end)
    def _():
        for u in range(2):
            for kv in range(2):
                w_send(u, kv).start()

    tables(0, sp)

    @pl.when(mid)
    def _():
        for slot in range(1, len(columns)):
            tables(slot, columns[slot])

    new_angles = jnp.full((NEW_ROWS, LANES), n_sp * span, F32) * inverse
    new_cos = jnp.cos(new_angles)
    new_sin = jnp.sin(new_angles) * first_half
    head_of = lane_iota((1, inner)) // HD
    rate = jnp.zeros((1, inner), F32)
    for h in range(heads):
        rate = jnp.where(head_of == h, decay_ref[h], rate)
    to_end = (span - 1 - lax.broadcasted_iota(jnp.int32, (span, 1), 0)).astype(F32)
    fade_ref[...] = jnp.exp(to_end * rate)
    rows_ref[0:1] = jnp.exp(rate * (span * (n_sp - 1 - sp)).astype(F32))
    rows_ref[1:2] = jnp.exp(rate)
    hint[...] = jnp.zeros(hint.shape, F32)
    hint[1:2] = rate
    weight_loads[2].wait()

    def add(p, s, fresh_total):
        block = x[p, s]
        where = w_rows(p)
        part_k = jnp.dot(block, wk[where, :], preferred_element_type=F32)
        part_v = jnp.dot(block, wv[where, :], preferred_element_type=F32)
        if fresh_total:
            acc_k[s] = part_k
            acc_v[s] = part_v
        else:
            acc_k[s] += part_k
            acc_v[s] += part_v

    same = (
        lax.broadcasted_iota(jnp.int32, (inner, inner), 0) // HD
        == lax.broadcasted_iota(jnp.int32, (inner, inner), 1) // HD
    )
    pick = lax.broadcasted_iota(jnp.int32, (HD, inner), 0) == lane_iota((HD, inner)) % HD

    @pl.when(mid)
    def _():
        n_arrived(third)
        n_to(third, mate_tp)
        n_share(third)
        for s in main[2:]:
            to_mate(z, s).start()

    own_pieces = end_int * len(main) + (1 - end_int) * pieces

    @pl.loop(0, pieces)
    def _(i):
        s = lax.rem(i + (1 - end_int) * len(main), pieces)

        @pl.when(i < own_pieces)
        def _():
            add(tp, s, True)

        @pl.when(i < own_pieces)
        def _():
            x_arrived(partner, s)
            add(partner, s, False)

    @pl.when(end)
    def _():
        for c in (mate, second, third):
            n_arrived(c)
            n_share(c)

    arrived(nx.at[pl.ds(0, chips)], rn.at[chips])

    def project_new():
        def piece(p, totals):
            where = w_rows(p)
            block = jnp.concatenate(
                [nx[p].astype(F32), jnp.zeros((NEW_ROWS - seqs, feat), F32)], axis=0
            ).astype(BF16)
            return tuple(
                t + jnp.dot(block, w[where, :], preferred_element_type=F32)
                for t, w in zip(totals, (wk, wv, wq))
            )

        zero = jnp.zeros((NEW_ROWS, inner), F32)
        new_k, new_v, new_q = lax.fori_loop(0, n_tp, piece, (zero, zero, zero))
        keys, queries = [], []
        for j in range(inner // LANES):
            at = slice(j * LANES, (j + 1) * LANES)
            keys.append((rotated(new_k[:, at], new_cos, new_sin) * HD**-0.5).astype(BF16))
            queries.append(rotated(new_q[:, at], new_cos, new_sin).astype(BF16))
        key = jnp.concatenate(keys, axis=1).astype(F32)
        query = jnp.concatenate(queries, axis=1).astype(F32)
        value = new_v.astype(BF16).astype(F32)
        product = query * key
        for h in range(heads):
            at = slice(h * HD, (h + 1) * HD)
            own_term[:, at] = jnp.sum(product[:, at], axis=-1, keepdims=True) * value[:, at]
        hint[0:1] = query[moved_seq : moved_seq + 1]
        for s in range(seqs):
            spread = jnp.where(pick, query[s : s + 1], 0.0).astype(BF16)
            q_spread[s] = jnp.dot(
                spread, jnp.where(same, 1.0, 0.0).astype(BF16), preferred_element_type=F32
            )

    project_new()

    @pl.when(end)
    def _():
        hint_copy.start()
        for s in main:
            to_mate(z, s).start()
        final = units - 1
        for u in range(2, final - 1):
            for kv in range(2):
                w_send(u, kv).start()
        for u, kv in ((final, 0), (final - 1, 0), (final - 1, 1), (final, 1)):
            w_send(u, kv).start()

    def rs_copy(s, o):
        peer = lax.rem(sp + o, n_sp)
        return remote(
            stage.at[s, peer], landed.at[s, sp], tx.at[rs_tx], rs_rx.at[s], {"sp": peer}
        )

    pl.semaphore_wait(ready.at[0], 2)
    pl.semaphore_signal(ready.at[1], inc=1, device_id={"sp": x_peer}, device_id_type=MESH)

    def y_half(s):
        return remote(
            stage.at[s, pl.ds(2 - 2 * row_y, 2)], landed.at[s, pl.ds(0, 2)],
            tx.at[rs_tx], rs_rx.at[s], {"sp": y_peer},
        )

    def x_half(s):
        return remote(
            stage.at[s, x_peer], landed.at[s, 2], tx.at[rs_tx], rs_rx.at[seqs + s], {"sp": x_peer}
        )

    def outer(weighted, value):
        both = lax.dot_general(
            weighted, value, (((0,), (0,)), ((), ())), preferred_element_type=F32
        )
        return jnp.where(lane_iota((HD, LANES)) < HD, both[:HD], both[HD:])

    def finish(i):
        s, part = i // parts, i % parts
        where = pl.ds(pl.multiple_of(part * size, size), size)
        cosine, sine = cos_ref[0, where, :], sin_ref[0, where, :]
        for j in range(inner // LANES):
            at = slice(j * LANES, (j + 1) * LANES)
            key = (rotated(acc_k[i, :, at], cosine, sine) * HD**-0.5).astype(BF16)
            weighted = (key.astype(F32) * fade_ref[where, at]).astype(BF16)
            value = acc_v[i, :, at].astype(BF16)
            state = outer(weighted, value)
            sums[:, at] = jnp.where(part == 0, state, sums[:, at] + state)

        @pl.when(part == parts - 1)
        def _():
            scaled = sums[...] * rows_ref[0:1]
            read = jnp.sum(scaled * q_spread[s], axis=0, keepdims=True)
            for o in range(n_sp):
                stage[s, o, 0:keep] = scaled[o * keep : (o + 1) * keep]
                stage[s, o, keep : keep + 1] = read
            totals[s] = stage[s, sp]

            @pl.when(end | (s == moved_seq))
            def _():
                for o in range(1, n_sp):
                    rs_copy(s, o).start()

            @pl.when(mid & (s < moved_seq))
            def _():
                y_half(s).start()

    def c_add(u, cx, at, halves):
        p = 2 * cx + u % 2
        for kv in halves:
            arrived(we.at[w_rows(p), at], w_sem(u, kv))
        for t in range(parts):
            for slot in range(len(columns)):
                block = x[p, moved[0] + t] if slot == 0 else xc[slot - 1, p, t]
                both = jnp.dot(block, we[w_rows(p), at], preferred_element_type=F32)
                if u == 0:
                    acc_c[slot, t, :, at] = both
                else:
                    acc_c[slot, t, :, at] += both

    def unit(u):
        c_add(u, (z, mate, second, third)[u // 2], slice(0, 2 * LANES), (0,))

    def c_copy(o):
        return remote(
            stage_c.at[o], landed_c.at[sp], tx.at[c_tx], c_rx.at[0], {"sp": o, "tp": mate_tp}
        )

    def key_rows(slot, t):
        return pl.ds((slot * parts + t) * size, size)

    def c_keys():
        pair_rate = hint_in[1:2, w_cols()]
        for t in range(parts):
            at = slice(t * size, (t + 1) * size)
            fade = jnp.exp(to_end[at] * pair_rate)
            for slot in range(len(columns)):
                key = (
                    rotated(acc_c[slot, t, :, :LANES], cos_ref[slot, at], sin_ref[slot, at])
                    * HD**-0.5
                ).astype(BF16)
                wq[key_rows(slot, t), 0:LANES] = (key.astype(F32) * fade).astype(BF16)

    def c_states():
        pair_rate = hint_in[1:2, w_cols()]
        query = hint_in[0:1, w_cols()]
        total = jnp.zeros((HD, LANES), F32)
        for slot, column in enumerate(columns):
            state = jnp.zeros((HD, LANES), F32)
            for t in range(parts):
                state = state + outer(wq[key_rows(slot, t), 0:LANES], acc_c[slot, t, :, LANES:].astype(BF16))
            total = total + state * jnp.exp(
                pair_rate * (span * (n_sp - 1 - column)).astype(F32)
            )
        spread = jnp.where(pick[:, :LANES], query, 0.0).astype(BF16)
        spread = jnp.dot(
            spread, jnp.where(same[:LANES, :LANES], 1.0, 0.0).astype(BF16),
            preferred_element_type=F32,
        )
        read = jnp.sum(total * spread, axis=0, keepdims=True)
        for o in range(n_sp):
            stage_c[o, 0:keep] = total[o * keep : (o + 1) * keep]
            stage_c[o, keep : keep + 1] = read
        for o in range(n_sp):
            c_copy(o).start()

    order = middle_order(main, moved)
    steps = end_int * (len(main) * (chips - 1)) + (1 - end_int) * len(order)

    def decode(n):
        kind = end_int * (n // len(main)) + (1 - end_int) * one_of(n, [o[0] for o in order])
        s = end_int * (n % len(main)) + (1 - end_int) * one_of(n, [o[1] for o in order])
        c = (
            (kind == 0).astype(jnp.int32) * mate
            + (kind == 1).astype(jnp.int32) * second
            + (kind == 2).astype(jnp.int32) * third
        )
        return kind, c, s

    last = len(order) - 1
    passes = (
        (0, ((0, 0, 0), (1, 0, 0))),
        (1, ((0, 0, 1), (1, 0, 1))),
        (5, ((0, 1, 0), (1, 1, 0))),
        (7, ((2, 0, 0), (2, 0, 1), (0, 2, 0), (1, 2, 0))),
        (8, ((0, 1, 1), (1, 1, 1))),
        (9, ((0, 2, 1), (1, 2, 1))),
        (13, ((2, 1, 0), (2, 1, 1))),
        (15, ((2, 2, 0), (2, 2, 1), (0, 3, 0), (1, 3, 0))),
        (17, ((0, 3, 1), (1, 3, 1))),
    )
    adds = ((8, 0), (9, 1), (14, 2), (15, 3), (16, 4))

    def chip(kind):
        return (z, mate, second, third)[kind]

    def shared(kind):
        arrived(xc.at[0, pl.ds(0, 3)], ry.at[3 * chips * parts + chip(kind)])

    @pl.loop(0, len(order) + 1)
    def _(n):
        kind, c, s = decode(n)
        is_moved = s >= moved[0]
        kind_b, c_b, s_b = decode(n - 1)

        @pl.when(end & (n >= 1) & (n <= steps))
        def _():
            x_arrived(2 * c_b + 1 - k, s_b)
            add(2 * c_b + 1 - k, s_b, False)

            @pl.when(kind_b == 2)
            def _():
                finish(s_b)

        @pl.when(n < steps)
        def _():
            x_arrived(2 * c + k, s)

            @pl.when(mid & (kind == 0))
            def _():
                to_other(c, s).start()

            @pl.when(mid & (kind > 0) & (s < moved[0]))
            def _():
                to_mate(c, s).start()

            @pl.when(mid & is_moved)
            def _():
                token_send(c, s - moved[0])

            to_partner(c, s).start()

        for step, events in passes:

            @pl.when(mid & (n == step))
            def _(events=events):
                for slot, kind, j in events:
                    token_pass(slot, chip(kind), j)

        @pl.when(n < steps)
        def _():
            add(2 * c + k, s, False)

        @pl.when(mid & (n >= 1))
        def _():
            x_arrived(2 * c_b + 1 - k, s_b)
            add(2 * c_b + 1 - k, s_b, False)

            @pl.when(kind_b == 2)
            def _():
                finish(s_b)

        for step, u in adds:

            @pl.when(mid & (n == step))
            def _(u=u):
                if u % 2 == 0:
                    shared(u // 2)
                unit(u)

    @pl.when(mid)
    def _():
        hint_copy.wait_recv()
        pl.semaphore_wait(ready.at[1], 1)
        unit(early)
        for j in range(parts):
            token_pass(2, third, j)
        shared(3)
        c_add(units - 1, third, slice(0, LANES), (0,))
        unit(units - 2)
        c_keys()
        for s in range(moved_seq):
            arrived(landed.at[s, pl.ds(0, 2)], rs_rx.at[s])
            for side in range(2):
                stage[s, 2 * row_y + side] += landed[s, side]
            x_half(s).start()
        c_add(units - 1, third, slice(LANES, 2 * LANES), (1,))
        c_states()

    def gather(s):
        arrived(landed.at[s, pl.ds(0, n_sp - 1)], rs_rx.at[s])
        total = None
        for j in range(n_sp):
            term = jnp.where(sp == j, totals[s], landed[s, j])
            total = term if total is None else total + term
        totals[s] = total

    sent(nx.at[pl.ds(0, chips)], n_share_tx)

    @pl.when(end)
    def _():
        pl.semaphore_wait(ready.at[1], 1)
        sent(nx.at[0], n_tx)
        sent(hint, hint_tx)
        sent(x.at[0], to_mate_tx)
        sent(x.at[pl.ds(0, chips), pl.ds(0, len(main))], share_tx)
        sent(we, w_tx)
        sent(stage.at[pl.ds(0, moved_seq), pl.ds(0, n_sp - 1)], rs_tx)

    @pl.when(mid)
    def _():
        sent(nx.at[pl.ds(0, 5)], n_tx)
        sent(x.at[pl.ds(0, chips - 1), pl.ds(0, len(main))], to_mate_tx)
        sent(x.at[pl.ds(0, 2)], to_other_tx)
        sent(x.at[pl.ds(0, chips)], share_tx)
        sent(xc.at[:, pl.ds(0, chips)], token_tx)
        sent(xc.at[:, pl.ds(0, chips)], token_share_tx)
        sent(stage.at[:, pl.ds(0, n_sp - 1)], rs_tx)

    @pl.when(mid)
    def _():
        for s in range(moved_seq):
            arrived(landed.at[s, 2], rs_rx.at[seqs + s])
            totals[s] = stage[s, sp] + landed[s, 2]
        gather(moved_seq)

    @pl.when(end)
    def _():
        for s in range(moved_seq):
            gather(s)
        arrived(landed_c, c_rx.at[0])
        for o in range(n_sp):
            start = (o // 2) * half + (o % 2) * LANES
            totals[moved_seq, :, start : start + LANES] = landed_c[o]

    for s in range(seqs):
        read = totals[s, keep : keep + 1]
        totals[s, keep : keep + 1] = read * rows_ref[1:2] + own_term[s : s + 1]

    @pl.when(mid)
    def _():
        sent(stage_c, c_tx)


def solution(mesh):
    n_sp, n_tp = mesh.shape["sp"], mesh.shape["tp"]

    def body(tokens, new_token, query_weight, key_weight, value_weight, log_decay):
        seqs, span, feat = tokens.shape
        width, inner = key_weight.shape
        heads = inner // HD
        keep = HD // n_sp
        rows = -(-(keep + 1) // 8) * 8
        chips = n_tp // 2
        half = HD // 2
        parts = max(1, 8 // chips)
        pieces = seqs * parts
        size = span // parts
        inverse = jnp.asarray(np.tile(inverse_angles(), LANES // half)[None])
        anywhere = pl.BlockSpec(memory_space=pl.ANY)
        vmem = pl.BlockSpec(memory_space=pltpu.VMEM)
        dma = pltpu.SemaphoreType.DMA
        moves = chips == 4 and n_sp == 4 and seqs > 1 and inner == 4 * LANES
        tokens_in = [
            pltpu.VMEM((n_tp, pieces, size, feat), BF16),
            pltpu.VMEM((n_tp, seqs, feat), BF16),
        ]
        weights_in = [pltpu.VMEM((width, inner), BF16)] * 3
        totals = [pltpu.VMEM((pieces, size, inner), F32)] * 2
        ends = [
            pltpu.VMEM((8, inner), F32),
            pltpu.VMEM((seqs, HD, inner), F32),
            pltpu.VMEM((NEW_ROWS, inner), F32),
            pltpu.VMEM((HD, inner), F32),
            pltpu.VMEM((seqs, n_sp, rows, inner), F32),
            pltpu.VMEM((seqs, n_sp, rows, inner), F32),
        ]
        if moves:
            call = moved_kernel
            scratch = (
                tokens_in[:1]
                + [pltpu.VMEM((3, n_tp, parts, size, feat), BF16)]
                + tokens_in[1:]
                + weights_in
                + [pltpu.VMEM((width, 2 * LANES), BF16)]
                + totals
                + [
                    pltpu.VMEM((n_sp, parts, size, 2 * LANES), F32),
                    pltpu.VMEM((n_sp, span, LANES), F32),
                    pltpu.VMEM((n_sp, span, LANES), F32),
                    pltpu.VMEM((span, inner), F32),
                ]
                + ends
                + [
                    pltpu.VMEM((8, inner), F32),
                    pltpu.VMEM((8, inner), F32),
                    pltpu.VMEM((n_sp, rows, LANES), F32),
                    pltpu.VMEM((n_sp, rows, LANES), F32),
                    dma((pieces + 1,)),
                    dma((3,)),
                    dma((n_tp, pieces)),
                    dma((chips + 1,)),
                    dma((3 * chips * parts + chips,)),
                    dma((n_tp + 1,)),
                    dma((11,)),
                    dma((1,)),
                    dma((2 * seqs,)),
                    dma((1,)),
                    pltpu.SemaphoreType.REGULAR((2,)),
                ]
            )
        else:
            call = kernel
            scratch = (
                tokens_in
                + weights_in
                + totals
                + [
                    pltpu.VMEM((span, LANES), F32),
                    pltpu.VMEM((span, LANES), F32),
                    pltpu.VMEM((span, inner), F32),
                ]
                + ends
                + [
                    pltpu.VMEM((seqs, rows, inner), F32),
                    dma((pieces + 1,)),
                    dma((3,)),
                    dma((n_tp, pieces)),
                    dma((n_tp,)),
                    dma((2, chips, pieces)),
                    dma((chips, pieces)),
                    dma((2, chips)),
                    dma((chips,)),
                    dma((seqs, n_sp)),
                    dma((seqs, n_sp)),
                ]
            )
        out_shape = (
            jax.ShapeDtypeStruct((seqs, heads, keep, HD), BF16),
            jax.ShapeDtypeStruct((seqs, inner), BF16),
        )
        shared = dict(
            scratch_shapes=scratch,
            name="retention",
        )
        args = (
            tokens, new_token.reshape(seqs, feat), query_weight, key_weight, value_weight
        )
        args = tuple(pltpu.with_memory_space_constraint(a, pltpu.HBM) for a in args)
        smem = pl.BlockSpec(memory_space=pltpu.SMEM)
        limit = (215 if moves else 240) * 256 * 1024
        params = pltpu.CompilerParams(
            collective_id=0, has_side_effects=True, vmem_limit_bytes=limit
        )
        call = functools.partial(call, n_sp, n_tp, parts)
        if not moves:
            return pl.pallas_call(
                call,
                out_shape=out_shape,
                in_specs=[anywhere] * 5 + [vmem, smem],
                out_specs=(vmem, vmem),
                compiler_params=params,
                **shared,
            )(*args, inverse, log_decay)
        sums = pl.pallas_call(
            call,
            out_shape=jax.ShapeDtypeStruct((seqs, rows, inner), F32),
            in_specs=[anywhere] * 5 + [smem],
            out_specs=vmem,
            compiler_params=params,
            **shared,
        )(*args, pltpu.with_memory_space_constraint(log_decay, pltpu.HBM))
        return pl.pallas_call(
            outputs,
            out_shape=out_shape,
            in_specs=[vmem],
            out_specs=(anywhere, anywhere),
            scratch_shapes=[pltpu.VMEM(out.shape, BF16) for out in out_shape] + [dma((2,))],
            compiler_params=pltpu.CompilerParams(vmem_limit_bytes=4 * 1024 * 1024),
            name="outputs",
        )(sums)

    return jax.shard_map(
        body,
        mesh=mesh,
        in_specs=(
            P(None, "sp", "tp"),
            P(None, None, "tp"),
            P(None, "tp"),
            P(None, "tp"),
            P(None, "tp"),
            P("tp"),
        ),
        out_specs=(P(None, "tp", "sp", None), P(None, "tp")),
        check_vma=False,
    )
```
